32 devices in a mesh: sp: 16 (over z, y, x), tp: 2 (over core).
Axes of the slice: x: 2, y: 2, z: 4, core: 2. Of those that a mesh axis runs over, the one named last changes fastest.
Arguments:
- stream: bfloat16 [6144, 2048], P('sp'), may hold values from -40 to 40
- query_rows: bfloat16 [6144, 1024], P('sp', 'tp'), may hold values from -10 to 10
- key_rows: bfloat16 [6144, 256], P('sp'), may hold values from -10 to 10
- value_rows: bfloat16 [6144, 256], P('sp'), may hold values from -6 to 6
- doc_ids: int32 [6144], P('sp'), may hold values from 0 to 7, never falling along the last dimension, each value on 1 to 1536 neighbouring positions
- sink_logit: float32 [8], P('tp'), may hold values from 2 to 7
- out_weight: bfloat16 [1024, 2048], P('tp'), may hold values from -1.5 to 1.5
- norm_gain: float32 [2048], replicated, may hold values from 0.1 to 1.9
- gate_weight: bfloat16 [2048, 5632], P('sp', 'tp'), may hold values from -0.125 to 0.125
- up_weight: bfloat16 [2048, 5632], P('sp', 'tp'), may hold values from -0.125 to 0.125
- down_weight: bfloat16 [5632, 2048], P('tp', 'sp'), may hold values from -0.078125 to 0.078125
Outputs:
- mixed_out: bfloat16 [6144, 2048], P('sp')
The draws below stay inside these ranges and needn't reach their ends.
Inputs may be any that keep to these rules, and one draw needn't show every extreme that they name: `doc_ids`: document numbers never fall along the sequence; each document has 1 to 1536 positions.
All inputs are finite; a program needn't handle non-finite values.
Results may differ from the reference program's by a relative error of at most 0.009.
Values may be sent and summed in bfloat16 or wider, within the bound.
A program may use at most 128 MiB of HBM per device.

```python
import math
import jax
import jax.numpy as jnp
import numpy as np
from jax import lax

D = 2048
FF = 5632
HEADS = 8
KVH = 2
HD = 128
WIN = 128
TOK_DEV = 384
TOKENS = 6144
DOCS = 8
DOC_MOST = 1536
N_TP = 2


def draw_stream(key, part):
    first_key, second_key = jax.random.split(key, 2)
    column_scale = 3.0 ** (jnp.arange(D, dtype=jnp.float32) / D)
    base = jnp.clip(jax.random.normal(first_key, (TOKENS, D), jnp.float32), -6.0, 6.0)
    row_scale = jnp.exp(jax.random.uniform(second_key, (TOKENS, 1), jnp.float32, -0.7, 0.7))
    values = base * row_scale * column_scale[None, :]
    return values.astype(jnp.bfloat16)


def draw_query_rows(key, part):
    values = jnp.clip(jax.random.normal(jax.random.fold_in(key, 1), (TOKENS, HEADS * HD), jnp.float32), -6.0, 6.0)
    return values.astype(jnp.bfloat16)


def draw_key_rows(key, part):
    values = jnp.clip(jax.random.normal(jax.random.fold_in(key, 2), (TOKENS, KVH * HD), jnp.float32), -6.0, 6.0)
    return values.astype(jnp.bfloat16)


def block_levels(stream_key, dims, pieces, least, largest):
    def one(dim, blocks):
        heights = jax.random.uniform(jax.random.fold_in(jax.random.fold_in(stream_key, 6), dim), (blocks,), jnp.float32, least / len(pieces), largest / len(pieces))
        return jnp.repeat(jnp.exp(heights), dims[dim] // blocks).reshape((-1,) + (1,) * (len(dims) - dim - 1))

    loudness = one(*pieces[0])
    for cut in pieces[1:]:
        loudness = loudness * one(*cut)
    return loudness


def profile(count, total, reach, slope):
    portions = [(1 << 20) // math.isqrt(rank ** slope) + 1 for rank in range(2, count + 1)]
    surplus, holding = total - reach - (count - 1), [1] * (count - 1)
    while surplus > 0:
        free = [i for i in range(count - 1) if holding[i] < reach]
        whole, remaining = sum([portions[i] for i in free]), surplus
        for i in free:
            more = min(reach - holding[i], max(1, remaining * portions[i] // whole), surplus)
            holding[i] = holding[i] + more
            surplus = surplus - more
    return np.array([reach] + holding)


def uneven_parts(rng, count, total, limit, skew):
    if count == 2:
        one = jax.random.randint(rng, (), max(1, total - limit), min(limit, total - 1) + 1)
        return jnp.stack([one, total - one])
    lengths = jnp.asarray(profile(count, total, limit, skew), jnp.int32)
    couples = (count - 1) // 2
    source_of, sink = lengths[1:1 + 2 * couples:2], lengths[2:2 + 2 * couples:2]
    room = jnp.minimum(source_of - 1, limit - sink)
    passed = jax.random.randint(jax.random.fold_in(rng, 1), (couples,), 0, 1 << 20) % (room + 1)
    lengths = lengths.at[1:1 + 2 * couples:2].set(source_of - passed).at[2:2 + 2 * couples:2].set(sink + passed)
    return lengths[jax.random.permutation(jax.random.fold_in(rng, 2), count)]


def noise(own_key, shape, scale, bound, cuts=(), kind=jnp.bfloat16):
    level = block_levels(own_key, shape, cuts, -0.22, 0.18) if cuts else 1.0
    entries = jax.random.normal(own_key, shape, jnp.float32) * scale * level
    return jnp.minimum(jnp.maximum(entries, -bound), bound).astype(kind)


def setup_inputs(seed: int = 0) -> dict:
    splits = jax.random.split(jax.random.key(seed), 12)
    return {
        "stream": draw_stream(jax.random.fold_in(splits[11], 71), 0),
        "query_rows": draw_query_rows(jax.random.fold_in(splits[11], 71), 0),
        "key_rows": draw_key_rows(jax.random.fold_in(splits[11], 71), 0),
        "value_rows": noise(splits[3], (TOKENS, KVH * HD), 1.0, 6.0, ((0, 16),)),
        "doc_ids": jnp.searchsorted(jnp.cumsum(uneven_parts(splits[4], DOCS, TOKENS, DOC_MOST, 1)), jnp.arange(TOKENS), side="right").astype(jnp.int32),
        "sink_logit": jnp.clip(2.0 + 5.0 * jax.random.uniform(splits[5], (HEADS,), jnp.float32) ** block_levels(splits[5], (HEADS,), ((0, 2),), -0.2, 0.2), 2.0, 7.0),
        "out_weight": noise(splits[6], (HEADS * HD, D), (HEADS * HD // 64) ** -0.5, 1.5, ((0, 2),)),
        "norm_gain": jnp.clip(1.0 + 0.18 * jax.random.normal(splits[7], (D,), jnp.float32), 0.1, 1.9),
        "gate_weight": noise(splits[8], (D, FF), D ** -0.5, 0.125, ((0, 16), (1, 2))),
        "up_weight": noise(splits[9], (D, FF), D ** -0.5, 0.125, ((0, 16), (1, 2))),
        "down_weight": noise(splits[10], (FF, D), FF ** -0.5, 0.078125, ((0, 2), (1, 16))),
    }


norm_eps = 1e-06
masked_low = -1e+30

def reference(stream, query_rows, key_rows, value_rows, doc_ids, sink_logit, out_weight, norm_gain, gate_weight, up_weight, down_weight):
    seq_total = stream.shape[0]
    group_share = HEADS // KVH
    keys_pad = jnp.pad(key_rows, ((WIN, WIN), (0, 0)))
    values_pad = jnp.pad(value_rows, ((WIN, WIN), (0, 0)))
    docs_pad = jnp.pad(doc_ids, (WIN, WIN))
    head_block = HEADS * HD // N_TP
    ff_block = FF // N_TP
    span = TOK_DEV + 2 * WIN

    def one_block(block_id):
        begin_at = (block_id * TOK_DEV).astype(jnp.int32)
        queries = lax.dynamic_slice_in_dim(query_rows, begin_at, TOK_DEV, 0).astype(jnp.float32).reshape(TOK_DEV, KVH, group_share, HD)
        keys_grid = lax.dynamic_slice_in_dim(keys_pad, begin_at, span, 0).astype(jnp.float32).reshape(span, KVH, HD)
        values_grid = lax.dynamic_slice_in_dim(values_pad, begin_at, span, 0).astype(jnp.float32).reshape(span, KVH, HD)
        docs_here = lax.dynamic_slice_in_dim(doc_ids, begin_at, TOK_DEV, 0)
        docs_wide = lax.dynamic_slice_in_dim(docs_pad, begin_at, span, 0)
        query_pos = begin_at + jnp.arange(TOK_DEV, dtype=jnp.int32)
        key_pos = begin_at - WIN + jnp.arange(span, dtype=jnp.int32)
        allowed = (jnp.abs(query_pos[:, None] - key_pos[None, :]) <= WIN) & (key_pos[None, :] >= 0) & (key_pos[None, :] < seq_total) & (docs_here[:, None] == docs_wide[None, :])
        scores = jnp.einsum('qgrd,kgd->grqk', queries, keys_grid) * HD ** (-0.5)
        masked = jnp.where(allowed[None, None], scores, masked_low)
        sinks = sink_logit.astype(jnp.float32).reshape(KVH, group_share, 1, 1)
        peak = jnp.maximum(lax.optimization_barrier(jnp.max(masked, axis=-1, keepdims=True)), sinks)
        lifted = jnp.where(allowed[None, None], jnp.exp(masked - peak), 0.0)
        denom = lax.optimization_barrier(jnp.sum(lifted, axis=-1, keepdims=True)) + jnp.exp(sinks - peak)
        probs = (lifted / denom).astype(jnp.bfloat16)
        attended = jnp.einsum('grqk,kgd->qgrd', probs.astype(jnp.float32), values_grid)
        attended = attended.astype(jnp.bfloat16).reshape(TOK_DEV, HEADS * HD)
        branch_sum = jnp.zeros((TOK_DEV, D), jnp.float32)
        for part_id in range(N_TP):
            term = jnp.dot(attended[:, part_id * head_block:(part_id + 1) * head_block], out_weight[part_id * head_block:(part_id + 1) * head_block], preferred_element_type=jnp.float32)
            branch_sum = branch_sum + lax.optimization_barrier(term.astype(jnp.bfloat16)).astype(jnp.float32)
        branch = branch_sum.astype(jnp.bfloat16)
        stream_here = lax.dynamic_slice_in_dim(stream, begin_at, TOK_DEV, 0)
        carried = (stream_here.astype(jnp.float32) + branch.astype(jnp.float32)).astype(jnp.bfloat16)
        carried_f = carried.astype(jnp.float32)
        normed = (carried_f * lax.rsqrt(lax.optimization_barrier(jnp.mean(carried_f * carried_f, axis=1, keepdims=True)) + norm_eps) * norm_gain.astype(jnp.float32)).astype(jnp.bfloat16)
        gate_acc = jnp.dot(normed, gate_weight, preferred_element_type=jnp.float32)
        up_acc = jnp.dot(normed, up_weight, preferred_element_type=jnp.float32)
        hidden = (jax.nn.silu(gate_acc) * up_acc).astype(jnp.bfloat16)
        feed_sum = jnp.zeros((TOK_DEV, D), jnp.float32)
        for part_id in range(N_TP):
            term = jnp.dot(hidden[:, part_id * ff_block:(part_id + 1) * ff_block], down_weight[part_id * ff_block:(part_id + 1) * ff_block], preferred_element_type=jnp.float32)
            feed_sum = feed_sum + lax.optimization_barrier(term.astype(jnp.bfloat16)).astype(jnp.float32)
        feed = feed_sum.astype(jnp.bfloat16)
        return (carried_f + 0.5 * feed.astype(jnp.float32)).astype(jnp.bfloat16)
    blocks_all = lax.map(one_block, jnp.arange(seq_total // TOK_DEV, dtype=jnp.int32))
    return blocks_all.reshape(seq_total, D)
```

```python
import jax
import jax.numpy as jnp
from jax import lax
from jax.experimental import pallas as pl
from jax.experimental.pallas import tpu as pltpu
from jax.sharding import Mesh, PartitionSpec as P

HEADS = 8
KVH = 2
HD = 128
WIN = 128

norm_eps = 1e-06
masked_low = -1e30
SP = ("sa", "sb")


def halo(value, width):
    peers = lax.axis_size(SP)
    length = value.shape[0]
    up = [(i, i + 1) for i in range(peers - 1)]
    down = [(j, i) for i, j in up]
    before = lax.ppermute(value[length - width :], SP, up)
    after = lax.ppermute(value[:width], SP, down)
    return jnp.concatenate([before, value, after], axis=0)


def exchange(blocks):
    peers = lax.axis_size("sa")
    here = lax.axis_index("sa")
    got = [lax.dynamic_index_in_dim(blocks, here, 0, keepdims=True)]
    for k in range(1, peers):
        out = lax.dynamic_index_in_dim(blocks, lax.rem(here + k, peers), 0, keepdims=True)
        got.append(lax.ppermute(out, "sa", [(i, (i + k) % peers) for i in range(peers)]))
    ring = got[::-1]
    both = jnp.concatenate(ring + ring, axis=0)
    return lax.dynamic_slice_in_dim(both, peers - 1 - here, peers, 0)


def per_device(
    stream,
    query_rows,
    key_rows,
    value_rows,
    doc_ids,
    sink_logit,
    out_weight,
    norm_gain,
    gate_weight,
    up_weight,
    down_weight,
):
    row_count, width = stream.shape
    n_a, n_b, n_tp = lax.axis_size("sa"), lax.axis_size("sb"), lax.axis_size("tp")
    depth, hidden_here = gate_weight.shape
    share = hidden_here // n_a
    tp_place = lax.axis_index("tp")
    sp_place = lax.axis_index(SP)

    def shares(w):
        return w.reshape(depth, n_a, share).transpose(1, 0, 2)

    gate_up = exchange(jnp.concatenate([shares(gate_weight), shares(up_weight)], axis=2))
    gate_up = gate_up.reshape(n_a * depth, 2 * share)
    gate_up = lax.all_gather(gate_up, "sb", axis=0, tiled=True)
    down_mine = exchange(down_weight.reshape(n_a, share, depth))
    down_mine = down_mine.transpose(0, 2, 1).reshape(n_a * depth, share)

    heads_here = query_rows.shape[1] // HD
    group_share = HEADS // KVH
    groups_here = max(1, heads_here // group_share)
    per_group = heads_here // groups_here
    group_first = tp_place * heads_here // group_share
    keys_here = lax.dynamic_slice_in_dim(key_rows, group_first * HD, groups_here * HD, 1)
    values_here = lax.dynamic_slice_in_dim(value_rows, group_first * HD, groups_here * HD, 1)
    docs_col = jnp.broadcast_to(doc_ids.astype(jnp.bfloat16)[:, None], (row_count, HD))
    packed = halo(jnp.concatenate([keys_here, values_here, docs_col], axis=1), WIN)
    span = groups_here * HD
    keys_wide, values_wide = packed[:, :span], packed[:, span : 2 * span]
    docs_wide = packed[:, 2 * span].astype(jnp.int32)
    seq_offset = sp_place * row_count
    seq_total = row_count * n_a * n_b
    query_pos = seq_offset + jnp.arange(row_count, dtype=jnp.int32)
    key_pos = seq_offset - WIN + jnp.arange(row_count + 2 * WIN, dtype=jnp.int32)
    allowed = (
        (jnp.abs(query_pos[:, None] - key_pos[None, :]) <= WIN)
        & (key_pos[None, :] >= 0)
        & (key_pos[None, :] < seq_total)
        & (doc_ids[:, None] == docs_wide[None, :])
    )
    queries = query_rows.reshape(row_count, groups_here, per_group, HD)
    keys_grid = keys_wide.reshape(row_count + 2 * WIN, groups_here, HD)
    values_grid = values_wide.reshape(row_count + 2 * WIN, groups_here, HD)
    scores = jnp.einsum(
        "qgrd,kgd->grqk", queries, keys_grid, preferred_element_type=jnp.float32
    ) * HD ** (-0.5)
    masked = jnp.where(allowed[None, None], scores, masked_low)
    sinks = sink_logit.reshape(groups_here, per_group, 1, 1)
    peak = jnp.maximum(jnp.max(masked, axis=-1, keepdims=True), sinks)
    lifted = jnp.where(allowed[None, None], jnp.exp(masked - peak), 0.0)
    denom = jnp.sum(lifted, axis=-1, keepdims=True) + jnp.exp(sinks - peak)
    probs = (lifted / denom).astype(jnp.bfloat16)
    attended = jnp.einsum("grqk,kgd->qgrd", probs, values_grid, preferred_element_type=jnp.float32)
    attended = attended.astype(jnp.bfloat16).reshape(row_count, heads_here * HD)
    partial_value = jnp.dot(attended, out_weight, preferred_element_type=jnp.float32)

    rows_mine = row_count // n_tp
    branch = lax.psum_scatter(
        partial_value.astype(jnp.bfloat16), "tp", scatter_dimension=0, tiled=True
    )
    stream_mine = lax.dynamic_slice_in_dim(stream, tp_place * rows_mine, rows_mine, 0)
    carried = (stream_mine.astype(jnp.float32) + branch.astype(jnp.float32)).astype(jnp.bfloat16)
    carried_f = carried.astype(jnp.float32)
    normed = (
        carried_f
        * lax.rsqrt(jnp.mean(carried_f * carried_f, axis=1, keepdims=True) + norm_eps)
        * norm_gain[None, :]
    ).astype(jnp.bfloat16)
    normed = normed.reshape(rows_mine, n_a, n_b, depth).transpose(0, 2, 1, 3).reshape(rows_mine, width)
    rows_all = lax.all_gather(normed, ("sa", "tp"), axis=0, tiled=True)
    down_mine, _ = lax.optimization_barrier((down_mine, normed))
    down_all = lax.all_gather(down_mine, "sb", axis=0, tiled=True)

    gate_acc = jnp.dot(rows_all, gate_up[:, :share], preferred_element_type=jnp.float32)
    up_acc = jnp.dot(rows_all, gate_up[:, share:], preferred_element_type=jnp.float32)
    hidden = (jax.nn.silu(gate_acc) * up_acc).astype(jnp.bfloat16)
    terms = lax.dot_general(
        hidden, down_all, (((1,), (1,)), ((), ())), preferred_element_type=jnp.float32
    )
    feed = lax.psum_scatter(
        terms.astype(jnp.bfloat16), ("sa", "tp"), scatter_dimension=0, tiled=True
    )
    feed = feed.reshape(rows_mine, n_b, n_a, depth).transpose(0, 2, 1, 3).reshape(rows_mine, width)
    mixed = (carried_f + 0.5 * feed.astype(jnp.float32)).astype(jnp.bfloat16)
    return lax.all_gather(mixed, "tp", axis=0, tiled=True)


MESH = pl.DeviceIdType.MESH
AX = ("sa", "sy", "sx", "tp")


def fused(
    stream_ref, query_ref, key_ref, value_ref, docs_ref, sink_ref, out_w_ref, gain_ref, own_w_ref,
    mixed_ref,
    keys, values, docs, attended, branch_out, branch_in, carried_keep, rows, weights, hidden_keep,
    sum_keep, pair_out, pair_in, chain_out, chain_fwd, chain_back,
    halo_s, halo_r, a2a_s, a2a_r, x_s, x_r, y_s, y_r, fx_s, fx_r, fy_s, fy_r,
    br_s, br_r, agf_s, agb_s, agz_r, agc_s, agc_r, pair_s, pair_r,
    cf_s, cb_s, cf_r, cb_r, fin_s, fin_r,
):
    n_a = own_w_ref.shape[0]
    n_tp = 2
    z, y, x, c = [lax.axis_index(a) for a in AX]
    place = (z * 2 + y) * 2 + x
    places = n_a * 4
    row_count, width = stream_ref.shape
    half = row_count // n_tp
    piece = own_w_ref.shape[1]
    share = piece // 3
    part = piece // 2
    hi = z // 2
    w = z + hi * (3 - 2 * z)
    z_fwd = z + 1 - 2 * hi
    z_back = z - 1 + 2 * hi
    here = (z, y, x, c)
    partner = (z, y, x, 1 - c)
    x_next = (z, y, 1 - x, c)
    y_next = (z, 1 - y, x, c)
    fwd = (z_fwd, y, x, c)
    back = (z_back, y, x, c)

    def block_at(b):
        return b + hi * (3 - 2 * b)

    def remote(src, dst, s_sem, r_sem, device):
        return pltpu.make_async_remote_copy(
            src_ref=src, dst_ref=dst, send_sem=s_sem, recv_sem=r_sem,
            device_id=device, device_id_type=MESH,
        )

    def at_place(p):
        return (p // 4, (p // 2) % 2, p % 2, c)

    head_cols = pl.ds(pl.multiple_of(c * HD, HD), HD)
    edge = row_count - WIN
    blocks = row_count // WIN

    def halo_copies(to_next):
        if to_next:
            dev, src, dst, d_src, d_dst, o = at_place(place + 1), edge, 0, blocks - 1, 0, 0
        else:
            dev, src, dst, d_src, d_dst, o = at_place(place - 1), 0, row_count + WIN, 0, blocks + 1, 3
        return [
            remote(key_ref.at[pl.ds(src, WIN), head_cols], keys.at[pl.ds(dst, WIN)], halo_s.at[o], halo_r.at[o], dev),
            remote(value_ref.at[pl.ds(src, WIN), head_cols], values.at[pl.ds(dst, WIN)], halo_s.at[o + 1], halo_r.at[o + 1], dev),
            remote(docs_ref.at[d_src], docs.at[d_dst], halo_s.at[o + 2], halo_r.at[o + 2], dev),
        ]

    @pl.when(place < places - 1)
    def _():
        for cp in halo_copies(True):
            cp.start()

    @pl.when(place > 0)
    def _():
        for cp in halo_copies(False):
            cp.start()

    def column(zz, yy, xx):
        return pl.ds(pl.multiple_of(((zz * 2 + yy) * 2 + xx) * HD, HD), HD)

    peers = [z + 1 - 2 * (z % 2), (z + 2) % n_a, n_a - 1 - z]

    def a2a(k):
        to = peers[k]
        return remote(own_w_ref.at[to], weights.at[:, column(z, y, x)], a2a_s.at[to], a2a_r.at[z], (to, y, x, c))

    def a2a_arrived(k):
        frm = peers[k]
        remote(own_w_ref.at[frm], weights.at[:, column(frm, y, x)], a2a_s.at[frm], a2a_r.at[frm], here).wait_recv()

    def side(zz, along_x):
        block = weights.at[:, column(zz, y, x)]
        if along_x:
            return remote(block, block, x_s.at[zz], x_r.at[zz], x_next)
        return remote(block, block, y_s.at[zz], y_r.at[zz], y_next)

    def side_arrived(zz, along_x):
        if along_x:
            block = weights.at[:, column(zz, y, 1 - x)]
            remote(block, block, x_s.at[zz], x_r.at[zz], here).wait_recv()
        else:
            block = weights.at[:, column(zz, 1 - y, x)]
            remote(block, block, y_s.at[zz], y_r.at[zz], here).wait_recv()

    def corner(zz, along_x):
        if along_x:
            block = weights.at[pl.ds(part, part), column(zz, 1 - y, x)]
            return remote(block, block, fx_s.at[zz], fx_r.at[zz], x_next)
        block = weights.at[pl.ds(0, part), column(zz, y, 1 - x)]
        return remote(block, block, fy_s.at[zz], fy_r.at[zz], y_next)

    def corner_arrived(zz, along_x):
        first = part if along_x else 0
        block = weights.at[pl.ds(first, part), column(zz, 1 - y, 1 - x)]
        if along_x:
            remote(block, block, fx_s.at[zz], fx_r.at[zz], here).wait_recv()
        else:
            remote(block, block, fy_s.at[zz], fy_r.at[zz], here).wait_recv()

    own_first = [own_w_ref.at[z], weights.at[:, column(z, y, x)]]
    start_x = remote(own_first[0], own_first[1], x_s.at[z], x_r.at[z], x_next)
    start_y = remote(own_first[0], own_first[1], y_s.at[z], y_r.at[z], y_next)
    for k in range(n_a - 1):
        a2a(k).start()
    start_x.start()
    start_y.start()

    keys[pl.ds(WIN, row_count), :] = key_ref[:, head_cols]
    values[pl.ds(WIN, row_count), :] = value_ref[:, head_cols]
    docs[pl.ds(1, blocks)] = docs_ref[...]

    @pl.when(place == 0)
    def _():
        keys[pl.ds(0, WIN), :] = jnp.zeros((WIN, HD), keys.dtype)
        values[pl.ds(0, WIN), :] = jnp.zeros((WIN, HD), values.dtype)
        docs[0] = jnp.full((1, WIN), -1, jnp.int32)

    @pl.when(place == places - 1)
    def _():
        keys[pl.ds(row_count + WIN, WIN), :] = jnp.zeros((WIN, HD), keys.dtype)
        values[pl.ds(row_count + WIN, WIN), :] = jnp.zeros((WIN, HD), values.dtype)
        docs[blocks + 1] = jnp.full((1, WIN), -1, jnp.int32)

    heads_here = query_ref.shape[1] // HD
    row_id = lax.broadcasted_iota(jnp.int32, (WIN, 3 * WIN), 0)
    col_id = lax.broadcasted_iota(jnp.int32, (WIN, 3 * WIN), 1)
    band = (col_id >= row_id) & (col_id <= row_id + 2 * WIN)

    def attend(b):
        mine = jnp.broadcast_to(docs[b + 1], (WIN, WIN)).T
        key_docs = jnp.concatenate([jnp.broadcast_to(docs[b + t], (WIN, WIN)) for t in range(3)], axis=1)
        query_docs = jnp.concatenate([mine] * 3, axis=1)
        allowed = band & (key_docs == query_docs)
        k_block = keys[pl.ds(b * WIN, 3 * WIN), :]
        v_block = values[pl.ds(b * WIN, 3 * WIN), :]
        for h in range(heads_here):
            q = query_ref[pl.ds(b * WIN, WIN), pl.ds(h * HD, HD)]
            scores = lax.dot_general(
                q, k_block, (((1,), (1,)), ((), ())), preferred_element_type=jnp.float32
            ) * HD ** (-0.5)
            masked = jnp.where(allowed, scores, masked_low)
            sink = sink_ref[h]
            peak = jnp.maximum(jnp.max(masked, axis=1, keepdims=True), sink)
            lifted = jnp.where(allowed, jnp.exp(masked - peak), 0.0)
            denom = jnp.sum(lifted, axis=1, keepdims=True) + jnp.exp(sink - peak)
            probs = (lifted / denom).astype(jnp.bfloat16)
            got = jnp.dot(probs, v_block, preferred_element_type=jnp.float32)
            attended[pl.ds(b * WIN, WIN), pl.ds(h * HD, HD)] = got.astype(jnp.bfloat16)

    for b in range(1, blocks - 1):
        attend(b)

    @pl.when(place > 0)
    def _():
        for cp in halo_copies(True):
            cp.wait_recv()

    @pl.when(place < places - 1)
    def _():
        for cp in halo_copies(False):
            cp.wait_recv()

    attend(0)
    attend(blocks - 1)

    mine_rows = pl.ds(pl.multiple_of(c * half, half), half)
    other_rows = pl.ds(pl.multiple_of((1 - c) * half, half), half)
    branch_out[...] = jnp.dot(
        attended[other_rows, :], out_w_ref[...], preferred_element_type=jnp.float32
    ).astype(jnp.bfloat16)
    branch_copy = remote(branch_out, branch_in, br_s, br_r, partner)
    branch_copy.start()
    weights[:, column(z, y, x)] = own_w_ref[z]
    own_branch = jnp.dot(
        attended[mine_rows, :], out_w_ref[...], preferred_element_type=jnp.float32
    ).astype(jnp.bfloat16)
    branch_copy.wait_recv()
    branch = (own_branch.astype(jnp.float32) + branch_in[...].astype(jnp.float32)).astype(jnp.bfloat16)
    carried = (
        stream_ref[mine_rows, :].astype(jnp.float32) + branch.astype(jnp.float32)
    ).astype(jnp.bfloat16)
    carried_keep[...] = carried
    carried_f = carried.astype(jnp.float32)
    normed = (
        carried_f
        * lax.rsqrt(jnp.mean(carried_f * carried_f, axis=1, keepdims=True) + norm_eps)
        * gain_ref[...]
    ).astype(jnp.bfloat16)
    rows[z, mine_rows, :] = normed

    def ag(blk, to):
        block = rows.at[blk, mine_rows]
        if to == "core":
            return remote(block, block, agc_s.at[blk], agc_r.at[blk], partner)
        if to == "fwd":
            return remote(block, block, agf_s.at[blk], agz_r.at[blk], fwd)
        return remote(block, block, agb_s.at[blk], agz_r.at[blk], back)

    def ag_arrived(blk):
        block = rows.at[blk, mine_rows]
        remote(block, block, agf_s.at[blk], agz_r.at[blk], here).wait_recv()

    def ag_core_arrived(blk):
        block = rows.at[blk, other_rows]
        remote(block, block, agc_s.at[blk], agc_r.at[blk], here).wait_recv()

    ag(z, "fwd").start()

    @pl.when(w == 1)
    def _():
        ag(z, "back").start()

    ag(z, "core").start()

    def relay_rows(b_end, b_mid, mid_to):
        @pl.when(w == 0)
        def _():
            ag_arrived(block_at(b_end))
            ag(block_at(b_end), "core").start()

        @pl.when(w == 1)
        def _():
            ag_arrived(block_at(b_mid))
            ag(block_at(b_mid), mid_to).start()
            ag(block_at(b_mid), "core").start()

    def relay_corner(zz):
        side_arrived(zz, True)
        corner(zz, False).start()
        side_arrived(zz, False)
        corner(zz, True).start()

    def relay_side(k):
        a2a_arrived(k)
        side(peers[k], True).start()
        side(peers[k], False).start()

    relay_side(0)
    relay_corner(z)
    relay_side(1)
    relay_corner(peers[0])
    relay_rows(1, 0, "fwd")
    relay_side(2)
    relay_corner(peers[1])
    relay_rows(2, 2, "back")
    relay_corner(peers[2])
    for zz in [z] + peers:
        corner_arrived(zz, True)
        corner_arrived(zz, False)
    relay_rows(3, 3, "back")

    def blk_of(step):
        order = [3 - 3 * hi, 2 - hi, 1 - z + 4 * hi, z]
        if isinstance(step, int):
            return order[step]
        return jnp.where(step == 0, order[0], jnp.where(step == 1, order[1], jnp.where(step == 2, order[2], order[3])))

    dims = (((1,), (1,)), ((), ()))

    def pair(blk):
        return remote(pair_out.at[blk], pair_in.at[blk], pair_s.at[blk], pair_r.at[blk], partner)

    def chain_fwd_copy(step):
        return remote(chain_out.at[step], chain_fwd.at[step], cf_s.at[step], cf_r.at[step], fwd)

    def chain_mid_copy(step):
        return remote(chain_out.at[step], chain_back.at[step], cf_s.at[step], cb_r.at[step], fwd)

    chain_last = remote(chain_out.at[2], chain_back.at[0], cb_s, cb_r.at[0], back)

    def feed_forward(step, _):
        blk = blk_of(step)
        ag_core_arrived(blk)
        x_rows = rows[blk]
        gate_acc = lax.dot_general(x_rows, weights[pl.ds(0, share), :], dims, preferred_element_type=jnp.float32)
        up_acc = lax.dot_general(x_rows, weights[pl.ds(share, share), :], dims, preferred_element_type=jnp.float32)
        hidden = (gate_acc / (1.0 + jnp.exp(-gate_acc)) * up_acc).astype(jnp.bfloat16)
        hidden_keep[...] = hidden
        pair_out[blk] = jnp.dot(
            hidden_keep[other_rows, :], weights[pl.ds(2 * share, share), :], preferred_element_type=jnp.float32
        ).astype(jnp.bfloat16)
        pair(blk).start()
        sum_keep[blk] = jnp.dot(
            hidden_keep[mine_rows, :], weights[pl.ds(2 * share, share), :], preferred_element_type=jnp.float32
        )

        @pl.when((w == 0) & (step < 3))
        def _():
            pair(blk).wait_recv()
            chain_out[step] = (sum_keep[blk] + pair_in[blk].astype(jnp.float32)).astype(jnp.bfloat16)
            chain_fwd_copy(step).start()

        return 0

    lax.fori_loop(0, n_a, feed_forward, 0)

    def chip_sum(blk):
        return sum_keep[blk] + pair_in[blk].astype(jnp.float32)

    def finish(total):
        feed = total.astype(jnp.bfloat16).astype(jnp.float32)
        mixed_ref[mine_rows, :] = (carried_keep[...].astype(jnp.float32) + 0.5 * feed).astype(jnp.bfloat16)

    @pl.when(w == 0)
    def _():
        pair(z).wait_recv()
        chain_last.wait_recv()
        finish(chip_sum(z) + chain_back[0].astype(jnp.float32))

    @pl.when(w == 1)
    def _():
        for step in range(2):
            pair(blk_of(step)).wait_recv()
            chain_fwd_copy(step).wait_recv()
            chain_out[step] = (chip_sum(blk_of(step)) + chain_fwd[step].astype(jnp.float32)).astype(jnp.bfloat16)
            chain_mid_copy(step).start()
        pair(blk_of(2)).wait_recv()
        chain_mid_copy(0).wait_recv()
        chain_out[2] = (chip_sum(blk_of(2)) + chain_back[0].astype(jnp.float32)).astype(jnp.bfloat16)
        chain_last.start()
        pair(z).wait_recv()
        chain_mid_copy(1).wait_recv()
        chain_fwd_copy(2).wait_recv()
        finish(chip_sum(z) + chain_fwd[2].astype(jnp.float32) + chain_back[1].astype(jnp.float32))

    last = remote(mixed_ref.at[mine_rows], mixed_ref.at[mine_rows], fin_s, fin_r, partner)
    last.start()

    @pl.when(place < places - 1)
    def _():
        for cp in halo_copies(True):
            cp.wait_send()

    @pl.when(place > 0)
    def _():
        for cp in halo_copies(False):
            cp.wait_send()

    for k in range(n_a - 1):
        a2a(k).wait_send()
        side(peers[k], True).wait_send()
        side(peers[k], False).wait_send()
    start_x.wait_send()
    start_y.wait_send()
    for zz in [z] + peers:
        corner(zz, True).wait_send()
        corner(zz, False).wait_send()
    branch_copy.wait_send()
    for zz in [z] + peers:
        ag(zz, "core").wait_send()
        pair(zz).wait_send()
    ag(z, "fwd").wait_send()

    @pl.when(w == 0)
    def _():
        for step in range(3):
            chain_fwd_copy(step).wait_send()

    @pl.when(w == 1)
    def _():
        ag(z, "back").wait_send()
        ag(block_at(0), "fwd").wait_send()
        ag(block_at(2), "back").wait_send()
        ag(block_at(3), "back").wait_send()
        for step in range(2):
            chain_mid_copy(step).wait_send()
        chain_last.wait_send()

    last.wait_send()
    remote(mixed_ref.at[other_rows], mixed_ref.at[other_rows], fin_s, fin_r, partner).wait_recv()


def fused_device(
    stream, query_rows, key_rows, value_rows, doc_ids, sink_logit,
    out_weight, norm_gain, gate_weight, up_weight, down_weight,
):
    n_a = lax.axis_size("sa")
    row_count, width = stream.shape
    half = row_count // 2
    hidden_here = gate_weight.shape[1]
    share = hidden_here // n_a
    depth = gate_weight.shape[0]
    own_w = jnp.concatenate(
        [m.reshape(n_a, share, depth) for m in (gate_weight.T, up_weight.T, down_weight)], axis=1
    )
    docs = doc_ids.reshape(row_count // WIN, 1, WIN)
    bf = jnp.bfloat16
    vm = pltpu.VMEM
    dma = pltpu.SemaphoreType.DMA
    wide = row_count + 2 * WIN
    scratch = [
        vm((wide, HD), bf), vm((wide, HD), bf), vm((row_count // WIN + 2, 1, WIN), jnp.int32),
        vm((row_count, query_rows.shape[1]), bf), vm((half, width), bf), vm((half, width), bf),
        vm((half, width), bf), vm((n_a, row_count, width), bf), vm((3 * share, width), bf),
        vm((row_count, share), bf),
        vm((n_a, half, width), jnp.float32), vm((n_a, half, width), bf), vm((n_a, half, width), bf),
        vm((3, half, width), bf), vm((3, half, width), bf), vm((2, half, width), bf),
        dma((6,)), dma((6,)),
        dma((n_a,)), dma((n_a,)), dma((n_a,)), dma((n_a,)), dma((n_a,)), dma((n_a,)),
        dma((n_a,)), dma((n_a,)), dma((n_a,)), dma((n_a,)),
        dma, dma, dma((n_a,)), dma((n_a,)), dma((n_a,)), dma((n_a,)), dma((n_a,)), dma((n_a,)), dma((n_a,)),
        dma((3,)), dma, dma((3,)), dma((2,)), dma, dma,
    ]
    inside = pl.BlockSpec(memory_space=vm)
    return pl.pallas_call(
        fused,
        out_shape=jax.ShapeDtypeStruct((row_count, width), bf),
        in_specs=[inside] * 5 + [pl.BlockSpec(memory_space=pltpu.SMEM)] + [inside] * 3,
        out_specs=inside,
        scratch_shapes=scratch,
        compiler_params=pltpu.CompilerParams(has_side_effects=True, vmem_limit_bytes=67043328),
        name="fused_layer",
    )(stream, query_rows, key_rows, value_rows, docs, sink_logit, out_weight, norm_gain.reshape(1, width), own_w)


def solution(mesh):
    n_sp, n_tp = mesh.shape["sp"], mesh.shape["tp"]
    n_a = 4 if n_sp % 4 == 0 else 1
    n_b = n_sp // n_a
    if n_a == 4 and n_b == 4 and n_tp == KVH:
        fine = Mesh(mesh.devices.reshape(n_a, 2, 2, n_tp), AX)
        sp, body = AX[:3], fused_device
    else:
        fine = Mesh(mesh.devices.reshape(n_a, n_b, n_tp), ("sa", "sb", "tp"))
        sp, body = SP, per_device
    in_specs = (
        P(sp, None),
        P(sp, "tp"),
        P(sp, None),
        P(sp, None),
        P(sp),
        P("tp"),
        P("tp", None),
        P(),
        P(sp, "tp"),
        P(sp, "tp"),
        P("tp", sp),
    )
    return jax.shard_map(body, mesh=fine, in_specs=in_specs, out_specs=P(sp, None), check_vma=False)
```

```python
import jax
import jax.numpy as jnp
from jax import lax
from jax.experimental import pallas as pl
from jax.experimental.pallas import tpu as pltpu
from jax.sharding import Mesh, PartitionSpec as P

HEADS = 8
KVH = 2
HD = 128
WIN = 128

norm_eps = 1e-06
masked_low = -1e30
SP = ("sa", "sb")


def halo(value, width):
    peers = lax.axis_size(SP)
    length = value.shape[0]
    up = [(i, i + 1) for i in range(peers - 1)]
    down = [(j, i) for i, j in up]
    before = lax.ppermute(value[length - width :], SP, up)
    after = lax.ppermute(value[:width], SP, down)
    return jnp.concatenate([before, value, after], axis=0)


def exchange(blocks):
    peers = lax.axis_size("sa")
    here = lax.axis_index("sa")
    got = [lax.dynamic_index_in_dim(blocks, here, 0, keepdims=True)]
    for k in range(1, peers):
        out = lax.dynamic_index_in_dim(blocks, lax.rem(here + k, peers), 0, keepdims=True)
        got.append(lax.ppermute(out, "sa", [(i, (i + k) % peers) for i in range(peers)]))
    ring = got[::-1]
    both = jnp.concatenate(ring + ring, axis=0)
    return lax.dynamic_slice_in_dim(both, peers - 1 - here, peers, 0)


def per_device(
    stream,
    query_rows,
    key_rows,
    value_rows,
    doc_ids,
    sink_logit,
    out_weight,
    norm_gain,
    gate_weight,
    up_weight,
    down_weight,
):
    row_count, width = stream.shape
    n_a, n_b, n_tp = lax.axis_size("sa"), lax.axis_size("sb"), lax.axis_size("tp")
    depth, hidden_here = gate_weight.shape
    share = hidden_here // n_a
    tp_place = lax.axis_index("tp")
    sp_place = lax.axis_index(SP)

    def shares(w):
        return w.reshape(depth, n_a, share).transpose(1, 0, 2)

    gate_up = exchange(jnp.concatenate([shares(gate_weight), shares(up_weight)], axis=2))
    gate_up = gate_up.reshape(n_a * depth, 2 * share)
    gate_up = lax.all_gather(gate_up, "sb", axis=0, tiled=True)
    down_mine = exchange(down_weight.reshape(n_a, share, depth))
    down_mine = down_mine.transpose(0, 2, 1).reshape(n_a * depth, share)

    heads_here = query_rows.shape[1] // HD
    group_share = HEADS // KVH
    groups_here = max(1, heads_here // group_share)
    per_group = heads_here // groups_here
    group_first = tp_place * heads_here // group_share
    keys_here = lax.dynamic_slice_in_dim(key_rows, group_first * HD, groups_here * HD, 1)
    values_here = lax.dynamic_slice_in_dim(value_rows, group_first * HD, groups_here * HD, 1)
    docs_col = jnp.broadcast_to(doc_ids.astype(jnp.bfloat16)[:, None], (row_count, HD))
    packed = halo(jnp.concatenate([keys_here, values_here, docs_col], axis=1), WIN)
    span = groups_here * HD
    keys_wide, values_wide = packed[:, :span], packed[:, span : 2 * span]
    docs_wide = packed[:, 2 * span].astype(jnp.int32)
    seq_offset = sp_place * row_count
    seq_total = row_count * n_a * n_b
    query_pos = seq_offset + jnp.arange(row_count, dtype=jnp.int32)
    key_pos = seq_offset - WIN + jnp.arange(row_count + 2 * WIN, dtype=jnp.int32)
    allowed = (
        (jnp.abs(query_pos[:, None] - key_pos[None, :]) <= WIN)
        & (key_pos[None, :] >= 0)
        & (key_pos[None, :] < seq_total)
        & (doc_ids[:, None] == docs_wide[None, :])
    )
    queries = query_rows.reshape(row_count, groups_here, per_group, HD)
    keys_grid = keys_wide.reshape(row_count + 2 * WIN, groups_here, HD)
    values_grid = values_wide.reshape(row_count + 2 * WIN, groups_here, HD)
    scores = jnp.einsum(
        "qgrd,kgd->grqk", queries, keys_grid, preferred_element_type=jnp.float32
    ) * HD ** (-0.5)
    masked = jnp.where(allowed[None, None], scores, masked_low)
    sinks = sink_logit.reshape(groups_here, per_group, 1, 1)
    peak = jnp.maximum(jnp.max(masked, axis=-1, keepdims=True), sinks)
    lifted = jnp.where(allowed[None, None], jnp.exp(masked - peak), 0.0)
    denom = jnp.sum(lifted, axis=-1, keepdims=True) + jnp.exp(sinks - peak)
    probs = (lifted / denom).astype(jnp.bfloat16)
    attended = jnp.einsum("grqk,kgd->qgrd", probs, values_grid, preferred_element_type=jnp.float32)
    attended = attended.astype(jnp.bfloat16).reshape(row_count, heads_here * HD)
    partial_value = jnp.dot(attended, out_weight, preferred_element_type=jnp.float32)

    rows_mine = row_count // n_tp
    branch = lax.psum_scatter(
        partial_value.astype(jnp.bfloat16), "tp", scatter_dimension=0, tiled=True
    )
    stream_mine = lax.dynamic_slice_in_dim(stream, tp_place * rows_mine, rows_mine, 0)
    carried = (stream_mine.astype(jnp.float32) + branch.astype(jnp.float32)).astype(jnp.bfloat16)
    carried_f = carried.astype(jnp.float32)
    normed = (
        carried_f
        * lax.rsqrt(jnp.mean(carried_f * carried_f, axis=1, keepdims=True) + norm_eps)
        * norm_gain[None, :]
    ).astype(jnp.bfloat16)
    normed = normed.reshape(rows_mine, n_a, n_b, depth).transpose(0, 2, 1, 3).reshape(rows_mine, width)
    rows_all = lax.all_gather(normed, ("sa", "tp"), axis=0, tiled=True)
    down_mine, _ = lax.optimization_barrier((down_mine, normed))
    down_all = lax.all_gather(down_mine, "sb", axis=0, tiled=True)

    gate_acc = jnp.dot(rows_all, gate_up[:, :share], preferred_element_type=jnp.float32)
    up_acc = jnp.dot(rows_all, gate_up[:, share:], preferred_element_type=jnp.float32)
    hidden = (jax.nn.silu(gate_acc) * up_acc).astype(jnp.bfloat16)
    terms = lax.dot_general(
        hidden, down_all, (((1,), (1,)), ((), ())), preferred_element_type=jnp.float32
    )
    feed = lax.psum_scatter(
        terms.astype(jnp.bfloat16), ("sa", "tp"), scatter_dimension=0, tiled=True
    )
    feed = feed.reshape(rows_mine, n_b, n_a, depth).transpose(0, 2, 1, 3).reshape(rows_mine, width)
    mixed = (carried_f + 0.5 * feed.astype(jnp.float32)).astype(jnp.bfloat16)
    return lax.all_gather(mixed, "tp", axis=0, tiled=True)


MESH = pl.DeviceIdType.MESH
AX = ("sa", "sy", "sx", "tp")
CHUNKS = 4
UNITS = 2


def fused(
    stream_hbm, query_hbm, key_hbm, value_hbm, docs_ref, sink_ref, out_w_hbm, gain_ref,
    gate_hbm, up_hbm, down_hbm,
    mixed_ref,
    stream_ref, query_ref, key_ref, value_ref, out_w_ref, gate_ref, up_ref, gate_t, up_t,
    keys, values, docs, attended, branch_out, branch_in, carried_keep, rows, weights,
    sum_keep, pair_out, pair_in, chain_out, chain_fwd, chain_back,
    load_s, halo_s, halo_r, a2a_s, a2a_r, x_s, x_r, y_s, y_r, fx_s, fx_r, fy_s, fy_r,
    br_s, br_r, agf_s, agb_s, agz_r, agc_s, agc_r, pair_s, pair_r,
    cf_s, cl_s, cf_r, cb_r, fin_s, fin_r,
):
    n_a, row_count, width = rows.shape
    n_tp = 2
    z, y, x, c = [lax.axis_index(a) for a in AX]
    place = (z * 2 + y) * 2 + x
    places = n_a * 4
    half = row_count // n_tp
    size = half // CHUNKS
    piece = weights.shape[0]
    share = piece // 3
    part = piece // 2
    depth = gate_hbm.shape[0]
    hi = z // 2
    w = z + hi * (3 - 2 * z)
    here = (z, y, x, c)
    partner = (z, y, x, 1 - c)
    x_next = (z, y, 1 - x, c)
    y_next = (z, 1 - y, x, c)
    fwd = (z + 1 - 2 * hi, y, x, c)
    back = (z - 1 + 2 * hi, y, x, c)
    peers = [z + 1 - 2 * (z % 2), (z + 2) % n_a, n_a - 1 - z]

    def block_at(b):
        return b + hi * (3 - 2 * b)

    def remote(src, dst, s_sem, r_sem, device):
        return pltpu.make_async_remote_copy(
            src_ref=src, dst_ref=dst, send_sem=s_sem, recv_sem=r_sem,
            device_id=device, device_id_type=MESH,
        )

    def at_place(p):
        return (p // 4, (p // 2) % 2, p % 2, c)

    head_cols = pl.ds(pl.multiple_of(c * HD, HD), HD)
    edge = row_count - WIN
    blocks = row_count // WIN

    loads = [
        pltpu.make_async_copy(a, b, load_s.at[i])
        for i, (a, b) in enumerate([
            (key_hbm.at[:, head_cols], key_ref), (value_hbm.at[:, head_cols], value_ref),
            (gate_hbm, gate_ref), (up_hbm, up_ref), (query_hbm, query_ref),
            (out_w_hbm, out_w_ref), (stream_hbm, stream_ref),
        ])
    ]
    for cp in loads:
        cp.start()

    barrier = pltpu.get_barrier_semaphore()
    nearby = [at_place((place + 1) % places), at_place((place + places - 1) % places)]
    for device in [partner, x_next, y_next] + [(p, y, x, c) for p in peers] + nearby:
        pl.semaphore_signal(barrier, inc=1, device_id=device, device_id_type=MESH)
    pl.semaphore_wait(barrier, 8)
    loads[0].wait()
    loads[1].wait()

    def halo_copies(to_next):
        if to_next:
            dev, src, dst, o = at_place(place + 1), edge, 0, 0
        else:
            dev, src, dst, o = at_place(place - 1), 0, row_count + WIN, 3
        src, dst = pl.ds(src, WIN), pl.ds(dst, WIN)
        return [
            remote(key_ref.at[src], keys.at[dst], halo_s.at[o], halo_r.at[o], dev),
            remote(value_ref.at[src], values.at[dst], halo_s.at[o + 1], halo_r.at[o + 1], dev),
            remote(docs_ref.at[:, src], docs.at[:, dst], halo_s.at[o + 2], halo_r.at[o + 2], dev),
        ]

    @pl.when(place < places - 1)
    def _():
        for cp in halo_copies(True):
            cp.start()

    @pl.when(place > 0)
    def _():
        for cp in halo_copies(False):
            cp.start()

    def column(zz, yy, xx):
        return pl.ds(pl.multiple_of(((zz * 2 + yy) * 2 + xx) * depth, depth), depth)

    mine_col = column(z, y, x)

    def own_piece(q, part_id, s_sem, r_sem, device):
        src = (gate_t, up_t, down_hbm)[part_id].at[pl.ds(pl.multiple_of(q * share, 16), share)]
        dst = weights.at[pl.ds(part_id * share, share), mine_col]
        return remote(src, dst, s_sem, r_sem, device)

    def a2a(k, part_id):
        to = peers[k]
        return own_piece(to, part_id, a2a_s.at[to], a2a_r.at[z], (to, y, x, c))

    def own_x(part_id):
        return own_piece(z, part_id, x_s.at[z], x_r.at[z], x_next)

    def own_y(part_id):
        return own_piece(z, part_id, y_s.at[z], y_r.at[z], y_next)

    def wait_bytes(block, s_sem, r_sem):
        return remote(block, block, s_sem, r_sem, here)

    def side(zz, along_x):
        block = weights.at[:, column(zz, y, x)]
        if along_x:
            return remote(block, block, x_s.at[zz], x_r.at[zz], x_next)
        return remote(block, block, y_s.at[zz], y_r.at[zz], y_next)

    def side_arrived(zz, along_x):
        if along_x:
            wait_bytes(weights.at[:, column(zz, y, 1 - x)], x_s.at[zz], x_r.at[zz]).wait_recv()
        else:
            wait_bytes(weights.at[:, column(zz, 1 - y, x)], y_s.at[zz], y_r.at[zz]).wait_recv()

    def corner(zz, along_x):
        if along_x:
            block = weights.at[pl.ds(part, part), column(zz, 1 - y, x)]
            return remote(block, block, fx_s.at[zz], fx_r.at[zz], x_next)
        block = weights.at[pl.ds(0, part), column(zz, y, 1 - x)]
        return remote(block, block, fy_s.at[zz], fy_r.at[zz], y_next)

    def corner_arrived(zz):
        wait_bytes(weights.at[pl.ds(part, part), column(zz, 1 - y, 1 - x)], fx_s.at[zz], fx_r.at[zz]).wait_recv()
        wait_bytes(weights.at[pl.ds(0, part), column(zz, 1 - y, 1 - x)], fy_s.at[zz], fy_r.at[zz]).wait_recv()

    a2a(0, 2).start()
    own_x(2).start()
    own_y(2).start()

    @pl.when(w == 1)
    def _():
        a2a(2, 2).start()

    own_down = pltpu.make_async_copy(
        down_hbm.at[pl.ds(pl.multiple_of(z * share, 16), share)], weights.at[pl.ds(2 * share, share), mine_col], load_s.at[7]
    )
    own_down.start()

    with jax.named_scope("turn"):
        loads[2].wait()
        loads[3].wait()

        def turn(i, _):
            at = pl.ds(pl.multiple_of(i * HD, HD), HD)
            gate_t[at, :] = gate_ref[:, at].T
            up_t[at, :] = up_ref[:, at].T
            return 0

        lax.fori_loop(0, gate_hbm.shape[1] // HD, turn, 0)

    for part_id in range(2):
        a2a(0, part_id).start()
    for part_id in range(2):
        own_x(part_id).start()
        own_y(part_id).start()

    @pl.when(w == 0)
    def _():
        a2a(2, 2).start()

    for part_id in range(2):
        a2a(2, part_id).start()

    def far_send(k):
        for part_id in range(3):
            a2a(k, part_id).start()

    @pl.when(w == 1)
    def _():
        far_send(1)

    own_rows_w = pl.ds(pl.multiple_of(z * share, 16), share)
    weights[pl.ds(0, share), mine_col] = gate_t[own_rows_w, :]
    weights[pl.ds(share, share), mine_col] = up_t[own_rows_w, :]

    keys[pl.ds(WIN, row_count), :] = key_ref[...]
    values[pl.ds(WIN, row_count), :] = value_ref[...]
    docs[:, pl.ds(WIN, row_count)] = docs_ref[...]

    @pl.when(place == 0)
    def _():
        keys[pl.ds(0, WIN), :] = jnp.zeros((WIN, HD), keys.dtype)
        values[pl.ds(0, WIN), :] = jnp.zeros((WIN, HD), values.dtype)
        docs[:, pl.ds(0, WIN)] = jnp.full((1, WIN), -1, jnp.int32)

    @pl.when(place == places - 1)
    def _():
        keys[pl.ds(row_count + WIN, WIN), :] = jnp.zeros((WIN, HD), keys.dtype)
        values[pl.ds(row_count + WIN, WIN), :] = jnp.zeros((WIN, HD), values.dtype)
        docs[:, pl.ds(row_count + WIN, WIN)] = jnp.full((1, WIN), -1, jnp.int32)

    heads_here = query_ref.shape[1] // HD
    row_id = lax.broadcasted_iota(jnp.int32, (WIN, 3 * WIN), 0)
    col_id = lax.broadcasted_iota(jnp.int32, (WIN, 3 * WIN), 1)
    band = (col_id >= row_id) & (col_id <= row_id + 2 * WIN)
    loads[4].wait()

    def attend(b):
        mine = jnp.broadcast_to(docs[:, pl.ds((b + 1) * WIN, WIN)], (WIN, WIN)).T
        key_docs = jnp.broadcast_to(docs[:, pl.ds(b * WIN, 3 * WIN)], (WIN, 3 * WIN))
        query_docs = jnp.concatenate([mine] * 3, axis=1)
        allowed = band & (key_docs == query_docs)
        k_block = keys[pl.ds(b * WIN, 3 * WIN), :]
        v_block = values[pl.ds(b * WIN, 3 * WIN), :]
        for h in range(heads_here):
            q = query_ref[pl.ds(b * WIN, WIN), pl.ds(h * HD, HD)]
            scores = lax.dot_general(
                q, k_block, (((1,), (1,)), ((), ())), preferred_element_type=jnp.float32
            ) * HD ** (-0.5)
            masked = jnp.where(allowed, scores, masked_low)
            sink = sink_ref[h]
            peak = jnp.maximum(jnp.max(masked, axis=1, keepdims=True), sink)
            lifted = jnp.where(allowed, jnp.exp(masked - peak), 0.0)
            denom = jnp.sum(lifted, axis=1, keepdims=True) + jnp.exp(sink - peak)
            probs = (lifted / denom).astype(jnp.bfloat16)
            got = jnp.dot(probs, v_block, preferred_element_type=jnp.float32)
            attended[pl.ds(b * WIN, WIN), pl.ds(h * HD, HD)] = got.astype(jnp.bfloat16)

    with jax.named_scope("attend_mid"):
        for b in range(1, blocks - 1):
            attend(b)

    with jax.named_scope("halo_wait"):

        @pl.when(place > 0)
        def _():
            for cp in halo_copies(True):
                cp.wait_recv()

        @pl.when(place < places - 1)
        def _():
            for cp in halo_copies(False):
                cp.wait_recv()

    with jax.named_scope("attend_edge"):
        attend(0)
        attend(blocks - 1)

    mine_rows = pl.ds(pl.multiple_of(c * half, half), half)
    other_rows = pl.ds(pl.multiple_of((1 - c) * half, half), half)
    loads[5].wait()
    loads[6].wait()
    branch_out[...] = jnp.dot(
        attended[other_rows, :], out_w_ref[...], preferred_element_type=jnp.float32
    ).astype(jnp.bfloat16)
    branch_copy = remote(branch_out, branch_in, br_s, br_r, partner)
    branch_copy.start()
    own_branch = jnp.dot(
        attended[mine_rows, :], out_w_ref[...], preferred_element_type=jnp.float32
    ).astype(jnp.bfloat16)
    own_down.wait()
    with jax.named_scope("branch_wait"):
        branch_copy.wait_recv()
    branch = (own_branch.astype(jnp.float32) + branch_in[...].astype(jnp.float32)).astype(jnp.bfloat16)
    carried = (
        stream_ref[mine_rows, :].astype(jnp.float32) + branch.astype(jnp.float32)
    ).astype(jnp.bfloat16)
    carried_keep[...] = carried
    carried_f = carried.astype(jnp.float32)
    normed = (
        carried_f
        * lax.rsqrt(jnp.mean(carried_f * carried_f, axis=1, keepdims=True) + norm_eps)
        * gain_ref[...]
    ).astype(jnp.bfloat16)
    rows[z, mine_rows, :] = normed

    def chunk_rows(core, j):
        return pl.ds(pl.multiple_of(core * half + j * size, 16), size)

    def ag(blk, j, to):
        block = rows.at[blk, chunk_rows(c, j)]
        if to == "core":
            return remote(block, block, agc_s.at[blk, j], agc_r.at[blk, j], partner)
        if to == "fwd":
            return remote(block, block, agf_s.at[blk, j], agz_r.at[blk, j], fwd)
        return remote(block, block, agb_s.at[blk, j], agz_r.at[blk, j], back)

    def ag_arrived(blk, j):
        wait_bytes(rows.at[blk, chunk_rows(c, j)], agf_s.at[blk, j], agz_r.at[blk, j]).wait_recv()

    def ag_core_arrived(blk, j):
        wait_bytes(rows.at[blk, chunk_rows(1 - c, j)], agc_s.at[blk, j], agc_r.at[blk, j]).wait_recv()

    for j in range(CHUNKS):
        ag(z, j, "fwd").start()

    for j in range(CHUNKS):
        ag(z, j, "core").start()

    def far_sent(k):
        wait_bytes(weights.at[:, mine_col], a2a_s.at[peers[k]], a2a_r.at[peers[k]]).wait_send()

    def rows_back():
        far_sent(1)
        for j in range(CHUNKS):
            ag(z, j, "back").start()

    def relay_rows(b, j, to=None):
        blk = block_at(b)
        ag_arrived(blk, j)
        if to is not None:
            ag(blk, j, to).start()
        ag(blk, j, "core").start()

    def relay_corner(zz):
        side_arrived(zz, True)
        corner(zz, False).start()
        side_arrived(zz, False)
        corner(zz, True).start()

    def relay_side(k):
        frm = peers[k]
        wait_bytes(weights.at[:, column(frm, y, x)], a2a_s.at[frm], a2a_r.at[frm]).wait_recv()
        side(frm, True).start()
        side(frm, False).start()

    def run(plan):
        for name, step, args in plan:
            with jax.named_scope(name):
                step(*args)

    every = range(CHUNKS)

    @pl.when(w == 0)
    def _():
        run(
            [
                ("side0", relay_side, (0,)),
                ("corner_own", relay_corner, (z,)),
                ("corner0", relay_corner, (peers[0],)),
                ("side2", relay_side, (2,)),
                ("side1", relay_side, (1,)),
                ("far", far_send, (1,)),
                ("corner2", relay_corner, (peers[2],)),
            ]
            + [("rows1", relay_rows, (1, j)) for j in every]
            + [
                ("corner1", relay_corner, (peers[1],)),
                ("last_own", corner_arrived, (z,)),
                ("last0", corner_arrived, (peers[0],)),
                ("last2", corner_arrived, (peers[2],)),
                ("last1", corner_arrived, (peers[1],)),
            ]
            + [("rows2", relay_rows, (2, j)) for j in every]
        )

    @pl.when(w == 1)
    def _():
        first, second = every[: CHUNKS // 2], every[CHUNKS // 2 :]
        early = [[("rows0", relay_rows, (0, j, "fwd")), ("rows2", relay_rows, (2, j, "back"))] for j in first]
        later = [[("rows0", relay_rows, (0, j, "fwd")), ("rows2", relay_rows, (2, j, "back"))] for j in second]
        run(
            [
                ("side0", relay_side, (0,)),
                ("corner_own", relay_corner, (z,)),
                ("side2", relay_side, (2,)),
                ("corner0", relay_corner, (peers[0],)),
                ("rows_back", rows_back, ()),
                ("corner2", relay_corner, (peers[2],)),
                ("side1", relay_side, (1,)),
            ]
            + sum(early, [])
            + [("corner1", relay_corner, (peers[1],))]
            + sum(later, [])
            + [
                ("last_own", corner_arrived, (z,)),
                ("last0", corner_arrived, (peers[0],)),
                ("last2", corner_arrived, (peers[2],)),
                ("last1", corner_arrived, (peers[1],)),
            ]
        )

    def blk_of(step):
        b = [2, 0, 1, 3]
        if isinstance(step, int):
            return block_at(b[step])
        return jnp.where(
            step == 0, block_at(b[0]),
            jnp.where(step == 1, block_at(b[1]), jnp.where(step == 2, block_at(b[2]), block_at(b[3]))),
        )

    chain_b = [2, 3, 1]
    dims = (((1,), (1,)), ((), ()))
    unit = half // UNITS
    per_unit = CHUNKS // UNITS

    def unit_rows(u):
        return pl.ds(pl.multiple_of(u * unit, 16), unit)

    def pair(blk, u):
        return remote(
            pair_out.at[blk, unit_rows(u)], pair_in.at[blk, unit_rows(u)], pair_s.at[blk, u], pair_r.at[blk, u], partner
        )

    def chunk(j):
        return pl.ds(pl.multiple_of(j * size, 16), size)

    def chip_sum(blk, j):
        return sum_keep[blk, chunk(j)] + pair_in[blk, chunk(j)].astype(jnp.float32)

    def chain_fwd_copy(slot, j):
        return remote(chain_out.at[slot, chunk(j)], chain_fwd.at[slot, chunk(j)], cf_s.at[slot, j], cf_r.at[slot, j], fwd)

    def chain_mid_copy(slot, j):
        return remote(chain_out.at[slot, chunk(j)], chain_back.at[1 - slot, chunk(j)], cf_s.at[slot, j], cb_r.at[1 - slot, j], fwd)

    def chain_last_copy(j):
        return remote(chain_out.at[2, chunk(j)], chain_back.at[0, chunk(j)], cl_s.at[j], cb_r.at[0, j], back)

    def back_arrived(slot, j):
        wait_bytes(chain_back.at[slot, chunk(j)], cl_s.at[j], cb_r.at[slot, j]).wait_recv()

    def send_end(slot, u):
        blk = block_at(chain_b[slot])
        pair(blk, u).wait_recv()
        for t in range(per_unit):
            j = u * per_unit + t
            chain_out[slot, chunk(j)] = chip_sum(blk, j).astype(jnp.bfloat16)
            chain_fwd_copy(slot, j).start()

    def feed_forward(i, _):
        step = i // UNITS
        u = i % UNITS

        @pl.when((w == 1) & (i < CHUNKS))
        def _():
            relay_rows(3, i, "back")

        @pl.when((w == 0) & (step == n_a - 1))
        def _():
            for t in range(per_unit):
                relay_rows(3, u * per_unit + t)

        blk = blk_of(step)
        for t in range(per_unit):
            ag_core_arrived(blk, u * per_unit + t)
        x_rows = jnp.concatenate(
            [rows[blk, pl.ds(pl.multiple_of(h * half + u * unit, 16), unit)] for h in (1 - c, c)], axis=0
        )
        gate_acc = lax.dot_general(x_rows, weights[pl.ds(0, share), :], dims, preferred_element_type=jnp.float32)
        up_acc = lax.dot_general(x_rows, weights[pl.ds(share, share), :], dims, preferred_element_type=jnp.float32)
        hidden = (gate_acc / (1.0 + jnp.exp(-gate_acc)) * up_acc).astype(jnp.bfloat16)
        out = jnp.dot(hidden, weights[pl.ds(2 * share, share), :], preferred_element_type=jnp.float32)
        pair_out[blk, unit_rows(u)] = out[:unit].astype(jnp.bfloat16)
        pair(blk, u).start()
        sum_keep[blk, unit_rows(u)] = out[unit:]

        @pl.when((w == 0) & (step == 0))
        def _():
            send_end(0, u)

        @pl.when((w == 0) & (step == n_a - 1))
        def _():
            send_end(1, u)

        return 0

    with jax.named_scope("ffn"):
        lax.fori_loop(0, n_a * UNITS, feed_forward, 0)

    def last(core, j):
        block = mixed_ref.at[chunk_rows(core, j)]
        return remote(block, block, fin_s.at[j], fin_r.at[j], partner)

    def finish(j, total):
        feed = total.astype(jnp.bfloat16).astype(jnp.float32)
        mixed_ref[chunk_rows(c, j), :] = (
            carried_keep[chunk(j)].astype(jnp.float32) + 0.5 * feed
        ).astype(jnp.bfloat16)
        last(c, j).start()

    @pl.when(w == 0)
    def _():
        for u in range(UNITS):
            send_end(2, u)
        for u in range(UNITS):
            pair(z, u).wait_recv()
        for j in range(CHUNKS):
            with jax.named_scope(f"fin{j}"):
                back_arrived(0, j)
                finish(j, chip_sum(z, j) + chain_back[0, chunk(j)].astype(jnp.float32))

    @pl.when(w == 1)
    def _():
        for b in range(n_a):
            for u in range(UNITS):
                pair(block_at(b), u).wait_recv()

        def pass_on(slot, j):
            chain_fwd_copy(slot, j).wait_recv()
            total = chip_sum(block_at(chain_b[slot]), j) + chain_fwd[slot, chunk(j)].astype(jnp.float32)
            chain_out[slot, chunk(j)] = total.astype(jnp.bfloat16)
            chain_mid_copy(slot, j).start()

        def pass_back(j):
            back_arrived(0, j)
            total = chip_sum(block_at(0), j) + chain_back[0, chunk(j)].astype(jnp.float32)
            chain_out[2, chunk(j)] = total.astype(jnp.bfloat16)
            chain_last_copy(j).start()

        def close(j):
            back_arrived(1, j)
            chain_fwd_copy(2, j).wait_recv()
            finish(
                j,
                chip_sum(z, j)
                + chain_fwd[2, chunk(j)].astype(jnp.float32)
                + chain_back[1, chunk(j)].astype(jnp.float32),
            )

        plan = [("on0", pass_on, (0, j)) for j in range(CHUNKS)]
        plan += [("on1", pass_on, (1, 0))]
        for j in range(1, CHUNKS):
            plan += [("on1", pass_on, (1, j)), ("pback", pass_back, (j - 1,))]
        plan += [("pback", pass_back, (CHUNKS - 1,))]
        plan += [("close", close, (j,)) for j in range(CHUNKS)]
        run(plan)

    with jax.named_scope("sends_done"):
        @pl.when(place < places - 1)
        def _():
            for cp in halo_copies(True):
                cp.wait_send()

        @pl.when(place > 0)
        def _():
            for cp in halo_copies(False):
                cp.wait_send()

        whole = weights.at[:, mine_col]
        far_sent(0)
        far_sent(2)

        @pl.when(w == 0)
        def _():
            far_sent(1)

        for zz in [z] + peers:
            wait_bytes(whole, x_s.at[zz], x_r.at[zz]).wait_send()
            wait_bytes(whole, y_s.at[zz], y_r.at[zz]).wait_send()
            corner(zz, True).wait_send()
            corner(zz, False).wait_send()
            for u in range(UNITS):
                pair(zz, u).wait_send()
            for j in range(CHUNKS):
                ag(zz, j, "core").wait_send()
        branch_copy.wait_send()
        for j in range(CHUNKS):
            ag(z, j, "fwd").wait_send()

        @pl.when(w == 0)
        def _():
            for slot in range(3):
                for j in range(CHUNKS):
                    chain_fwd_copy(slot, j).wait_send()

        @pl.when(w == 1)
        def _():
            for j in range(CHUNKS):
                ag(z, j, "back").wait_send()
                ag(block_at(0), j, "fwd").wait_send()
                ag(block_at(2), j, "back").wait_send()
                ag(block_at(3), j, "back").wait_send()
                for slot in range(2):
                    chain_mid_copy(slot, j).wait_send()
                chain_last_copy(j).wait_send()

        for j in range(CHUNKS):
            last(c, j).wait_send()
            last(1 - c, j).wait_recv()


def fused_device(
    stream, query_rows, key_rows, value_rows, doc_ids, sink_logit,
    out_weight, norm_gain, gate_weight, up_weight, down_weight,
):
    n_a = lax.axis_size("sa")
    row_count, width = stream.shape
    half = row_count // 2
    depth, hidden_here = gate_weight.shape
    share = hidden_here // n_a
    bf = jnp.bfloat16
    vm = pltpu.VMEM
    dma = pltpu.SemaphoreType.DMA
    wide = row_count + 2 * WIN
    per_block = dma((n_a,))
    per_chunk = dma((n_a, CHUNKS))
    per_unit = dma((n_a, UNITS))
    scratch = [
        vm((row_count, width), bf), vm(query_rows.shape, bf), vm((row_count, HD), bf), vm((row_count, HD), bf),
        vm(out_weight.shape, bf), vm(gate_weight.shape, bf), vm(gate_weight.shape, bf),
        vm((hidden_here, depth), bf), vm((hidden_here, depth), bf),
        vm((wide, HD), bf), vm((wide, HD), bf), vm((1, wide), jnp.int32),
        vm(query_rows.shape, bf), vm((half, width), bf), vm((half, width), bf),
        vm((half, width), bf), vm((n_a, row_count, width), bf), vm((3 * share, width), bf),
        vm((n_a, half, width), jnp.float32), vm((n_a, half, width), bf), vm((n_a, half, width), bf),
        vm((3, half, width), bf), vm((3, half, width), bf), vm((2, half, width), bf),
        dma((8,)), dma((6,)), dma((6,)),
        *([per_block] * 10),
        dma, dma, per_chunk, per_chunk, per_chunk, per_chunk, per_chunk, per_unit, per_unit,
        dma((3, CHUNKS)), dma((CHUNKS,)), dma((3, CHUNKS)), dma((2, CHUNKS)), dma((CHUNKS,)), dma((CHUNKS,)),
    ]
    inside = pl.BlockSpec(memory_space=vm)
    anywhere = pl.BlockSpec(memory_space=pl.ANY)
    return pl.pallas_call(
        fused,
        out_shape=jax.ShapeDtypeStruct((row_count, width), bf),
        in_specs=[anywhere] * 4 + [inside, pl.BlockSpec(memory_space=pltpu.SMEM), anywhere, inside] + [anywhere] * 3,
        out_specs=inside,
        scratch_shapes=scratch,
        compiler_params=pltpu.CompilerParams(collective_id=0, has_side_effects=True, vmem_limit_bytes=56 * 2**20),
        name="fused_layer",
    )(
        stream, query_rows, key_rows, value_rows, doc_ids.reshape(1, row_count), sink_logit, out_weight,
        norm_gain.reshape(1, width), gate_weight, up_weight, down_weight,
    )


def solution(mesh):
    n_sp, n_tp = mesh.shape["sp"], mesh.shape["tp"]
    n_a = 4 if n_sp % 4 == 0 else 1
    n_b = n_sp // n_a
    if n_a == 4 and n_b == 4 and n_tp == KVH:
        fine = Mesh(mesh.devices.reshape(n_a, 2, 2, n_tp), AX)
        sp, body = AX[:3], fused_device
    else:
        fine = Mesh(mesh.devices.reshape(n_a, n_b, n_tp), ("sa", "sb", "tp"))
        sp, body = SP, per_device
    in_specs = (
        P(sp, None),
        P(sp, "tp"),
        P(sp, None),
        P(sp, None),
        P(sp),
        P("tp"),
        P("tp", None),
        P(),
        P(sp, "tp"),
        P(sp, "tp"),
        P("tp", sp),
    )
    return jax.shard_map(body, mesh=fine, in_specs=in_specs, out_specs=P(sp, None), check_vma=False)
```

```python
import jax
import jax.numpy as jnp
from jax import lax
from jax.experimental import pallas as pl
from jax.experimental.pallas import tpu as pltpu
from jax.sharding import Mesh, PartitionSpec as P

HEADS = 8
KVH = 2
HD = 128
WIN = 128

norm_eps = 1e-06
masked_low = -1e30
SP = ("sa", "sb")


def halo(value, width):
    peers = lax.axis_size(SP)
    length = value.shape[0]
    up = [(i, i + 1) for i in range(peers - 1)]
    down = [(j, i) for i, j in up]
    before = lax.ppermute(value[length - width :], SP, up)
    after = lax.ppermute(value[:width], SP, down)
    return jnp.concatenate([before, value, after], axis=0)


def exchange(blocks):
    peers = lax.axis_size("sa")
    here = lax.axis_index("sa")
    got = [lax.dynamic_index_in_dim(blocks, here, 0, keepdims=True)]
    for k in range(1, peers):
        out = lax.dynamic_index_in_dim(blocks, lax.rem(here + k, peers), 0, keepdims=True)
        got.append(lax.ppermute(out, "sa", [(i, (i + k) % peers) for i in range(peers)]))
    ring = got[::-1]
    both = jnp.concatenate(ring + ring, axis=0)
    return lax.dynamic_slice_in_dim(both, peers - 1 - here, peers, 0)


def per_device(
    stream,
    query_rows,
    key_rows,
    value_rows,
    doc_ids,
    sink_logit,
    out_weight,
    norm_gain,
    gate_weight,
    up_weight,
    down_weight,
):
    row_count, width = stream.shape
    n_a, n_b, n_tp = lax.axis_size("sa"), lax.axis_size("sb"), lax.axis_size("tp")
    depth, hidden_here = gate_weight.shape
    share = hidden_here // n_a
    tp_place = lax.axis_index("tp")
    sp_place = lax.axis_index(SP)

    def shares(w):
        return w.reshape(depth, n_a, share).transpose(1, 0, 2)

    gate_up = exchange(jnp.concatenate([shares(gate_weight), shares(up_weight)], axis=2))
    gate_up = gate_up.reshape(n_a * depth, 2 * share)
    gate_up = lax.all_gather(gate_up, "sb", axis=0, tiled=True)
    down_mine = exchange(down_weight.reshape(n_a, share, depth))
    down_mine = down_mine.transpose(0, 2, 1).reshape(n_a * depth, share)

    heads_here = query_rows.shape[1] // HD
    group_share = HEADS // KVH
    groups_here = max(1, heads_here // group_share)
    per_group = heads_here // groups_here
    group_first = tp_place * heads_here // group_share
    keys_here = lax.dynamic_slice_in_dim(key_rows, group_first * HD, groups_here * HD, 1)
    values_here = lax.dynamic_slice_in_dim(value_rows, group_first * HD, groups_here * HD, 1)
    docs_col = jnp.broadcast_to(doc_ids.astype(jnp.bfloat16)[:, None], (row_count, HD))
    packed = halo(jnp.concatenate([keys_here, values_here, docs_col], axis=1), WIN)
    span = groups_here * HD
    keys_wide, values_wide = packed[:, :span], packed[:, span : 2 * span]
    docs_wide = packed[:, 2 * span].astype(jnp.int32)
    seq_offset = sp_place * row_count
    seq_total = row_count * n_a * n_b
    query_pos = seq_offset + jnp.arange(row_count, dtype=jnp.int32)
    key_pos = seq_offset - WIN + jnp.arange(row_count + 2 * WIN, dtype=jnp.int32)
    allowed = (
        (jnp.abs(query_pos[:, None] - key_pos[None, :]) <= WIN)
        & (key_pos[None, :] >= 0)
        & (key_pos[None, :] < seq_total)
        & (doc_ids[:, None] == docs_wide[None, :])
    )
    queries = query_rows.reshape(row_count, groups_here, per_group, HD)
    keys_grid = keys_wide.reshape(row_count + 2 * WIN, groups_here, HD)
    values_grid = values_wide.reshape(row_count + 2 * WIN, groups_here, HD)
    scores = jnp.einsum(
        "qgrd,kgd->grqk", queries, keys_grid, preferred_element_type=jnp.float32
    ) * HD ** (-0.5)
    masked = jnp.where(allowed[None, None], scores, masked_low)
    sinks = sink_logit.reshape(groups_here, per_group, 1, 1)
    peak = jnp.maximum(jnp.max(masked, axis=-1, keepdims=True), sinks)
    lifted = jnp.where(allowed[None, None], jnp.exp(masked - peak), 0.0)
    denom = jnp.sum(lifted, axis=-1, keepdims=True) + jnp.exp(sinks - peak)
    probs = (lifted / denom).astype(jnp.bfloat16)
    attended = jnp.einsum("grqk,kgd->qgrd", probs, values_grid, preferred_element_type=jnp.float32)
    attended = attended.astype(jnp.bfloat16).reshape(row_count, heads_here * HD)
    partial_value = jnp.dot(attended, out_weight, preferred_element_type=jnp.float32)

    rows_mine = row_count // n_tp
    branch = lax.psum_scatter(
        partial_value.astype(jnp.bfloat16), "tp", scatter_dimension=0, tiled=True
    )
    stream_mine = lax.dynamic_slice_in_dim(stream, tp_place * rows_mine, rows_mine, 0)
    carried = (stream_mine.astype(jnp.float32) + branch.astype(jnp.float32)).astype(jnp.bfloat16)
    carried_f = carried.astype(jnp.float32)
    normed = (
        carried_f
        * lax.rsqrt(jnp.mean(carried_f * carried_f, axis=1, keepdims=True) + norm_eps)
        * norm_gain[None, :]
    ).astype(jnp.bfloat16)
    normed = normed.reshape(rows_mine, n_a, n_b, depth).transpose(0, 2, 1, 3).reshape(rows_mine, width)
    rows_all = lax.all_gather(normed, ("sa", "tp"), axis=0, tiled=True)
    down_mine, _ = lax.optimization_barrier((down_mine, normed))
    down_all = lax.all_gather(down_mine, "sb", axis=0, tiled=True)

    gate_acc = jnp.dot(rows_all, gate_up[:, :share], preferred_element_type=jnp.float32)
    up_acc = jnp.dot(rows_all, gate_up[:, share:], preferred_element_type=jnp.float32)
    hidden = (jax.nn.silu(gate_acc) * up_acc).astype(jnp.bfloat16)
    terms = lax.dot_general(
        hidden, down_all, (((1,), (1,)), ((), ())), preferred_element_type=jnp.float32
    )
    feed = lax.psum_scatter(
        terms.astype(jnp.bfloat16), ("sa", "tp"), scatter_dimension=0, tiled=True
    )
    feed = feed.reshape(rows_mine, n_b, n_a, depth).transpose(0, 2, 1, 3).reshape(rows_mine, width)
    mixed = (carried_f + 0.5 * feed.astype(jnp.float32)).astype(jnp.bfloat16)
    return lax.all_gather(mixed, "tp", axis=0, tiled=True)


MESH = pl.DeviceIdType.MESH
AX = ("sa", "sy", "sx", "tp")
CHUNKS = 4
UNITS = 2


def fused(
    stream_hbm, query_hbm, key_hbm, value_hbm, docs_ref, sink_ref, out_w_hbm, gain_ref,
    gate_hbm, up_hbm, down_hbm,
    mixed_ref,
    stream_ref, query_ref, key_ref, value_ref, out_w_ref, gate_ref, up_ref, gate_t, up_t,
    keys, values, docs, attended, branch_out, branch_in, carried_keep, rows, weights,
    sum_keep, pair_out, pair_in, chain_out, chain_fwd, chain_back,
    load_s, halo_s, halo_r, a2a_s, a2a_r, x_s, x_r, y_s, y_r, fx_s, fx_r, fy_s, fy_r,
    br_s, br_r, agf_s, agb_s, agz_r, agc_s, agc_r, pair_s, pair_r,
    cf_s, cl_s, cf_r, cb_r, fin_s, fin_r,
):
    n_a, row_count, width = rows.shape
    n_tp = 2
    z, y, x, c = [lax.axis_index(a) for a in AX]
    place = (z * 2 + y) * 2 + x
    places = n_a * 4
    half = row_count // n_tp
    size = half // CHUNKS
    piece = weights.shape[0]
    share = piece // 3
    part = piece // 2
    depth = gate_hbm.shape[0]
    hi = z // 2
    w = z + hi * (3 - 2 * z)
    here = (z, y, x, c)
    partner = (z, y, x, 1 - c)
    x_next = (z, y, 1 - x, c)
    y_next = (z, 1 - y, x, c)
    fwd = (z + 1 - 2 * hi, y, x, c)
    back = (z - 1 + 2 * hi, y, x, c)
    peers = [z + 1 - 2 * (z % 2), (z + 2) % n_a, n_a - 1 - z]

    def block_at(b):
        return b + hi * (3 - 2 * b)

    def remote(src, dst, s_sem, r_sem, device):
        return pltpu.make_async_remote_copy(
            src_ref=src, dst_ref=dst, send_sem=s_sem, recv_sem=r_sem,
            device_id=device, device_id_type=MESH,
        )

    def at_place(p):
        return (p // 4, (p // 2) % 2, p % 2, c)

    head_cols = pl.ds(pl.multiple_of(c * HD, HD), HD)
    edge = row_count - WIN
    blocks = row_count // WIN

    loads = [
        pltpu.make_async_copy(a, b, load_s.at[i])
        for i, (a, b) in enumerate([
            (key_hbm.at[:, head_cols], key_ref), (value_hbm.at[:, head_cols], value_ref),
            (gate_hbm, gate_ref), (up_hbm, up_ref), (query_hbm, query_ref),
            (out_w_hbm, out_w_ref), (stream_hbm, stream_ref),
        ])
    ]
    for cp in loads:
        cp.start()

    barrier = pltpu.get_barrier_semaphore()
    nearby = [at_place((place + 1) % places), at_place((place + places - 1) % places)]
    for device in [partner, x_next, y_next] + [(p, y, x, c) for p in peers] + nearby:
        pl.semaphore_signal(barrier, inc=1, device_id=device, device_id_type=MESH)
    pl.semaphore_wait(barrier, 8)
    loads[0].wait()
    loads[1].wait()

    def halo_copies(to_next):
        if to_next:
            dev, src, dst, o = at_place(place + 1), edge, 0, 0
        else:
            dev, src, dst, o = at_place(place - 1), 0, row_count + WIN, 3
        src, dst = pl.ds(src, WIN), pl.ds(dst, WIN)
        return [
            remote(key_ref.at[src], keys.at[dst], halo_s.at[o], halo_r.at[o], dev),
            remote(value_ref.at[src], values.at[dst], halo_s.at[o + 1], halo_r.at[o + 1], dev),
            remote(docs_ref.at[src], docs.at[dst], halo_s.at[o + 2], halo_r.at[o + 2], dev),
        ]

    @pl.when(place < places - 1)
    def _():
        for cp in halo_copies(True):
            cp.start()

    @pl.when(place > 0)
    def _():
        for cp in halo_copies(False):
            cp.start()

    def column(zz, yy, xx):
        return pl.ds(pl.multiple_of(((zz * 2 + yy) * 2 + xx) * depth, depth), depth)

    mine_col = column(z, y, x)

    def own_piece(q, part_id, s_sem, r_sem, device):
        src = (gate_t, up_t, down_hbm)[part_id].at[pl.ds(pl.multiple_of(q * share, 16), share)]
        dst = weights.at[pl.ds(part_id * share, share), mine_col]
        return remote(src, dst, s_sem, r_sem, device)

    def a2a(k, part_id):
        to = peers[k]
        return own_piece(to, part_id, a2a_s.at[to], a2a_r.at[z], (to, y, x, c))

    def own_x(part_id):
        return own_piece(z, part_id, x_s.at[z], x_r.at[z], x_next)

    def own_y(part_id):
        return own_piece(z, part_id, y_s.at[z], y_r.at[z], y_next)

    def wait_bytes(block, s_sem, r_sem):
        return remote(block, block, s_sem, r_sem, here)

    def side(zz, along_x):
        block = weights.at[:, column(zz, y, x)]
        if along_x:
            return remote(block, block, x_s.at[zz], x_r.at[zz], x_next)
        return remote(block, block, y_s.at[zz], y_r.at[zz], y_next)

    def side_arrived(zz, along_x):
        if along_x:
            wait_bytes(weights.at[:, column(zz, y, 1 - x)], x_s.at[zz], x_r.at[zz]).wait_recv()
        else:
            wait_bytes(weights.at[:, column(zz, 1 - y, x)], y_s.at[zz], y_r.at[zz]).wait_recv()

    def corner(zz, along_x):
        if along_x:
            block = weights.at[pl.ds(part, part), column(zz, 1 - y, x)]
            return remote(block, block, fx_s.at[zz], fx_r.at[zz], x_next)
        block = weights.at[pl.ds(0, part), column(zz, y, 1 - x)]
        return remote(block, block, fy_s.at[zz], fy_r.at[zz], y_next)

    def corner_arrived(zz):
        wait_bytes(weights.at[pl.ds(part, part), column(zz, 1 - y, 1 - x)], fx_s.at[zz], fx_r.at[zz]).wait_recv()
        wait_bytes(weights.at[pl.ds(0, part), column(zz, 1 - y, 1 - x)], fy_s.at[zz], fy_r.at[zz]).wait_recv()

    a2a(0, 2).start()
    own_x(2).start()
    own_y(2).start()

    @pl.when(w == 1)
    def _():
        a2a(2, 2).start()

    own_down = pltpu.make_async_copy(
        down_hbm.at[pl.ds(pl.multiple_of(z * share, 16), share)], weights.at[pl.ds(2 * share, share), mine_col], load_s.at[7]
    )
    own_down.start()

    with jax.named_scope("turn"):
        loads[2].wait()
        loads[3].wait()

        def turn(i, _):
            at = pl.ds(pl.multiple_of(i * HD, HD), HD)
            gate_t[at, :] = gate_ref[:, at].T
            up_t[at, :] = up_ref[:, at].T
            return 0

        lax.fori_loop(0, gate_hbm.shape[1] // HD, turn, 0)

    for part_id in range(2):
        a2a(0, part_id).start()

    @pl.when(w == 1)
    def _():
        for part_id in range(2):
            a2a(2, part_id).start()

    for part_id in range(2):
        own_x(part_id).start()
        own_y(part_id).start()

    def far_send(k):
        for part_id in range(3):
            a2a(k, part_id).start()

    own_rows_w = pl.ds(pl.multiple_of(z * share, 16), share)
    weights[pl.ds(0, share), mine_col] = gate_t[own_rows_w, :]
    weights[pl.ds(share, share), mine_col] = up_t[own_rows_w, :]

    keys[pl.ds(WIN, row_count), :] = key_ref[...]
    values[pl.ds(WIN, row_count), :] = value_ref[...]
    docs[pl.ds(WIN, row_count)] = docs_ref[...]

    @pl.when(place == 0)
    def _():
        keys[pl.ds(0, WIN), :] = jnp.zeros((WIN, HD), keys.dtype)
        values[pl.ds(0, WIN), :] = jnp.zeros((WIN, HD), values.dtype)
        docs[pl.ds(0, WIN)] = jnp.full((WIN,), -1, jnp.int32)

    @pl.when(place == places - 1)
    def _():
        keys[pl.ds(row_count + WIN, WIN), :] = jnp.zeros((WIN, HD), keys.dtype)
        values[pl.ds(row_count + WIN, WIN), :] = jnp.zeros((WIN, HD), values.dtype)
        docs[pl.ds(row_count + WIN, WIN)] = jnp.full((WIN,), -1, jnp.int32)

    heads_here = query_ref.shape[1] // HD
    row_id = lax.broadcasted_iota(jnp.int32, (WIN, 3 * WIN), 0)
    col_id = lax.broadcasted_iota(jnp.int32, (WIN, 3 * WIN), 1)
    band = (col_id >= row_id) & (col_id <= row_id + 2 * WIN)
    loads[4].wait()

    def attend(b):
        mine = jnp.broadcast_to(docs[pl.ds((b + 1) * WIN, WIN)].reshape(1, WIN), (WIN, WIN)).T
        key_docs = jnp.broadcast_to(docs[pl.ds(b * WIN, 3 * WIN)].reshape(1, 3 * WIN), (WIN, 3 * WIN))
        query_docs = jnp.concatenate([mine] * 3, axis=1)
        allowed = band & (key_docs == query_docs)
        k_block = keys[pl.ds(b * WIN, 3 * WIN), :]
        v_block = values[pl.ds(b * WIN, 3 * WIN), :]
        for h in range(heads_here):
            q = query_ref[pl.ds(b * WIN, WIN), pl.ds(h * HD, HD)]
            scores = lax.dot_general(
                q, k_block, (((1,), (1,)), ((), ())), preferred_element_type=jnp.float32
            ) * HD ** (-0.5)
            masked = jnp.where(allowed, scores, masked_low)
            sink = sink_ref[h]
            peak = jnp.maximum(jnp.max(masked, axis=1, keepdims=True), sink)
            lifted = jnp.where(allowed, jnp.exp(masked - peak), 0.0)
            denom = jnp.sum(lifted, axis=1, keepdims=True) + jnp.exp(sink - peak)
            probs = (lifted / denom).astype(jnp.bfloat16)
            got = jnp.dot(probs, v_block, preferred_element_type=jnp.float32)
            attended[pl.ds(b * WIN, WIN), pl.ds(h * HD, HD)] = got.astype(jnp.bfloat16)

    with jax.named_scope("attend_mid"):
        for b in range(1, blocks - 1):
            attend(b)

    with jax.named_scope("halo_wait"):

        @pl.when(place > 0)
        def _():
            for cp in halo_copies(True):
                cp.wait_recv()

        @pl.when(place < places - 1)
        def _():
            for cp in halo_copies(False):
                cp.wait_recv()

    with jax.named_scope("attend_edge"):
        attend(0)
        attend(blocks - 1)

    mine_rows = pl.ds(pl.multiple_of(c * half, half), half)
    other_rows = pl.ds(pl.multiple_of((1 - c) * half, half), half)
    loads[5].wait()
    loads[6].wait()
    branch_out[...] = jnp.dot(
        attended[other_rows, :], out_w_ref[...], preferred_element_type=jnp.float32
    ).astype(jnp.bfloat16)
    branch_copy = remote(branch_out, branch_in, br_s, br_r, partner)
    branch_copy.start()
    own_branch = jnp.dot(
        attended[mine_rows, :], out_w_ref[...], preferred_element_type=jnp.float32
    ).astype(jnp.bfloat16)
    own_down.wait()
    with jax.named_scope("branch_wait"):
        branch_copy.wait_recv()
    branch = (own_branch.astype(jnp.float32) + branch_in[...].astype(jnp.float32)).astype(jnp.bfloat16)
    carried = (
        stream_ref[mine_rows, :].astype(jnp.float32) + branch.astype(jnp.float32)
    ).astype(jnp.bfloat16)
    carried_keep[...] = carried
    carried_f = carried.astype(jnp.float32)
    normed = (
        carried_f
        * lax.rsqrt(jnp.mean(carried_f * carried_f, axis=1, keepdims=True) + norm_eps)
        * gain_ref[...]
    ).astype(jnp.bfloat16)
    rows[z, mine_rows, :] = normed

    def chunk_rows(core, j):
        return pl.ds(pl.multiple_of(core * half + j * size, 16), size)

    def ag(blk, j, to):
        block = rows.at[blk, chunk_rows(c, j)]
        if to == "core":
            return remote(block, block, agc_s.at[blk, j], agc_r.at[blk, j], partner)
        if to == "fwd":
            return remote(block, block, agf_s.at[blk, j], agz_r.at[blk, j], fwd)
        return remote(block, block, agb_s.at[blk, j], agz_r.at[blk, j], back)

    def ag_arrived(blk, j):
        wait_bytes(rows.at[blk, chunk_rows(c, j)], agf_s.at[blk, j], agz_r.at[blk, j]).wait_recv()

    def ag_core_arrived(blk, j):
        wait_bytes(rows.at[blk, chunk_rows(1 - c, j)], agc_s.at[blk, j], agc_r.at[blk, j]).wait_recv()

    for j in range(CHUNKS):
        ag(z, j, "core").start()

    def rows_fwd():
        for j in range(CHUNKS):
            ag(z, j, "fwd").start()

    def far_sent(k):
        wait_bytes(weights.at[:, mine_col], a2a_s.at[peers[k]], a2a_r.at[peers[k]]).wait_send()

    def rows_back():
        far_sent(1)
        for j in range(CHUNKS):
            ag(z, j, "back").start()

    def relay_rows(b, j, to=None):
        blk = block_at(b)
        ag_arrived(blk, j)
        if to is not None:
            ag(blk, j, to).start()
        ag(blk, j, "core").start()

    def relay_corner(zz):
        side_arrived(zz, True)
        corner(zz, False).start()
        side_arrived(zz, False)
        corner(zz, True).start()

    def relay_side(k):
        frm = peers[k]
        wait_bytes(weights.at[:, column(frm, y, x)], a2a_s.at[frm], a2a_r.at[frm]).wait_recv()
        side(frm, True).start()
        side(frm, False).start()

    def run(plan):
        for name, step, args in plan:
            with jax.named_scope(name):
                step(*args)

    every = range(CHUNKS)

    @pl.when(w == 0)
    def _():
        run(
            [
                ("side0", relay_side, (0,)),
                ("far", far_send, (2,)),
                ("rows_fwd", rows_fwd, ()),
                ("corner_own", relay_corner, (z,)),
                ("corner0", relay_corner, (peers[0],)),
                ("side2", relay_side, (2,)),
                ("side1", relay_side, (1,)),
                ("far", far_send, (1,)),
                ("corner2", relay_corner, (peers[2],)),
            ]
            + [("rows1", relay_rows, (1, j)) for j in every]
            + [
                ("corner1", relay_corner, (peers[1],)),
                ("last_own", corner_arrived, (z,)),
                ("last0", corner_arrived, (peers[0],)),
                ("last2", corner_arrived, (peers[2],)),
                ("last1", corner_arrived, (peers[1],)),
            ]
            + [("rows2", relay_rows, (2, j)) for j in every]
        )

    @pl.when(w == 1)
    def _():
        both = [[("rows0", relay_rows, (0, j, "fwd")), ("rows2", relay_rows, (2, j, "back"))] for j in every]
        run(
            [
                ("side0", relay_side, (0,)),
                ("far", far_send, (1,)),
                ("rows_fwd", rows_fwd, ()),
                ("corner_own", relay_corner, (z,)),
                ("side2", relay_side, (2,)),
                ("corner0", relay_corner, (peers[0],)),
                ("rows_back", rows_back, ()),
                ("corner2", relay_corner, (peers[2],)),
                ("side1", relay_side, (1,)),
            ]
            + sum(both, [])
            + [
                ("corner1", relay_corner, (peers[1],)),
                ("last_own", corner_arrived, (z,)),
                ("last0", corner_arrived, (peers[0],)),
                ("last2", corner_arrived, (peers[2],)),
                ("last1", corner_arrived, (peers[1],)),
            ]
        )

    def blk_of(step):
        late = jnp.where(step == 2, block_at(3 - 2 * w), block_at(1 + 2 * w))
        return jnp.where(step == 0, block_at(2), jnp.where(step == 1, block_at(0), late))

    chain_b = [2, 3, 1]
    dims = (((1,), (1,)), ((), ()))
    unit = half // UNITS
    per_unit = CHUNKS // UNITS

    def unit_rows(u):
        return pl.ds(pl.multiple_of(u * unit, 16), unit)

    def pair(blk, u):
        return remote(
            pair_out.at[blk, unit_rows(u)], pair_in.at[blk, unit_rows(u)], pair_s.at[blk, u], pair_r.at[blk, u], partner
        )

    def chunk(j):
        return pl.ds(pl.multiple_of(j * size, 16), size)

    def chip_sum(blk, j):
        return sum_keep[blk, chunk(j)] + pair_in[blk, chunk(j)].astype(jnp.float32)

    def chain_fwd_copy(slot, j):
        return remote(chain_out.at[slot, chunk(j)], chain_fwd.at[slot, chunk(j)], cf_s.at[slot, j], cf_r.at[slot, j], fwd)

    def chain_mid_copy(slot, j):
        return remote(chain_out.at[slot, chunk(j)], chain_back.at[1 - slot, chunk(j)], cf_s.at[slot, j], cb_r.at[1 - slot, j], fwd)

    def chain_last_copy(j):
        return remote(chain_out.at[2, chunk(j)], chain_back.at[0, chunk(j)], cl_s.at[j], cb_r.at[0, j], back)

    def back_arrived(slot, j):
        wait_bytes(chain_back.at[slot, chunk(j)], cl_s.at[j], cb_r.at[slot, j]).wait_recv()

    def send_end(slot, u):
        blk = block_at(chain_b[slot])
        pair(blk, u).wait_recv()
        for t in range(per_unit):
            j = u * per_unit + t
            chain_out[slot, chunk(j)] = chip_sum(blk, j).astype(jnp.bfloat16)
            chain_fwd_copy(slot, j).start()

    def pass_on(slot, j):
        chain_fwd_copy(slot, j).wait_recv()
        total = chip_sum(block_at(chain_b[slot]), j) + chain_fwd[slot, chunk(j)].astype(jnp.float32)
        chain_out[slot, chunk(j)] = total.astype(jnp.bfloat16)
        chain_mid_copy(slot, j).start()

    def feed_forward(i, _):
        step = i // UNITS
        u = i % UNITS

        @pl.when((w == 1) & (i >= 1) & (i <= CHUNKS))
        def _():
            relay_rows(3, i - 1, "back")

        @pl.when((w == 1) & (i > CHUNKS))
        def _():
            @pl.when(i == CHUNKS + 1)
            def _():
                for v in range(UNITS):
                    pair(block_at(2), v).wait_recv()

            pass_on(0, i - CHUNKS - 1)

        @pl.when((w == 0) & (step == 2))
        def _():
            for t in range(per_unit):
                relay_rows(3, u * per_unit + t)

        blk = blk_of(step)
        for t in range(per_unit):
            ag_core_arrived(blk, u * per_unit + t)
        x_rows = jnp.concatenate(
            [rows[blk, pl.ds(pl.multiple_of(h * half + u * unit, 16), unit)] for h in (1 - c, c)], axis=0
        )
        gate_acc = lax.dot_general(x_rows, weights[pl.ds(0, share), :], dims, preferred_element_type=jnp.float32)
        up_acc = lax.dot_general(x_rows, weights[pl.ds(share, share), :], dims, preferred_element_type=jnp.float32)
        hidden = (gate_acc / (1.0 + jnp.exp(-gate_acc)) * up_acc).astype(jnp.bfloat16)
        out = jnp.dot(hidden, weights[pl.ds(2 * share, share), :], preferred_element_type=jnp.float32)
        pair_out[blk, unit_rows(u)] = out[:unit].astype(jnp.bfloat16)
        pair(blk, u).start()
        sum_keep[blk, unit_rows(u)] = out[unit:]

        @pl.when((w == 0) & (step == 0))
        def _():
            send_end(0, u)

        @pl.when((w == 0) & (step == 2))
        def _():
            send_end(1, u)

        @pl.when((w == 0) & (step == 3))
        def _():
            send_end(2, u)

        return 0

    with jax.named_scope("ffn"):
        lax.fori_loop(0, n_a * UNITS, feed_forward, 0)

    def last(core, j):
        block = mixed_ref.at[chunk_rows(core, j)]
        return remote(block, block, fin_s.at[j], fin_r.at[j], partner)

    def finish(j, total):
        feed = total.astype(jnp.bfloat16).astype(jnp.float32)
        mixed_ref[chunk_rows(c, j), :] = (
            carried_keep[chunk(j)].astype(jnp.float32) + 0.5 * feed
        ).astype(jnp.bfloat16)
        last(c, j).start()

    @pl.when(w == 0)
    def _():
        for u in range(UNITS):
            pair(z, u).wait_recv()
        for j in range(CHUNKS):
            with jax.named_scope(f"fin{j}"):
                back_arrived(0, j)
                finish(j, chip_sum(z, j) + chain_back[0, chunk(j)].astype(jnp.float32))

    @pl.when(w == 1)
    def _():
        for b in (3, 0, 1):
            for u in range(UNITS):
                pair(block_at(b), u).wait_recv()

        def pass_back(j):
            back_arrived(0, j)
            total = chip_sum(block_at(0), j) + chain_back[0, chunk(j)].astype(jnp.float32)
            chain_out[2, chunk(j)] = total.astype(jnp.bfloat16)
            chain_last_copy(j).start()

        def close(j):
            back_arrived(1, j)
            chain_fwd_copy(2, j).wait_recv()
            finish(
                j,
                chip_sum(z, j)
                + chain_fwd[2, chunk(j)].astype(jnp.float32)
                + chain_back[1, chunk(j)].astype(jnp.float32),
            )

        plan = [("on0", pass_on, (0, j)) for j in range(n_a * UNITS - CHUNKS - 1, CHUNKS)]
        plan += [("on1", pass_on, (1, 0))]
        for j in range(1, CHUNKS):
            plan += [("on1", pass_on, (1, j)), ("pback", pass_back, (j - 1,))]
        plan += [("pback", pass_back, (CHUNKS - 1,))]
        plan += [("close", close, (j,)) for j in range(CHUNKS)]
        run(plan)

    with jax.named_scope("sends_done"):
        @pl.when(place < places - 1)
        def _():
            for cp in halo_copies(True):
                cp.wait_send()

        @pl.when(place > 0)
        def _():
            for cp in halo_copies(False):
                cp.wait_send()

        whole = weights.at[:, mine_col]
        far_sent(0)
        far_sent(2)

        @pl.when(w == 0)
        def _():
            far_sent(1)

        for zz in [z] + peers:
            wait_bytes(whole, x_s.at[zz], x_r.at[zz]).wait_send()
            wait_bytes(whole, y_s.at[zz], y_r.at[zz]).wait_send()
            corner(zz, True).wait_send()
            corner(zz, False).wait_send()
            for u in range(UNITS):
                pair(zz, u).wait_send()
            for j in range(CHUNKS):
                ag(zz, j, "core").wait_send()
        branch_copy.wait_send()
        for j in range(CHUNKS):
            ag(z, j, "fwd").wait_send()

        @pl.when(w == 0)
        def _():
            for slot in range(3):
                for j in range(CHUNKS):
                    chain_fwd_copy(slot, j).wait_send()

        @pl.when(w == 1)
        def _():
            for j in range(CHUNKS):
                ag(z, j, "back").wait_send()
                ag(block_at(0), j, "fwd").wait_send()
                ag(block_at(2), j, "back").wait_send()
                ag(block_at(3), j, "back").wait_send()
                for slot in range(2):
                    chain_mid_copy(slot, j).wait_send()
                chain_last_copy(j).wait_send()

        for j in range(CHUNKS):
            last(c, j).wait_send()
            last(1 - c, j).wait_recv()


def fused_device(
    stream, query_rows, key_rows, value_rows, doc_ids, sink_logit,
    out_weight, norm_gain, gate_weight, up_weight, down_weight,
):
    n_a = lax.axis_size("sa")
    row_count, width = stream.shape
    half = row_count // 2
    depth, hidden_here = gate_weight.shape
    share = hidden_here // n_a
    bf = jnp.bfloat16
    vm = pltpu.VMEM
    dma = pltpu.SemaphoreType.DMA
    wide = row_count + 2 * WIN
    per_block = dma((n_a,))
    per_chunk = dma((n_a, CHUNKS))
    per_unit = dma((n_a, UNITS))
    scratch = [
        vm((row_count, width), bf), vm(query_rows.shape, bf), vm((row_count, HD), bf), vm((row_count, HD), bf),
        vm(out_weight.shape, bf), vm(gate_weight.shape, bf), vm(gate_weight.shape, bf),
        vm((hidden_here, depth), bf), vm((hidden_here, depth), bf),
        vm((wide, HD), bf), vm((wide, HD), bf), vm((wide,), jnp.int32),
        vm(query_rows.shape, bf), vm((half, width), bf), vm((half, width), bf),
        vm((half, width), bf), vm((n_a, row_count, width), bf), vm((3 * share, width), bf),
        vm((n_a, half, width), jnp.float32), vm((n_a, half, width), bf), vm((n_a, half, width), bf),
        vm((3, half, width), bf), vm((3, half, width), bf), vm((2, half, width), bf),
        dma((8,)), dma((6,)), dma((6,)),
        *([per_block] * 10),
        dma, dma, per_chunk, per_chunk, per_chunk, per_chunk, per_chunk, per_unit, per_unit,
        dma((3, CHUNKS)), dma((CHUNKS,)), dma((3, CHUNKS)), dma((2, CHUNKS)), dma((CHUNKS,)), dma((CHUNKS,)),
    ]
    inside = pl.BlockSpec(memory_space=vm)
    anywhere = pl.BlockSpec(memory_space=pl.ANY)
    return pl.pallas_call(
        fused,
        out_shape=vm((row_count, width), bf),
        in_specs=[anywhere] * 4 + [inside, pl.BlockSpec(memory_space=pltpu.SMEM), anywhere, inside] + [anywhere] * 3,
        out_specs=inside,
        scratch_shapes=scratch,
        compiler_params=pltpu.CompilerParams(collective_id=0, has_side_effects=True, vmem_limit_bytes=56 * 2**20),
        name="fused_layer",
    )(
        stream, query_rows, key_rows, value_rows, doc_ids, sink_logit, out_weight,
        norm_gain.reshape(1, width), gate_weight, up_weight, down_weight,
    )


def solution(mesh):
    n_sp, n_tp = mesh.shape["sp"], mesh.shape["tp"]
    n_a = 4 if n_sp % 4 == 0 else 1
    n_b = n_sp // n_a
    if n_a == 4 and n_b == 4 and n_tp == KVH:
        fine = Mesh(mesh.devices.reshape(n_a, 2, 2, n_tp), AX)
        sp, body = AX[:3], fused_device
    else:
        fine = Mesh(mesh.devices.reshape(n_a, n_b, n_tp), ("sa", "sb", "tp"))
        sp, body = SP, per_device
    in_specs = (
        P(sp, None),
        P(sp, "tp"),
        P(sp, None),
        P(sp, None),
        P(sp),
        P("tp"),
        P("tp", None),
        P(),
        P(sp, "tp"),
        P(sp, "tp"),
        P("tp", sp),
    )
    return jax.shard_map(body, mesh=fine, in_specs=in_specs, out_specs=P(sp, None), check_vma=False)
```

```python
import jax
import jax.numpy as jnp
from jax import lax
from jax.experimental import pallas as pl
from jax.experimental.pallas import tpu as pltpu
from jax.sharding import Mesh, PartitionSpec as P

HEADS = 8
KVH = 2
HD = 128
WIN = 128

norm_eps = 1e-06
masked_low = -1e30
SP = ("sa", "sb")


def halo(value, width):
    peers = lax.axis_size(SP)
    length = value.shape[0]
    up = [(i, i + 1) for i in range(peers - 1)]
    down = [(j, i) for i, j in up]
    before = lax.ppermute(value[length - width :], SP, up)
    after = lax.ppermute(value[:width], SP, down)
    return jnp.concatenate([before, value, after], axis=0)


def exchange(blocks):
    peers = lax.axis_size("sa")
    here = lax.axis_index("sa")
    got = [lax.dynamic_index_in_dim(blocks, here, 0, keepdims=True)]
    for k in range(1, peers):
        out = lax.dynamic_index_in_dim(blocks, lax.rem(here + k, peers), 0, keepdims=True)
        got.append(lax.ppermute(out, "sa", [(i, (i + k) % peers) for i in range(peers)]))
    ring = got[::-1]
    both = jnp.concatenate(ring + ring, axis=0)
    return lax.dynamic_slice_in_dim(both, peers - 1 - here, peers, 0)


def per_device(
    stream,
    query_rows,
    key_rows,
    value_rows,
    doc_ids,
    sink_logit,
    out_weight,
    norm_gain,
    gate_weight,
    up_weight,
    down_weight,
):
    row_count, width = stream.shape
    n_a, n_b, n_tp = lax.axis_size("sa"), lax.axis_size("sb"), lax.axis_size("tp")
    depth, hidden_here = gate_weight.shape
    share = hidden_here // n_a
    tp_place = lax.axis_index("tp")
    sp_place = lax.axis_index(SP)

    def shares(w):
        return w.reshape(depth, n_a, share).transpose(1, 0, 2)

    gate_up = exchange(jnp.concatenate([shares(gate_weight), shares(up_weight)], axis=2))
    gate_up = gate_up.reshape(n_a * depth, 2 * share)
    gate_up = lax.all_gather(gate_up, "sb", axis=0, tiled=True)
    down_mine = exchange(down_weight.reshape(n_a, share, depth))
    down_mine = down_mine.transpose(0, 2, 1).reshape(n_a * depth, share)

    heads_here = query_rows.shape[1] // HD
    group_share = HEADS // KVH
    groups_here = max(1, heads_here // group_share)
    per_group = heads_here // groups_here
    group_first = tp_place * heads_here // group_share
    keys_here = lax.dynamic_slice_in_dim(key_rows, group_first * HD, groups_here * HD, 1)
    values_here = lax.dynamic_slice_in_dim(value_rows, group_first * HD, groups_here * HD, 1)
    docs_col = jnp.broadcast_to(doc_ids.astype(jnp.bfloat16)[:, None], (row_count, HD))
    packed = halo(jnp.concatenate([keys_here, values_here, docs_col], axis=1), WIN)
    span = groups_here * HD
    keys_wide, values_wide = packed[:, :span], packed[:, span : 2 * span]
    docs_wide = packed[:, 2 * span].astype(jnp.int32)
    seq_offset = sp_place * row_count
    seq_total = row_count * n_a * n_b
    query_pos = seq_offset + jnp.arange(row_count, dtype=jnp.int32)
    key_pos = seq_offset - WIN + jnp.arange(row_count + 2 * WIN, dtype=jnp.int32)
    allowed = (
        (jnp.abs(query_pos[:, None] - key_pos[None, :]) <= WIN)
        & (key_pos[None, :] >= 0)
        & (key_pos[None, :] < seq_total)
        & (doc_ids[:, None] == docs_wide[None, :])
    )
    queries = query_rows.reshape(row_count, groups_here, per_group, HD)
    keys_grid = keys_wide.reshape(row_count + 2 * WIN, groups_here, HD)
    values_grid = values_wide.reshape(row_count + 2 * WIN, groups_here, HD)
    scores = jnp.einsum(
        "qgrd,kgd->grqk", queries, keys_grid, preferred_element_type=jnp.float32
    ) * HD ** (-0.5)
    masked = jnp.where(allowed[None, None], scores, masked_low)
    sinks = sink_logit.reshape(groups_here, per_group, 1, 1)
    peak = jnp.maximum(jnp.max(masked, axis=-1, keepdims=True), sinks)
    lifted = jnp.where(allowed[None, None], jnp.exp(masked - peak), 0.0)
    denom = jnp.sum(lifted, axis=-1, keepdims=True) + jnp.exp(sinks - peak)
    probs = (lifted / denom).astype(jnp.bfloat16)
    attended = jnp.einsum("grqk,kgd->qgrd", probs, values_grid, preferred_element_type=jnp.float32)
    attended = attended.astype(jnp.bfloat16).reshape(row_count, heads_here * HD)
    partial_value = jnp.dot(attended, out_weight, preferred_element_type=jnp.float32)

    rows_mine = row_count // n_tp
    branch = lax.psum_scatter(
        partial_value.astype(jnp.bfloat16), "tp", scatter_dimension=0, tiled=True
    )
    stream_mine = lax.dynamic_slice_in_dim(stream, tp_place * rows_mine, rows_mine, 0)
    carried = (stream_mine.astype(jnp.float32) + branch.astype(jnp.float32)).astype(jnp.bfloat16)
    carried_f = carried.astype(jnp.float32)
    normed = (
        carried_f
        * lax.rsqrt(jnp.mean(carried_f * carried_f, axis=1, keepdims=True) + norm_eps)
        * norm_gain[None, :]
    ).astype(jnp.bfloat16)
    normed = normed.reshape(rows_mine, n_a, n_b, depth).transpose(0, 2, 1, 3).reshape(rows_mine, width)
    rows_all = lax.all_gather(normed, ("sa", "tp"), axis=0, tiled=True)
    down_mine, _ = lax.optimization_barrier((down_mine, normed))
    down_all = lax.all_gather(down_mine, "sb", axis=0, tiled=True)

    gate_acc = jnp.dot(rows_all, gate_up[:, :share], preferred_element_type=jnp.float32)
    up_acc = jnp.dot(rows_all, gate_up[:, share:], preferred_element_type=jnp.float32)
    hidden = (jax.nn.silu(gate_acc) * up_acc).astype(jnp.bfloat16)
    terms = lax.dot_general(
        hidden, down_all, (((1,), (1,)), ((), ())), preferred_element_type=jnp.float32
    )
    feed = lax.psum_scatter(
        terms.astype(jnp.bfloat16), ("sa", "tp"), scatter_dimension=0, tiled=True
    )
    feed = feed.reshape(rows_mine, n_b, n_a, depth).transpose(0, 2, 1, 3).reshape(rows_mine, width)
    mixed = (carried_f + 0.5 * feed.astype(jnp.float32)).astype(jnp.bfloat16)
    return lax.all_gather(mixed, "tp", axis=0, tiled=True)


MESH = pl.DeviceIdType.MESH
AX = ("sa", "sy", "sx", "tp")
CHUNKS = 4
UNITS = 2


def kind_shares(share):
    shift = share // 14 // 16 * 16
    return share - shift, share + shift


def fused(
    stream_hbm, query_hbm, key_hbm, value_hbm, docs_ref, sink_ref, out_w_hbm, gain_ref,
    gate_hbm, up_hbm, down_hbm,
    mixed_ref,
    stream_ref, query_ref, key_ref, value_ref, out_w_ref, gate_ref, up_ref, gate_t, up_t,
    keys, values, docs, attended, branch_out, branch_in, carried_keep, rows, weights,
    sum_keep, pair_out, pair_in, chain_out, chain_fwd, chain_back,
    load_s, halo_s, halo_r, a2a_s, a2a_r, x_s, x_r, y_s, y_r, fx_s, fx_r, fy_s, fy_r,
    br_s, br_r, agf_s, agb_s, agz_r, agc_s, agc_r, pair_s, pair_r,
    cf_s, cl_s, cf_r, cb_r, fin_s, fin_r,
):
    n_a, row_count, width = rows.shape
    n_tp = 2
    z, y, x, c = [lax.axis_index(a) for a in AX]
    place = (z * 2 + y) * 2 + x
    places = n_a * 4
    half = row_count // n_tp
    size = half // CHUNKS
    shares = kind_shares(gate_hbm.shape[1] // n_a)
    depth = gate_hbm.shape[0]
    hi = z // 2
    w = z + hi * (3 - 2 * z)
    here = (z, y, x, c)
    partner = (z, y, x, 1 - c)
    x_next = (z, y, 1 - x, c)
    y_next = (z, 1 - y, x, c)
    fwd = (z + 1 - 2 * hi, y, x, c)
    back = (z - 1 + 2 * hi, y, x, c)
    peers = [z + 1 - 2 * (z % 2), (z + 2) % n_a, n_a - 1 - z]

    def block_at(b):
        return b + hi * (3 - 2 * b)

    def remote(src, dst, s_sem, r_sem, device):
        return pltpu.make_async_remote_copy(
            src_ref=src, dst_ref=dst, send_sem=s_sem, recv_sem=r_sem,
            device_id=device, device_id_type=MESH,
        )

    def at_place(p):
        return (p // 4, (p // 2) % 2, p % 2, c)

    head_cols = pl.ds(pl.multiple_of(c * HD, HD), HD)
    edge = row_count - WIN
    blocks = row_count // WIN

    loads = [
        pltpu.make_async_copy(a, b, load_s.at[i])
        for i, (a, b) in enumerate([
            (key_hbm.at[:, head_cols], key_ref), (value_hbm.at[:, head_cols], value_ref),
            (gate_hbm, gate_ref), (up_hbm, up_ref), (query_hbm, query_ref),
            (out_w_hbm, out_w_ref), (stream_hbm, stream_ref),
        ])
    ]
    for cp in loads:
        cp.start()

    barrier = pltpu.get_barrier_semaphore()
    nearby = [at_place((place + 1) % places), at_place((place + places - 1) % places)]
    for device in [partner, x_next, y_next] + [(p, y, x, c) for p in peers] + nearby:
        pl.semaphore_signal(barrier, inc=1, device_id=device, device_id_type=MESH)
    pl.semaphore_wait(barrier, 8)
    loads[0].wait()
    loads[1].wait()

    def halo_copies(to_next):
        if to_next:
            dev, src, dst, o = at_place(place + 1), edge, 0, 0
        else:
            dev, src, dst, o = at_place(place - 1), 0, row_count + WIN, 3
        src, dst = pl.ds(src, WIN), pl.ds(dst, WIN)
        return [
            remote(key_ref.at[src], keys.at[dst], halo_s.at[o], halo_r.at[o], dev),
            remote(value_ref.at[src], values.at[dst], halo_s.at[o + 1], halo_r.at[o + 1], dev),
            remote(docs_ref.at[src], docs.at[dst], halo_s.at[o + 2], halo_r.at[o + 2], dev),
        ]

    @pl.when(place < places - 1)
    def _():
        for cp in halo_copies(True):
            cp.start()

    @pl.when(place > 0)
    def _():
        for cp in halo_copies(False):
            cp.start()

    def column(zz, yy, xx):
        return pl.ds(pl.multiple_of(((zz * 2 + yy) * 2 + xx) * depth, depth), depth)

    mine_col = column(z, y, x)

    def by_kind(act):
        for kind in (0, 1):

            @pl.when(w == kind)
            def _(kind=kind):
                act(kind)

    def peer_kind(kind, k):
        return kind if k == 2 else 1 - kind

    def first_unit(q):
        inner = shares[0] + (q // 2) * (shares[1] - shares[0])
        return pl.multiple_of((q // 2) * (shares[0] + shares[1]) + (q % 2) * inner, 16)

    def own_piece(q, kind, part_id, s_sem, r_sem, device):
        share = shares[kind]
        src = (gate_t, up_t, down_hbm)[part_id].at[pl.ds(first_unit(q), share)]
        dst = weights.at[pl.ds(part_id * share, share), mine_col]
        return remote(src, dst, s_sem, r_sem, device)

    def a2a(kind, k, part_id):
        to = peers[k]
        return own_piece(to, peer_kind(kind, k), part_id, a2a_s.at[to], a2a_r.at[z], (to, y, x, c))

    def own_x(kind, part_id):
        return own_piece(z, kind, part_id, x_s.at[z], x_r.at[z], x_next)

    def own_y(kind, part_id):
        return own_piece(z, kind, part_id, y_s.at[z], y_r.at[z], y_next)

    def whole(kind, col):
        return weights.at[pl.ds(0, 3 * shares[kind]), col]

    def parts(kind, second):
        cut = 3 * shares[kind] // 32 * 16
        return pl.ds(cut, 3 * shares[kind] - cut) if second else pl.ds(0, cut)

    def wait_bytes(block, s_sem, r_sem):
        return remote(block, block, s_sem, r_sem, here)

    def side(kind, zz, along_x):
        block = whole(kind, column(zz, y, x))
        if along_x:
            return remote(block, block, x_s.at[zz], x_r.at[zz], x_next)
        return remote(block, block, y_s.at[zz], y_r.at[zz], y_next)

    def side_arrived(kind, zz, along_x):
        if along_x:
            wait_bytes(whole(kind, column(zz, y, 1 - x)), x_s.at[zz], x_r.at[zz]).wait_recv()
        else:
            wait_bytes(whole(kind, column(zz, 1 - y, x)), y_s.at[zz], y_r.at[zz]).wait_recv()

    def corner(kind, zz, along_x):
        if along_x:
            block = weights.at[parts(kind, True), column(zz, 1 - y, x)]
            return remote(block, block, fx_s.at[zz], fx_r.at[zz], x_next)
        block = weights.at[parts(kind, False), column(zz, y, 1 - x)]
        return remote(block, block, fy_s.at[zz], fy_r.at[zz], y_next)

    def corner_arrived(kind, zz):
        far_col = column(zz, 1 - y, 1 - x)
        wait_bytes(weights.at[parts(kind, True), far_col], fx_s.at[zz], fx_r.at[zz]).wait_recv()
        wait_bytes(weights.at[parts(kind, False), far_col], fy_s.at[zz], fy_r.at[zz]).wait_recv()

    def own_down(kind):
        share = shares[kind]
        return pltpu.make_async_copy(
            down_hbm.at[pl.ds(first_unit(z), share)], weights.at[pl.ds(2 * share, share), mine_col], load_s.at[7]
        )

    @by_kind
    def _(kind):
        a2a(kind, 0, 2).start()
        own_x(kind, 2).start()
        own_y(kind, 2).start()
        if kind == 1:
            a2a(kind, 2, 2).start()
        own_down(kind).start()

    with jax.named_scope("turn"):
        loads[2].wait()
        loads[3].wait()

        def turn(i, _):
            at = pl.ds(pl.multiple_of(i * HD, HD), HD)
            gate_t[at, :] = gate_ref[:, at].T
            up_t[at, :] = up_ref[:, at].T
            return 0

        lax.fori_loop(0, gate_hbm.shape[1] // HD, turn, 0)

    @by_kind
    def _(kind):
        for part_id in range(2):
            a2a(kind, 0, part_id).start()
        if kind == 1:
            for part_id in range(2):
                a2a(kind, 2, part_id).start()
        for part_id in range(2):
            own_x(kind, part_id).start()
            own_y(kind, part_id).start()
        share = shares[kind]
        weights[pl.ds(0, share), mine_col] = gate_t[pl.ds(first_unit(z), share), :]
        weights[pl.ds(share, share), mine_col] = up_t[pl.ds(first_unit(z), share), :]

    def far_send(kind, k):
        for part_id in range(3):
            a2a(kind, k, part_id).start()

    keys[pl.ds(WIN, row_count), :] = key_ref[...]
    values[pl.ds(WIN, row_count), :] = value_ref[...]
    docs[pl.ds(WIN, row_count)] = docs_ref[...]

    @pl.when(place == 0)
    def _():
        keys[pl.ds(0, WIN), :] = jnp.zeros((WIN, HD), keys.dtype)
        values[pl.ds(0, WIN), :] = jnp.zeros((WIN, HD), values.dtype)
        docs[pl.ds(0, WIN)] = jnp.full((WIN,), -1, jnp.int32)

    @pl.when(place == places - 1)
    def _():
        keys[pl.ds(row_count + WIN, WIN), :] = jnp.zeros((WIN, HD), keys.dtype)
        values[pl.ds(row_count + WIN, WIN), :] = jnp.zeros((WIN, HD), values.dtype)
        docs[pl.ds(row_count + WIN, WIN)] = jnp.full((WIN,), -1, jnp.int32)

    heads_here = query_ref.shape[1] // HD
    row_id = lax.broadcasted_iota(jnp.int32, (WIN, 3 * WIN), 0)
    col_id = lax.broadcasted_iota(jnp.int32, (WIN, 3 * WIN), 1)
    band = (col_id >= row_id) & (col_id <= row_id + 2 * WIN)
    loads[4].wait()

    def attend(b):
        mine = jnp.broadcast_to(docs[pl.ds((b + 1) * WIN, WIN)].reshape(1, WIN), (WIN, WIN)).T
        key_docs = jnp.broadcast_to(docs[pl.ds(b * WIN, 3 * WIN)].reshape(1, 3 * WIN), (WIN, 3 * WIN))
        query_docs = jnp.concatenate([mine] * 3, axis=1)
        allowed = band & (key_docs == query_docs)
        k_block = keys[pl.ds(b * WIN, 3 * WIN), :]
        v_block = values[pl.ds(b * WIN, 3 * WIN), :]
        for h in range(heads_here):
            q = query_ref[pl.ds(b * WIN, WIN), pl.ds(h * HD, HD)]
            scores = lax.dot_general(
                q, k_block, (((1,), (1,)), ((), ())), preferred_element_type=jnp.float32
            ) * HD ** (-0.5)
            masked = jnp.where(allowed, scores, masked_low)
            sink = sink_ref[h]
            peak = jnp.maximum(jnp.max(masked, axis=1, keepdims=True), sink)
            lifted = jnp.where(allowed, jnp.exp(masked - peak), 0.0)
            denom = jnp.sum(lifted, axis=1, keepdims=True) + jnp.exp(sink - peak)
            probs = (lifted / denom).astype(jnp.bfloat16)
            got = jnp.dot(probs, v_block, preferred_element_type=jnp.float32)
            attended[pl.ds(b * WIN, WIN), pl.ds(h * HD, HD)] = got.astype(jnp.bfloat16)

    with jax.named_scope("attend_mid"):
        for b in range(1, blocks - 1):
            attend(b)

    with jax.named_scope("halo_wait"):

        @pl.when(place > 0)
        def _():
            for cp in halo_copies(True):
                cp.wait_recv()

        @pl.when(place < places - 1)
        def _():
            for cp in halo_copies(False):
                cp.wait_recv()

    with jax.named_scope("attend_edge"):
        attend(0)
        attend(blocks - 1)

    mine_rows = pl.ds(pl.multiple_of(c * half, half), half)
    other_rows = pl.ds(pl.multiple_of((1 - c) * half, half), half)
    loads[5].wait()
    loads[6].wait()
    branch_out[...] = jnp.dot(
        attended[other_rows, :], out_w_ref[...], preferred_element_type=jnp.float32
    ).astype(jnp.bfloat16)
    branch_copy = remote(branch_out, branch_in, br_s, br_r, partner)
    branch_copy.start()
    own_branch = jnp.dot(
        attended[mine_rows, :], out_w_ref[...], preferred_element_type=jnp.float32
    ).astype(jnp.bfloat16)

    @by_kind
    def _(kind):
        own_down(kind).wait()

    with jax.named_scope("branch_wait"):
        branch_copy.wait_recv()
    branch = (own_branch.astype(jnp.float32) + branch_in[...].astype(jnp.float32)).astype(jnp.bfloat16)
    carried = (
        stream_ref[mine_rows, :].astype(jnp.float32) + branch.astype(jnp.float32)
    ).astype(jnp.bfloat16)
    carried_keep[...] = carried
    carried_f = carried.astype(jnp.float32)
    normed = (
        carried_f
        * lax.rsqrt(jnp.mean(carried_f * carried_f, axis=1, keepdims=True) + norm_eps)
        * gain_ref[...]
    ).astype(jnp.bfloat16)
    rows[z, mine_rows, :] = normed

    def chunk_rows(core, j):
        return pl.ds(pl.multiple_of(core * half + j * size, 16), size)

    def ag(blk, j, to):
        block = rows.at[blk, chunk_rows(c, j)]
        if to == "core":
            return remote(block, block, agc_s.at[blk, j], agc_r.at[blk, j], partner)
        if to == "fwd":
            return remote(block, block, agf_s.at[blk, j], agz_r.at[blk, j], fwd)
        return remote(block, block, agb_s.at[blk, j], agz_r.at[blk, j], back)

    def ag_arrived(blk, j):
        wait_bytes(rows.at[blk, chunk_rows(c, j)], agf_s.at[blk, j], agz_r.at[blk, j]).wait_recv()

    def ag_core_arrived(blk, j):
        wait_bytes(rows.at[blk, chunk_rows(1 - c, j)], agc_s.at[blk, j], agc_r.at[blk, j]).wait_recv()

    for j in range(CHUNKS):
        ag(z, j, "core").start()

    def rows_fwd():
        for j in range(CHUNKS):
            ag(z, j, "fwd").start()

    def far_sent(kind, k):
        block = whole(peer_kind(kind, k), mine_col)
        wait_bytes(block, a2a_s.at[peers[k]], a2a_r.at[peers[k]]).wait_send()

    def rows_back():
        far_sent(1, 1)
        for j in range(CHUNKS):
            ag(z, j, "back").start()

    def relay_rows(b, j, to=None):
        blk = block_at(b)
        ag_arrived(blk, j)
        if to is not None:
            ag(blk, j, to).start()
        ag(blk, j, "core").start()

    def relay_corner(kind, zz):
        side_arrived(kind, zz, True)
        corner(kind, zz, False).start()
        side_arrived(kind, zz, False)
        corner(kind, zz, True).start()

    def relay_side(kind, k):
        frm = peers[k]
        wait_bytes(whole(kind, column(frm, y, x)), a2a_s.at[frm], a2a_r.at[frm]).wait_recv()
        side(kind, frm, True).start()
        side(kind, frm, False).start()

    def run(plan):
        for name, step, args in plan:
            with jax.named_scope(name):
                step(*args)

    every = range(CHUNKS)
    unit = half // UNITS
    per_unit = CHUNKS // UNITS

    def gather_end():
        run(
            [
                ("corner_own", relay_corner, (0, z)),
                ("side0", relay_side, (0, 0)),
                ("far", far_send, (0, 2)),
                ("rows_fwd", rows_fwd, ()),
                ("corner0", relay_corner, (0, peers[0])),
                ("side2", relay_side, (0, 2)),
                ("side1", relay_side, (0, 1)),
                ("far", far_send, (0, 1)),
                ("corner2", relay_corner, (0, peers[2])),
            ]
            + [("rows1", relay_rows, (1, j)) for j in every]
            + [
                ("corner1", relay_corner, (0, peers[1])),
                ("last_own", corner_arrived, (0, z)),
                ("last0", corner_arrived, (0, peers[0])),
                ("last2", corner_arrived, (0, peers[2])),
            ]
            + [("rows2", relay_rows, (2, j)) for j in range(per_unit)]
            + [("last1", corner_arrived, (0, peers[1]))]
        )

    def gather_middle():
        both = [[("rows0", relay_rows, (0, j, "fwd")), ("rows2", relay_rows, (2, j, "back"))] for j in every]
        run(
            [
                ("corner_own", relay_corner, (1, z)),
                ("side0", relay_side, (1, 0)),
                ("far", far_send, (1, 1)),
                ("rows_fwd", rows_fwd, ()),
                ("side2", relay_side, (1, 2)),
                ("corner0", relay_corner, (1, peers[0])),
                ("rows_back", rows_back, ()),
                ("corner2", relay_corner, (1, peers[2])),
                ("side1", relay_side, (1, 1)),
            ]
            + sum(both, [])
            + [
                ("corner1", relay_corner, (1, peers[1])),
                ("rows3", relay_rows, (3, 0, "back")),
                ("last_own", corner_arrived, (1, z)),
                ("last0", corner_arrived, (1, peers[0])),
                ("last2", corner_arrived, (1, peers[2])),
                ("rows3", relay_rows, (3, 1, "back")),
                ("last1", corner_arrived, (1, peers[1])),
            ]
        )

    chain_b = [2, 3, 1]
    dims = (((1,), (1,)), ((), ()))

    def unit_rows(u):
        return pl.ds(pl.multiple_of(u * unit, 16), unit)

    def pair(blk, u):
        return remote(
            pair_out.at[blk, unit_rows(u)], pair_in.at[blk, unit_rows(u)], pair_s.at[blk, u], pair_r.at[blk, u], partner
        )

    def chunk(j):
        return pl.ds(pl.multiple_of(j * size, 16), size)

    def chip_sum(blk, j):
        return sum_keep[blk, chunk(j)] + pair_in[blk, chunk(j)].astype(jnp.float32)

    def chain_fwd_copy(slot, j):
        return remote(chain_out.at[slot, chunk(j)], chain_fwd.at[slot, chunk(j)], cf_s.at[slot, j], cf_r.at[slot, j], fwd)

    def chain_mid_copy(slot, j):
        return remote(chain_out.at[slot, chunk(j)], chain_back.at[1 - slot, chunk(j)], cf_s.at[slot, j], cb_r.at[1 - slot, j], fwd)

    def chain_last_copy(j):
        return remote(chain_out.at[2, chunk(j)], chain_back.at[0, chunk(j)], cl_s.at[j], cb_r.at[0, j], back)

    def back_arrived(slot, j):
        wait_bytes(chain_back.at[slot, chunk(j)], cl_s.at[j], cb_r.at[slot, j]).wait_recv()

    def send_end(slot, u):
        blk = block_at(chain_b[slot])
        pair(blk, u).wait_recv()
        for t in range(per_unit):
            j = u * per_unit + t
            chain_out[slot, chunk(j)] = chip_sum(blk, j).astype(jnp.bfloat16)
            chain_fwd_copy(slot, j).start()

    def pass_on(slot, j):
        chain_fwd_copy(slot, j).wait_recv()
        total = chip_sum(block_at(chain_b[slot]), j) + chain_fwd[slot, chunk(j)].astype(jnp.float32)
        chain_out[slot, chunk(j)] = total.astype(jnp.bfloat16)
        chain_mid_copy(slot, j).start()

    def feed_forward(kind, blk, u):
        for t in range(per_unit):
            ag_core_arrived(blk, u * per_unit + t)
        share = shares[kind]
        x_rows = jnp.concatenate(
            [rows[blk, pl.ds(pl.multiple_of(h * half + u * unit, 16), unit)] for h in (1 - c, c)], axis=0
        )
        gate_acc = lax.dot_general(x_rows, weights[pl.ds(0, share), :], dims, preferred_element_type=jnp.float32)
        up_acc = lax.dot_general(x_rows, weights[pl.ds(share, share), :], dims, preferred_element_type=jnp.float32)
        hidden = (gate_acc / (1.0 + jnp.exp(-gate_acc)) * up_acc).astype(jnp.bfloat16)
        out = jnp.dot(hidden, weights[pl.ds(2 * share, share), :], preferred_element_type=jnp.float32)
        pair_out[blk, unit_rows(u)] = out[:unit].astype(jnp.bfloat16)
        pair(blk, u).start()
        sum_keep[blk, unit_rows(u)] = out[unit:]

    def pick(step, order):
        late = jnp.where(step == 2, block_at(order[2]), block_at(order[3]))
        return jnp.where(step == 0, block_at(order[0]), jnp.where(step == 1, block_at(order[1]), late))

    def end_unit(i, _):
        step, u = i // UNITS, i % UNITS

        @pl.when(i == 1)
        def _():
            for j in range(per_unit, CHUNKS):
                relay_rows(2, j)

        @pl.when(step == 2)
        def _():
            for t in range(per_unit):
                relay_rows(3, u * per_unit + t)

        feed_forward(0, pick(step, (2, 0, 3, 1)), u)
        for at, slot in ((0, 0), (2, 1), (3, 2)):

            @pl.when(step == at)
            def _(slot=slot):
                send_end(slot, u)

        return 0

    def middle_unit(i, _):
        def back_rows(j):
            relay_rows(3, j, "back")

        def pair_come(b, v):
            pair(block_at(b), v).wait_recv()

        tasks = {
            1: [(back_rows, 2), (pair_come, 2, 0), (pass_on, 0, 0)],
            2: [(back_rows, 3), (pass_on, 0, 1)],
            3: [(pair_come, 2, 1), (pass_on, 0, 2)],
            4: [(pass_on, 0, 3)],
            6: [(pair_come, 3, 0), (pass_on, 1, 0)],
            7: [(pair_come, 3, 1), (pass_on, 1, 1)],
        }
        for at, todo in tasks.items():

            @pl.when(i == at)
            def _(todo=todo):
                for act, *args in todo:
                    act(*args)

        feed_forward(1, pick(i // UNITS, (2, 3, 0, 1)), i % UNITS)
        return 0

    @pl.when(w == 0)
    def _():
        gather_end()
        with jax.named_scope("ffn"):
            lax.fori_loop(0, n_a * UNITS, end_unit, 0)

    @pl.when(w == 1)
    def _():
        gather_middle()
        with jax.named_scope("ffn"):
            lax.fori_loop(0, n_a * UNITS, middle_unit, 0)

    def last(core, j):
        block = mixed_ref.at[chunk_rows(core, j)]
        return remote(block, block, fin_s.at[j], fin_r.at[j], partner)

    def finish(j, total):
        feed = total.astype(jnp.bfloat16).astype(jnp.float32)
        mixed_ref[chunk_rows(c, j), :] = (
            carried_keep[chunk(j)].astype(jnp.float32) + 0.5 * feed
        ).astype(jnp.bfloat16)
        last(c, j).start()

    @pl.when(w == 0)
    def _():
        for u in range(UNITS):
            pair(z, u).wait_recv()
        for j in range(CHUNKS):
            with jax.named_scope(f"fin{j}"):
                back_arrived(0, j)
                finish(j, chip_sum(z, j) + chain_back[0, chunk(j)].astype(jnp.float32))

    @pl.when(w == 1)
    def _():
        for b in (0, 1):
            for u in range(UNITS):
                pair(block_at(b), u).wait_recv()

        def pass_back(j):
            back_arrived(0, j)
            total = chip_sum(block_at(0), j) + chain_back[0, chunk(j)].astype(jnp.float32)
            chain_out[2, chunk(j)] = total.astype(jnp.bfloat16)
            chain_last_copy(j).start()

        def close(j):
            back_arrived(1, j)
            chain_fwd_copy(2, j).wait_recv()
            finish(
                j,
                chip_sum(z, j)
                + chain_fwd[2, chunk(j)].astype(jnp.float32)
                + chain_back[1, chunk(j)].astype(jnp.float32),
            )

        plan = [("on1", pass_on, (1, 2)), ("pback", pass_back, (0,)), ("on1", pass_on, (1, 3))]
        plan += [("pback", pass_back, (1,)), ("pback", pass_back, (2,))]
        plan += [("pback", pass_back, (CHUNKS - 1,))]
        plan += [("close", close, (j,)) for j in range(CHUNKS)]
        run(plan)

    with jax.named_scope("sends_done"):
        @pl.when(place < places - 1)
        def _():
            for cp in halo_copies(True):
                cp.wait_send()

        @pl.when(place > 0)
        def _():
            for cp in halo_copies(False):
                cp.wait_send()

        @by_kind
        def _(kind):
            far_sent(kind, 0)
            far_sent(kind, 2)
            if kind == 0:
                far_sent(kind, 1)
            for zz in [z] + peers:
                wait_bytes(whole(kind, mine_col), x_s.at[zz], x_r.at[zz]).wait_send()
                wait_bytes(whole(kind, mine_col), y_s.at[zz], y_r.at[zz]).wait_send()
                corner(kind, zz, True).wait_send()
                corner(kind, zz, False).wait_send()

        for zz in [z] + peers:
            for u in range(UNITS):
                pair(zz, u).wait_send()
            for j in range(CHUNKS):
                ag(zz, j, "core").wait_send()
        branch_copy.wait_send()
        for j in range(CHUNKS):
            ag(z, j, "fwd").wait_send()

        @pl.when(w == 0)
        def _():
            for slot in range(3):
                for j in range(CHUNKS):
                    chain_fwd_copy(slot, j).wait_send()

        @pl.when(w == 1)
        def _():
            for j in range(CHUNKS):
                ag(z, j, "back").wait_send()
                ag(block_at(0), j, "fwd").wait_send()
                ag(block_at(2), j, "back").wait_send()
                ag(block_at(3), j, "back").wait_send()
                for slot in range(2):
                    chain_mid_copy(slot, j).wait_send()
                chain_last_copy(j).wait_send()

        for j in range(CHUNKS):
            last(c, j).wait_send()
            last(1 - c, j).wait_recv()


def fused_device(
    stream, query_rows, key_rows, value_rows, doc_ids, sink_logit,
    out_weight, norm_gain, gate_weight, up_weight, down_weight,
):
    n_a = lax.axis_size("sa")
    row_count, width = stream.shape
    half = row_count // 2
    depth, hidden_here = gate_weight.shape
    share = hidden_here // n_a
    bf = jnp.bfloat16
    vm = pltpu.VMEM
    dma = pltpu.SemaphoreType.DMA
    wide = row_count + 2 * WIN
    per_block = dma((n_a,))
    per_chunk = dma((n_a, CHUNKS))
    per_unit = dma((n_a, UNITS))
    scratch = [
        vm((row_count, width), bf), vm(query_rows.shape, bf), vm((row_count, HD), bf), vm((row_count, HD), bf),
        vm(out_weight.shape, bf), vm(gate_weight.shape, bf), vm(gate_weight.shape, bf),
        vm((hidden_here, depth), bf), vm((hidden_here, depth), bf),
        vm((wide, HD), bf), vm((wide, HD), bf), vm((wide,), jnp.int32),
        vm(query_rows.shape, bf), vm((half, width), bf), vm((half, width), bf),
        vm((half, width), bf), vm((n_a, row_count, width), bf), vm((3 * max(kind_shares(share)), width), bf),
        vm((n_a, half, width), jnp.float32), vm((n_a, half, width), bf), vm((n_a, half, width), bf),
        vm((3, half, width), bf), vm((3, half, width), bf), vm((2, half, width), bf),
        dma((8,)), dma((6,)), dma((6,)),
        *([per_block] * 10),
        dma, dma, per_chunk, per_chunk, per_chunk, per_chunk, per_chunk, per_unit, per_unit,
        dma((3, CHUNKS)), dma((CHUNKS,)), dma((3, CHUNKS)), dma((2, CHUNKS)), dma((CHUNKS,)), dma((CHUNKS,)),
    ]
    inside = pl.BlockSpec(memory_space=vm)
    anywhere = pl.BlockSpec(memory_space=pl.ANY)
    return pl.pallas_call(
        fused,
        out_shape=vm((row_count, width), bf),
        in_specs=[anywhere] * 4 + [inside, pl.BlockSpec(memory_space=pltpu.SMEM), anywhere, inside] + [anywhere] * 3,
        out_specs=inside,
        scratch_shapes=scratch,
        compiler_params=pltpu.CompilerParams(collective_id=0, has_side_effects=True, vmem_limit_bytes=56 * 2**20),
        name="fused_layer",
    )(
        stream, query_rows, key_rows, value_rows, doc_ids, sink_logit, out_weight,
        norm_gain.reshape(1, width), gate_weight, up_weight, down_weight,
    )


def solution(mesh):
    n_sp, n_tp = mesh.shape["sp"], mesh.shape["tp"]
    n_a = 4 if n_sp % 4 == 0 else 1
    n_b = n_sp // n_a
    if n_a == 4 and n_b == 4 and n_tp == KVH:
        fine = Mesh(mesh.devices.reshape(n_a, 2, 2, n_tp), AX)
        sp, body = AX[:3], fused_device
    else:
        fine = Mesh(mesh.devices.reshape(n_a, n_b, n_tp), ("sa", "sb", "tp"))
        sp, body = SP, per_device
    in_specs = (
        P(sp, None),
        P(sp, "tp"),
        P(sp, None),
        P(sp, None),
        P(sp),
        P("tp"),
        P("tp", None),
        P(),
        P(sp, "tp"),
        P(sp, "tp"),
        P("tp", sp),
    )
    return jax.shard_map(body, mesh=fine, in_specs=in_specs, out_specs=P(sp, None), check_vma=False)
```

```python
import jax
import jax.numpy as jnp
from jax import lax
from jax.experimental import pallas as pl
from jax.experimental.pallas import tpu as pltpu
from jax.sharding import Mesh, PartitionSpec as P

HEADS = 8
KVH = 2
HD = 128
WIN = 128

norm_eps = 1e-06
masked_low = -1e30
SP = ("sa", "sb")


def halo(value, width):
    peers = lax.axis_size(SP)
    length = value.shape[0]
    up = [(i, i + 1) for i in range(peers - 1)]
    down = [(j, i) for i, j in up]
    before = lax.ppermute(value[length - width :], SP, up)
    after = lax.ppermute(value[:width], SP, down)
    return jnp.concatenate([before, value, after], axis=0)


def exchange(blocks):
    peers = lax.axis_size("sa")
    here = lax.axis_index("sa")
    got = [lax.dynamic_index_in_dim(blocks, here, 0, keepdims=True)]
    for k in range(1, peers):
        out = lax.dynamic_index_in_dim(blocks, lax.rem(here + k, peers), 0, keepdims=True)
        got.append(lax.ppermute(out, "sa", [(i, (i + k) % peers) for i in range(peers)]))
    ring = got[::-1]
    both = jnp.concatenate(ring + ring, axis=0)
    return lax.dynamic_slice_in_dim(both, peers - 1 - here, peers, 0)


def per_device(
    stream,
    query_rows,
    key_rows,
    value_rows,
    doc_ids,
    sink_logit,
    out_weight,
    norm_gain,
    gate_weight,
    up_weight,
    down_weight,
):
    row_count, width = stream.shape
    n_a, n_b, n_tp = lax.axis_size("sa"), lax.axis_size("sb"), lax.axis_size("tp")
    depth, hidden_here = gate_weight.shape
    share = hidden_here // n_a
    tp_place = lax.axis_index("tp")
    sp_place = lax.axis_index(SP)

    def shares(w):
        return w.reshape(depth, n_a, share).transpose(1, 0, 2)

    gate_up = exchange(jnp.concatenate([shares(gate_weight), shares(up_weight)], axis=2))
    gate_up = gate_up.reshape(n_a * depth, 2 * share)
    gate_up = lax.all_gather(gate_up, "sb", axis=0, tiled=True)
    down_mine = exchange(down_weight.reshape(n_a, share, depth))
    down_mine = down_mine.transpose(0, 2, 1).reshape(n_a * depth, share)

    heads_here = query_rows.shape[1] // HD
    group_share = HEADS // KVH
    groups_here = max(1, heads_here // group_share)
    per_group = heads_here // groups_here
    group_first = tp_place * heads_here // group_share
    keys_here = lax.dynamic_slice_in_dim(key_rows, group_first * HD, groups_here * HD, 1)
    values_here = lax.dynamic_slice_in_dim(value_rows, group_first * HD, groups_here * HD, 1)
    docs_col = jnp.broadcast_to(doc_ids.astype(jnp.bfloat16)[:, None], (row_count, HD))
    packed = halo(jnp.concatenate([keys_here, values_here, docs_col], axis=1), WIN)
    span = groups_here * HD
    keys_wide, values_wide = packed[:, :span], packed[:, span : 2 * span]
    docs_wide = packed[:, 2 * span].astype(jnp.int32)
    seq_offset = sp_place * row_count
    seq_total = row_count * n_a * n_b
    query_pos = seq_offset + jnp.arange(row_count, dtype=jnp.int32)
    key_pos = seq_offset - WIN + jnp.arange(row_count + 2 * WIN, dtype=jnp.int32)
    allowed = (
        (jnp.abs(query_pos[:, None] - key_pos[None, :]) <= WIN)
        & (key_pos[None, :] >= 0)
        & (key_pos[None, :] < seq_total)
        & (doc_ids[:, None] == docs_wide[None, :])
    )
    queries = query_rows.reshape(row_count, groups_here, per_group, HD)
    keys_grid = keys_wide.reshape(row_count + 2 * WIN, groups_here, HD)
    values_grid = values_wide.reshape(row_count + 2 * WIN, groups_here, HD)
    scores = jnp.einsum(
        "qgrd,kgd->grqk", queries, keys_grid, preferred_element_type=jnp.float32
    ) * HD ** (-0.5)
    masked = jnp.where(allowed[None, None], scores, masked_low)
    sinks = sink_logit.reshape(groups_here, per_group, 1, 1)
    peak = jnp.maximum(jnp.max(masked, axis=-1, keepdims=True), sinks)
    lifted = jnp.where(allowed[None, None], jnp.exp(masked - peak), 0.0)
    denom = jnp.sum(lifted, axis=-1, keepdims=True) + jnp.exp(sinks - peak)
    probs = (lifted / denom).astype(jnp.bfloat16)
    attended = jnp.einsum("grqk,kgd->qgrd", probs, values_grid, preferred_element_type=jnp.float32)
    attended = attended.astype(jnp.bfloat16).reshape(row_count, heads_here * HD)
    partial_value = jnp.dot(attended, out_weight, preferred_element_type=jnp.float32)

    rows_mine = row_count // n_tp
    branch = lax.psum_scatter(
        partial_value.astype(jnp.bfloat16), "tp", scatter_dimension=0, tiled=True
    )
    stream_mine = lax.dynamic_slice_in_dim(stream, tp_place * rows_mine, rows_mine, 0)
    carried = (stream_mine.astype(jnp.float32) + branch.astype(jnp.float32)).astype(jnp.bfloat16)
    carried_f = carried.astype(jnp.float32)
    normed = (
        carried_f
        * lax.rsqrt(jnp.mean(carried_f * carried_f, axis=1, keepdims=True) + norm_eps)
        * norm_gain[None, :]
    ).astype(jnp.bfloat16)
    normed = normed.reshape(rows_mine, n_a, n_b, depth).transpose(0, 2, 1, 3).reshape(rows_mine, width)
    rows_all = lax.all_gather(normed, ("sa", "tp"), axis=0, tiled=True)
    down_mine, _ = lax.optimization_barrier((down_mine, normed))
    down_all = lax.all_gather(down_mine, "sb", axis=0, tiled=True)

    gate_acc = jnp.dot(rows_all, gate_up[:, :share], preferred_element_type=jnp.float32)
    up_acc = jnp.dot(rows_all, gate_up[:, share:], preferred_element_type=jnp.float32)
    hidden = (jax.nn.silu(gate_acc) * up_acc).astype(jnp.bfloat16)
    terms = lax.dot_general(
        hidden, down_all, (((1,), (1,)), ((), ())), preferred_element_type=jnp.float32
    )
    feed = lax.psum_scatter(
        terms.astype(jnp.bfloat16), ("sa", "tp"), scatter_dimension=0, tiled=True
    )
    feed = feed.reshape(rows_mine, n_b, n_a, depth).transpose(0, 2, 1, 3).reshape(rows_mine, width)
    mixed = (carried_f + 0.5 * feed.astype(jnp.float32)).astype(jnp.bfloat16)
    return lax.all_gather(mixed, "tp", axis=0, tiled=True)


MESH = pl.DeviceIdType.MESH
AX = ("sa", "sy", "sx", "tp")
CHUNKS = 4
UNITS = 2


def kind_shares(share):
    shift = share // 14 // 16 * 16
    return share - shift, share + shift


def fused(
    stream_hbm, query_hbm, key_hbm, value_hbm, docs_ref, sink_ref, out_w_hbm, gain_ref,
    gate_hbm, up_hbm, down_hbm,
    mixed_ref,
    stream_ref, query_ref, key_ref, value_ref, out_w_ref, gate_ref, up_ref, gate_t, up_t,
    keys, values, docs, attended, branch_out, branch_in, carried_keep, rows, weights,
    sum_keep, pair_out, pair_in, chain_out, chain_fwd, chain_back,
    load_s, halo_s, halo_r, a2a_s, a2a_r, x_s, x_r, y_s, y_r, fx_s, fx_r, fy_s, fy_r,
    br_s, br_r, agf_s, agb_s, agz_r, agc_s, agc_r, pair_s, pair_r,
    cf_s, cl_s, cf_r, cb_r, fin_s, fin_r,
):
    n_a, row_count, width = rows.shape
    n_tp = 2
    z, y, x, c = [lax.axis_index(a) for a in AX]
    place = (z * 2 + y) * 2 + x
    places = n_a * 4
    half = row_count // n_tp
    size = half // CHUNKS
    shares = kind_shares(gate_hbm.shape[1] // n_a)
    depth = gate_hbm.shape[0]
    hi = z // 2
    w = z + hi * (3 - 2 * z)
    here = (z, y, x, c)
    partner = (z, y, x, 1 - c)
    x_next = (z, y, 1 - x, c)
    y_next = (z, 1 - y, x, c)
    fwd = (z + 1 - 2 * hi, y, x, c)
    back = (z - 1 + 2 * hi, y, x, c)
    peers = [z + 1 - 2 * (z % 2), (z + 2) % n_a, n_a - 1 - z]

    def block_at(b):
        return b + hi * (3 - 2 * b)

    def remote(src, dst, s_sem, r_sem, device):
        return pltpu.make_async_remote_copy(
            src_ref=src, dst_ref=dst, send_sem=s_sem, recv_sem=r_sem,
            device_id=device, device_id_type=MESH,
        )

    def at_place(p):
        return (p // 4, (p // 2) % 2, p % 2, c)

    head_cols = pl.ds(pl.multiple_of(c * HD, HD), HD)
    edge = row_count - WIN
    blocks = row_count // WIN

    loads = [
        pltpu.make_async_copy(a, b, load_s.at[i])
        for i, (a, b) in enumerate([
            (key_hbm.at[:, head_cols], key_ref), (value_hbm.at[:, head_cols], value_ref),
            (gate_hbm, gate_ref), (up_hbm, up_ref), (query_hbm, query_ref),
            (out_w_hbm, out_w_ref), (stream_hbm, stream_ref),
        ])
    ]
    barrier = pltpu.get_barrier_semaphore()
    nearby = [at_place((place + 1) % places), at_place((place + places - 1) % places)]
    for device in [partner, x_next, y_next] + [(p, y, x, c) for p in peers] + nearby:
        pl.semaphore_signal(barrier, inc=1, device_id=device, device_id_type=MESH)
    for cp in loads:
        cp.start()
    pl.semaphore_wait(barrier, 8)
    loads[0].wait()
    loads[1].wait()

    def halo_copies(to_next):
        if to_next:
            dev, src, dst, o = at_place(place + 1), edge, 0, 0
        else:
            dev, src, dst, o = at_place(place - 1), 0, row_count + WIN, 3
        src, dst = pl.ds(src, WIN), pl.ds(dst, WIN)
        return [
            remote(key_ref.at[src], keys.at[dst], halo_s.at[o], halo_r.at[o], dev),
            remote(value_ref.at[src], values.at[dst], halo_s.at[o + 1], halo_r.at[o + 1], dev),
            remote(docs_ref.at[src], docs.at[dst], halo_s.at[o + 2], halo_r.at[o + 2], dev),
        ]

    @pl.when(place < places - 1)
    def _():
        for cp in halo_copies(True):
            cp.start()

    @pl.when(place > 0)
    def _():
        for cp in halo_copies(False):
            cp.start()

    def column(zz, yy, xx):
        return pl.ds(pl.multiple_of(((zz * 2 + yy) * 2 + xx) * depth, depth), depth)

    mine_col = column(z, y, x)

    def by_kind(act):
        for kind in (0, 1):

            @pl.when(w == kind)
            def _(kind=kind):
                act(kind)

    def peer_kind(kind, k):
        return kind if k == 2 else 1 - kind

    def first_unit(q):
        inner = shares[0] + (q // 2) * (shares[1] - shares[0])
        return pl.multiple_of((q // 2) * (shares[0] + shares[1]) + (q % 2) * inner, 16)

    def own_piece(q, kind, part_id, s_sem, r_sem, device):
        share = shares[kind]
        src = (gate_t, up_t, down_hbm)[part_id].at[pl.ds(first_unit(q), share)]
        dst = weights.at[pl.ds(part_id * share, share), mine_col]
        return remote(src, dst, s_sem, r_sem, device)

    def a2a(kind, k, part_id):
        to = peers[k]
        return own_piece(to, peer_kind(kind, k), part_id, a2a_s.at[to], a2a_r.at[z], (to, y, x, c))

    def own_x(kind, part_id):
        return own_piece(z, kind, part_id, x_s, x_r.at[z], x_next)

    def own_y(kind, part_id):
        return own_piece(z, kind, part_id, y_s, y_r.at[z], y_next)

    def whole(kind, col):
        return weights.at[pl.ds(0, 3 * shares[kind]), col]

    def parts(kind, second):
        cut = 3 * shares[kind] // 32 * 16
        return pl.ds(cut, 3 * shares[kind] - cut) if second else pl.ds(0, cut)

    def wait_bytes(block, s_sem, r_sem):
        return remote(block, block, s_sem, r_sem, here)

    def side(kind, zz, along_x):
        block = whole(kind, column(zz, y, x))
        if along_x:
            return remote(block, block, x_s, x_r.at[zz], x_next)
        return remote(block, block, y_s, y_r.at[zz], y_next)

    def side_arrived(kind, zz, along_x):
        if along_x:
            wait_bytes(whole(kind, column(zz, y, 1 - x)), x_s, x_r.at[zz]).wait_recv()
        else:
            wait_bytes(whole(kind, column(zz, 1 - y, x)), y_s, y_r.at[zz]).wait_recv()

    def corner(kind, zz, along_x):
        if along_x:
            block = weights.at[parts(kind, True), column(zz, 1 - y, x)]
            return remote(block, block, fx_s, fx_r.at[zz], x_next)
        block = weights.at[parts(kind, False), column(zz, y, 1 - x)]
        return remote(block, block, fy_s, fy_r.at[zz], y_next)

    def corner_arrived(kind, zz):
        far_col = column(zz, 1 - y, 1 - x)
        wait_bytes(weights.at[parts(kind, True), far_col], fx_s, fx_r.at[zz]).wait_recv()
        wait_bytes(weights.at[parts(kind, False), far_col], fy_s, fy_r.at[zz]).wait_recv()

    def own_down(kind):
        share = shares[kind]
        return pltpu.make_async_copy(
            down_hbm.at[pl.ds(first_unit(z), share)], weights.at[pl.ds(2 * share, share), mine_col], load_s.at[7]
        )

    @by_kind
    def _(kind):
        a2a(kind, 0, 2).start()
        own_x(kind, 2).start()
        own_y(kind, 2).start()
        if kind == 1:
            a2a(kind, 2, 2).start()
        own_down(kind).start()

    with jax.named_scope("turn"):
        loads[2].wait()
        loads[3].wait()

        def turn(i, _):
            at = pl.ds(pl.multiple_of(i * HD, HD), HD)
            gate_t[at, :] = gate_ref[:, at].T
            up_t[at, :] = up_ref[:, at].T
            return 0

        lax.fori_loop(0, gate_hbm.shape[1] // HD, turn, 0)

    @by_kind
    def _(kind):
        for part_id in range(2):
            a2a(kind, 0, part_id).start()
        if kind == 1:
            for part_id in range(2):
                a2a(kind, 2, part_id).start()
        for part_id in range(2):
            own_x(kind, part_id).start()
            own_y(kind, part_id).start()
        share = shares[kind]
        weights[pl.ds(0, share), mine_col] = gate_t[pl.ds(first_unit(z), share), :]
        weights[pl.ds(share, share), mine_col] = up_t[pl.ds(first_unit(z), share), :]

    def far_send(kind, k):
        for part_id in range(3):
            a2a(kind, k, part_id).start()

    keys[pl.ds(WIN, row_count), :] = key_ref[...]
    values[pl.ds(WIN, row_count), :] = value_ref[...]
    docs[pl.ds(WIN, row_count)] = docs_ref[...]

    @pl.when(place == 0)
    def _():
        keys[pl.ds(0, WIN), :] = jnp.zeros((WIN, HD), keys.dtype)
        values[pl.ds(0, WIN), :] = jnp.zeros((WIN, HD), values.dtype)
        docs[pl.ds(0, WIN)] = jnp.full((WIN,), -1, jnp.int32)

    @pl.when(place == places - 1)
    def _():
        keys[pl.ds(row_count + WIN, WIN), :] = jnp.zeros((WIN, HD), keys.dtype)
        values[pl.ds(row_count + WIN, WIN), :] = jnp.zeros((WIN, HD), values.dtype)
        docs[pl.ds(row_count + WIN, WIN)] = jnp.full((WIN,), -1, jnp.int32)

    heads_here = query_ref.shape[1] // HD
    row_id = lax.broadcasted_iota(jnp.int32, (WIN, 3 * WIN), 0)
    col_id = lax.broadcasted_iota(jnp.int32, (WIN, 3 * WIN), 1)
    band = (col_id >= row_id) & (col_id <= row_id + 2 * WIN)
    loads[4].wait()

    def attend(b):
        mine = jnp.broadcast_to(docs[pl.ds((b + 1) * WIN, WIN)].reshape(1, WIN), (WIN, WIN)).T
        key_docs = jnp.broadcast_to(docs[pl.ds(b * WIN, 3 * WIN)].reshape(1, 3 * WIN), (WIN, 3 * WIN))
        query_docs = jnp.concatenate([mine] * 3, axis=1)
        allowed = band & (key_docs == query_docs)
        k_block = keys[pl.ds(b * WIN, 3 * WIN), :]
        v_block = values[pl.ds(b * WIN, 3 * WIN), :]
        for h in range(heads_here):
            q = query_ref[pl.ds(b * WIN, WIN), pl.ds(h * HD, HD)]
            scores = lax.dot_general(
                q, k_block, (((1,), (1,)), ((), ())), preferred_element_type=jnp.float32
            ) * HD ** (-0.5)
            masked = jnp.where(allowed, scores, masked_low)
            sink = sink_ref[h]
            peak = jnp.maximum(jnp.max(masked, axis=1, keepdims=True), sink)
            lifted = jnp.where(allowed, jnp.exp(masked - peak), 0.0)
            denom = jnp.sum(lifted, axis=1, keepdims=True) + jnp.exp(sink - peak)
            probs = (lifted / denom).astype(jnp.bfloat16)
            got = jnp.dot(probs, v_block, preferred_element_type=jnp.float32)
            attended[pl.ds(b * WIN, WIN), pl.ds(h * HD, HD)] = got.astype(jnp.bfloat16)

    with jax.named_scope("attend_mid"):
        for b in range(1, blocks - 1):
            attend(b)

    with jax.named_scope("halo_wait"):

        @pl.when(place > 0)
        def _():
            for cp in halo_copies(True):
                cp.wait_recv()

        @pl.when(place < places - 1)
        def _():
            for cp in halo_copies(False):
                cp.wait_recv()

    with jax.named_scope("attend_edge"):
        attend(0)
        attend(blocks - 1)

    mine_rows = pl.ds(pl.multiple_of(c * half, half), half)
    other_rows = pl.ds(pl.multiple_of((1 - c) * half, half), half)
    loads[5].wait()
    loads[6].wait()
    branch_out[...] = jnp.dot(
        attended[other_rows, :], out_w_ref[...], preferred_element_type=jnp.float32
    ).astype(jnp.bfloat16)
    branch_copy = remote(branch_out, branch_in, br_s, br_r, partner)
    branch_copy.start()
    own_branch = jnp.dot(
        attended[mine_rows, :], out_w_ref[...], preferred_element_type=jnp.float32
    ).astype(jnp.bfloat16)

    @by_kind
    def _(kind):
        own_down(kind).wait()

    with jax.named_scope("branch_wait"):
        branch_copy.wait_recv()
    branch = (own_branch.astype(jnp.float32) + branch_in[...].astype(jnp.float32)).astype(jnp.bfloat16)
    carried = (
        stream_ref[mine_rows, :].astype(jnp.float32) + branch.astype(jnp.float32)
    ).astype(jnp.bfloat16)
    carried_keep[...] = carried
    carried_f = carried.astype(jnp.float32)
    normed = (
        carried_f
        * lax.rsqrt(jnp.mean(carried_f * carried_f, axis=1, keepdims=True) + norm_eps)
        * gain_ref[...]
    ).astype(jnp.bfloat16)
    rows[z, mine_rows, :] = normed

    def chunk_rows(core, j):
        return pl.ds(pl.multiple_of(core * half + j * size, 16), size)

    def ag(blk, j, to):
        block = rows.at[blk, chunk_rows(c, j)]
        if to == "core":
            return remote(block, block, agc_s, agc_r.at[blk, j], partner)
        if to == "fwd":
            return remote(block, block, agf_s, agz_r.at[blk, j], fwd)
        return remote(block, block, agb_s, agz_r.at[blk, j], back)

    def ag_arrived(blk, j):
        wait_bytes(rows.at[blk, chunk_rows(c, j)], agf_s, agz_r.at[blk, j]).wait_recv()

    def ag_core_arrived(blk, j):
        wait_bytes(rows.at[blk, chunk_rows(1 - c, j)], agc_s, agc_r.at[blk, j]).wait_recv()

    for j in range(CHUNKS):
        ag(z, j, "core").start()

    def rows_fwd():
        for j in range(CHUNKS):
            ag(z, j, "fwd").start()

    def far_sent(kind, k):
        block = whole(peer_kind(kind, k), mine_col)
        wait_bytes(block, a2a_s.at[peers[k]], a2a_r.at[peers[k]]).wait_send()

    def rows_back():
        far_sent(1, 1)
        for j in range(CHUNKS):
            ag(z, j, "back").start()

    def relay_rows(b, j, to=None):
        blk = block_at(b)
        ag_arrived(blk, j)
        if to is not None:
            ag(blk, j, to).start()
        ag(blk, j, "core").start()

    def relay_corner(kind, zz):
        side_arrived(kind, zz, True)
        corner(kind, zz, False).start()
        side_arrived(kind, zz, False)
        corner(kind, zz, True).start()

    def relay_side(kind, k):
        frm = peers[k]
        wait_bytes(whole(kind, column(frm, y, x)), a2a_s.at[frm], a2a_r.at[frm]).wait_recv()
        side(kind, frm, True).start()
        side(kind, frm, False).start()

    def run(plan):
        for name, step, args in plan:
            with jax.named_scope(name):
                step(*args)

    every = range(CHUNKS)
    unit = half // UNITS
    per_unit = CHUNKS // UNITS

    def gather_end():
        run(
            [
                ("corner_own", relay_corner, (0, z)),
                ("side0", relay_side, (0, 0)),
                ("far", far_send, (0, 2)),
                ("rows_fwd", rows_fwd, ()),
                ("side2", relay_side, (0, 2)),
                ("corner0", relay_corner, (0, peers[0])),
                ("side1", relay_side, (0, 1)),
                ("far", far_send, (0, 1)),
                ("corner2", relay_corner, (0, peers[2])),
            ]
            + [("rows1", relay_rows, (1, j)) for j in every]
            + [
                ("corner1", relay_corner, (0, peers[1])),
                ("last_own", corner_arrived, (0, z)),
                ("last0", corner_arrived, (0, peers[0])),
                ("last2", corner_arrived, (0, peers[2])),
            ]
            + [("rows2", relay_rows, (2, j)) for j in range(per_unit)]
            + [("last1", corner_arrived, (0, peers[1]))]
        )

    def gather_middle():
        both = [[("rows0", relay_rows, (0, j, "fwd")), ("rows2", relay_rows, (2, j, "back"))] for j in every]
        run(
            [
                ("corner_own", relay_corner, (1, z)),
                ("side0", relay_side, (1, 0)),
                ("far", far_send, (1, 1)),
                ("rows_fwd", rows_fwd, ()),
                ("side2", relay_side, (1, 2)),
                ("corner0", relay_corner, (1, peers[0])),
                ("rows_back", rows_back, ()),
                ("corner2", relay_corner, (1, peers[2])),
                ("side1", relay_side, (1, 1)),
            ]
            + sum(both, [])
            + [
                ("corner1", relay_corner, (1, peers[1])),
                ("rows3", relay_rows, (3, 0, "back")),
                ("last_own", corner_arrived, (1, z)),
                ("last0", corner_arrived, (1, peers[0])),
                ("last2", corner_arrived, (1, peers[2])),
                ("rows3", relay_rows, (3, 1, "back")),
                ("last1", corner_arrived, (1, peers[1])),
            ]
        )

    chain_b = [2, 3, 1]
    dims = (((1,), (1,)), ((), ()))

    def unit_rows(u):
        return pl.ds(pl.multiple_of(u * unit, 16), unit)

    def pair(blk, u):
        return remote(
            pair_out.at[blk, unit_rows(u)], pair_in.at[blk, unit_rows(u)], pair_s, pair_r.at[blk, u], partner
        )

    def chunk(j):
        return pl.ds(pl.multiple_of(j * size, 16), size)

    def chip_sum(blk, j):
        return sum_keep[blk, chunk(j)] + pair_in[blk, chunk(j)].astype(jnp.float32)

    def chain_fwd_copy(slot, j):
        return remote(chain_out.at[slot, chunk(j)], chain_fwd.at[slot, chunk(j)], cf_s, cf_r.at[slot, j], fwd)

    def chain_mid_copy(slot, j):
        return remote(chain_out.at[slot, chunk(j)], chain_back.at[1 - slot, chunk(j)], cf_s, cb_r.at[1 - slot, j], fwd)

    def chain_last_copy(j):
        return remote(chain_out.at[2, chunk(j)], chain_back.at[0, chunk(j)], cl_s, cb_r.at[0, j], back)

    def back_arrived(slot, j):
        wait_bytes(chain_back.at[slot, chunk(j)], cl_s, cb_r.at[slot, j]).wait_recv()

    def send_end(slot, u):
        blk = block_at(chain_b[slot])
        pair(blk, u).wait_recv()
        for t in range(per_unit):
            j = u * per_unit + t
            chain_out[slot, chunk(j)] = chip_sum(blk, j).astype(jnp.bfloat16)
            chain_fwd_copy(slot, j).start()

    def pass_on(slot, j):
        chain_fwd_copy(slot, j).wait_recv()
        total = chip_sum(block_at(chain_b[slot]), j) + chain_fwd[slot, chunk(j)].astype(jnp.float32)
        chain_out[slot, chunk(j)] = total.astype(jnp.bfloat16)
        chain_mid_copy(slot, j).start()

    def feed_forward(kind, blk, u):
        for t in range(per_unit):
            ag_core_arrived(blk, u * per_unit + t)
        share = shares[kind]
        x_rows = jnp.concatenate(
            [rows[blk, pl.ds(pl.multiple_of(h * half + u * unit, 16), unit)] for h in (1 - c, c)], axis=0
        )
        gate_acc = lax.dot_general(x_rows, weights[pl.ds(0, share), :], dims, preferred_element_type=jnp.float32)
        up_acc = lax.dot_general(x_rows, weights[pl.ds(share, share), :], dims, preferred_element_type=jnp.float32)
        hidden = (gate_acc / (1.0 + jnp.exp(-gate_acc)) * up_acc).astype(jnp.bfloat16)
        out = jnp.dot(hidden, weights[pl.ds(2 * share, share), :], preferred_element_type=jnp.float32)
        pair_out[blk, unit_rows(u)] = out[:unit].astype(jnp.bfloat16)
        pair(blk, u).start()
        sum_keep[blk, unit_rows(u)] = out[unit:]

    def pick(step, order):
        late = jnp.where(step == 2, block_at(order[2]), block_at(order[3]))
        return jnp.where(step == 0, block_at(order[0]), jnp.where(step == 1, block_at(order[1]), late))

    def end_unit(i, _):
        step, u = i // UNITS, i % UNITS

        @pl.when(i == 1)
        def _():
            for j in range(per_unit, CHUNKS):
                relay_rows(2, j)

        @pl.when(step == 2)
        def _():
            for t in range(per_unit):
                relay_rows(3, u * per_unit + t)

        feed_forward(0, pick(step, (2, 0, 3, 1)), u)
        for at, slot in ((0, 0), (2, 1), (3, 2)):

            @pl.when(step == at)
            def _(slot=slot):
                send_end(slot, u)

        return 0

    def middle_unit(i, _):
        def back_rows(j):
            relay_rows(3, j, "back")

        def pair_come(b, v):
            pair(block_at(b), v).wait_recv()

        tasks = {
            1: [(back_rows, 2), (pair_come, 2, 0), (pass_on, 0, 0)],
            2: [(back_rows, 3), (pass_on, 0, 1)],
            3: [(pair_come, 2, 1), (pass_on, 0, 2)],
            4: [(pass_on, 0, 3)],
            6: [(pair_come, 3, 0), (pass_on, 1, 0)],
            7: [(pair_come, 3, 1), (pass_on, 1, 1)],
        }
        for at, todo in tasks.items():

            @pl.when(i == at)
            def _(todo=todo):
                for act, *args in todo:
                    act(*args)

        feed_forward(1, pick(i // UNITS, (2, 3, 0, 1)), i % UNITS)
        return 0

    @pl.when(w == 0)
    def _():
        gather_end()
        with jax.named_scope("ffn"):
            lax.fori_loop(0, n_a * UNITS, end_unit, 0)

    @pl.when(w == 1)
    def _():
        gather_middle()
        with jax.named_scope("ffn"):
            lax.fori_loop(0, n_a * UNITS, middle_unit, 0)

    def last(core, j):
        block = mixed_ref.at[chunk_rows(core, j)]
        return remote(block, block, fin_s, fin_r.at[j], partner)

    def finish(j, total):
        feed = total.astype(jnp.bfloat16).astype(jnp.float32)
        mixed_ref[chunk_rows(c, j), :] = (
            carried_keep[chunk(j)].astype(jnp.float32) + 0.5 * feed
        ).astype(jnp.bfloat16)
        last(c, j).start()

    @pl.when(w == 0)
    def _():
        for u in range(UNITS):
            pair(z, u).wait_recv()
        for j in range(CHUNKS):
            with jax.named_scope(f"fin{j}"):
                back_arrived(0, j)
                finish(j, chip_sum(z, j) + chain_back[0, chunk(j)].astype(jnp.float32))

    @pl.when(w == 1)
    def _():
        for b in (0, 1):
            for u in range(UNITS):
                pair(block_at(b), u).wait_recv()

        def pass_back(j):
            back_arrived(0, j)
            total = chip_sum(block_at(0), j) + chain_back[0, chunk(j)].astype(jnp.float32)
            chain_out[2, chunk(j)] = total.astype(jnp.bfloat16)
            chain_last_copy(j).start()

        def close(j):
            back_arrived(1, j)
            chain_fwd_copy(2, j).wait_recv()
            finish(
                j,
                chip_sum(z, j)
                + chain_fwd[2, chunk(j)].astype(jnp.float32)
                + chain_back[1, chunk(j)].astype(jnp.float32),
            )

        plan = [("on1", pass_on, (1, 2)), ("pback", pass_back, (0,)), ("on1", pass_on, (1, 3))]
        plan += [("pback", pass_back, (1,)), ("pback", pass_back, (2,))]
        plan += [("pback", pass_back, (CHUNKS - 1,))]
        plan += [("close", close, (j,)) for j in range(CHUNKS)]
        run(plan)

    with jax.named_scope("sends_done"):
        @pl.when(place < places - 1)
        def _():
            for cp in halo_copies(True):
                cp.wait_send()

        @pl.when(place > 0)
        def _():
            for cp in halo_copies(False):
                cp.wait_send()

        @by_kind
        def _(kind):
            far_sent(kind, 0)
            far_sent(kind, 2)
            if kind == 0:
                far_sent(kind, 1)
            four = pl.ds(0, n_a * depth)
            wait_bytes(whole(kind, four), x_s, x_r.at[0]).wait_send()
            wait_bytes(whole(kind, four), y_s, y_r.at[0]).wait_send()
            wait_bytes(weights.at[parts(kind, True), four], fx_s, fx_r.at[0]).wait_send()
            wait_bytes(weights.at[parts(kind, False), four], fy_s, fy_r.at[0]).wait_send()

        wait_bytes(pair_out, pair_s, pair_r.at[0, 0]).wait_send()
        wait_bytes(rows.at[:, mine_rows], agc_s, agc_r.at[0, 0]).wait_send()
        branch_copy.wait_send()

        @pl.when(w == 0)
        def _():
            wait_bytes(rows.at[z, mine_rows], agf_s, agz_r.at[0, 0]).wait_send()
            wait_bytes(chain_out, cf_s, cf_r.at[0, 0]).wait_send()

        @pl.when(w == 1)
        def _():
            wait_bytes(rows.at[pl.ds(0, 2), mine_rows], agf_s, agz_r.at[0, 0]).wait_send()
            wait_bytes(rows.at[pl.ds(0, 3), mine_rows], agb_s, agz_r.at[0, 0]).wait_send()
            wait_bytes(chain_out.at[pl.ds(0, 2)], cf_s, cf_r.at[0, 0]).wait_send()
            wait_bytes(chain_out.at[2], cl_s, cb_r.at[0, 0]).wait_send()

        for j in range(CHUNKS):
            last(1 - c, j).wait_recv()
        wait_bytes(mixed_ref.at[mine_rows], fin_s, fin_r.at[0]).wait_send()


def fused_device(
    stream, query_rows, key_rows, value_rows, doc_ids, sink_logit,
    out_weight, norm_gain, gate_weight, up_weight, down_weight,
):
    n_a = lax.axis_size("sa")
    row_count, width = stream.shape
    half = row_count // 2
    depth, hidden_here = gate_weight.shape
    share = hidden_here // n_a
    bf = jnp.bfloat16
    vm = pltpu.VMEM
    dma = pltpu.SemaphoreType.DMA
    wide = row_count + 2 * WIN
    per_block = dma((n_a,))
    per_chunk = dma((n_a, CHUNKS))
    per_unit = dma((n_a, UNITS))
    scratch = [
        vm((row_count, width), bf), vm(query_rows.shape, bf), vm((row_count, HD), bf), vm((row_count, HD), bf),
        vm(out_weight.shape, bf), vm(gate_weight.shape, bf), vm(gate_weight.shape, bf),
        vm((hidden_here, depth), bf), vm((hidden_here, depth), bf),
        vm((wide, HD), bf), vm((wide, HD), bf), vm((wide,), jnp.int32),
        vm(query_rows.shape, bf), vm((half, width), bf), vm((half, width), bf),
        vm((half, width), bf), vm((n_a, row_count, width), bf), vm((3 * max(kind_shares(share)), width), bf),
        vm((n_a, half, width), jnp.float32), vm((n_a, half, width), bf), vm((n_a, half, width), bf),
        vm((3, half, width), bf), vm((3, half, width), bf), vm((2, half, width), bf),
        dma((8,)), dma((6,)), dma((6,)), per_block, per_block,
        *([dma, per_block] * 4),
        dma, dma, dma, dma, per_chunk, dma, per_chunk, dma, per_unit,
        dma, dma, dma((3, CHUNKS)), dma((2, CHUNKS)), dma, dma((CHUNKS,)),
    ]
    inside = pl.BlockSpec(memory_space=vm)
    anywhere = pl.BlockSpec(memory_space=pl.ANY)
    return pl.pallas_call(
        fused,
        out_shape=vm((row_count, width), bf),
        in_specs=[anywhere] * 4 + [inside, pl.BlockSpec(memory_space=pltpu.SMEM), anywhere, inside] + [anywhere] * 3,
        out_specs=inside,
        scratch_shapes=scratch,
        compiler_params=pltpu.CompilerParams(collective_id=0, has_side_effects=True, vmem_limit_bytes=56 * 2**20),
        name="fused_layer",
    )(
        stream, query_rows, key_rows, value_rows, doc_ids, sink_logit, out_weight,
        norm_gain.reshape(1, width), gate_weight, up_weight, down_weight,
    )


def solution(mesh):
    n_sp, n_tp = mesh.shape["sp"], mesh.shape["tp"]
    n_a = 4 if n_sp % 4 == 0 else 1
    n_b = n_sp // n_a
    if n_a == 4 and n_b == 4 and n_tp == KVH:
        fine = Mesh(mesh.devices.reshape(n_a, 2, 2, n_tp), AX)
        sp, body = AX[:3], fused_device
    else:
        fine = Mesh(mesh.devices.reshape(n_a, n_b, n_tp), ("sa", "sb", "tp"))
        sp, body = SP, per_device
    in_specs = (
        P(sp, None),
        P(sp, "tp"),
        P(sp, None),
        P(sp, None),
        P(sp),
        P("tp"),
        P("tp", None),
        P(),
        P(sp, "tp"),
        P(sp, "tp"),
        P("tp", sp),
    )
    return jax.shard_map(body, mesh=fine, in_specs=in_specs, out_specs=P(sp, None), check_vma=False)
```

```python
import jax
import jax.numpy as jnp
from jax import lax
from jax.experimental import pallas as pl
from jax.experimental.pallas import tpu as pltpu
from jax.sharding import Mesh, PartitionSpec as P

HEADS = 8
KVH = 2
HD = 128
WIN = 128

norm_eps = 1e-06
masked_low = -1e30
SP = ("sa", "sb")


def halo(value, width):
    peers = lax.axis_size(SP)
    length = value.shape[0]
    up = [(i, i + 1) for i in range(peers - 1)]
    down = [(j, i) for i, j in up]
    before = lax.ppermute(value[length - width :], SP, up)
    after = lax.ppermute(value[:width], SP, down)
    return jnp.concatenate([before, value, after], axis=0)


def exchange(blocks):
    peers = lax.axis_size("sa")
    here = lax.axis_index("sa")
    got = [lax.dynamic_index_in_dim(blocks, here, 0, keepdims=True)]
    for k in range(1, peers):
        out = lax.dynamic_index_in_dim(blocks, lax.rem(here + k, peers), 0, keepdims=True)
        got.append(lax.ppermute(out, "sa", [(i, (i + k) % peers) for i in range(peers)]))
    ring = got[::-1]
    both = jnp.concatenate(ring + ring, axis=0)
    return lax.dynamic_slice_in_dim(both, peers - 1 - here, peers, 0)


def per_device(
    stream,
    query_rows,
    key_rows,
    value_rows,
    doc_ids,
    sink_logit,
    out_weight,
    norm_gain,
    gate_weight,
    up_weight,
    down_weight,
):
    row_count, width = stream.shape
    n_a, n_b, n_tp = lax.axis_size("sa"), lax.axis_size("sb"), lax.axis_size("tp")
    depth, hidden_here = gate_weight.shape
    share = hidden_here // n_a
    tp_place = lax.axis_index("tp")
    sp_place = lax.axis_index(SP)

    def shares(w):
        return w.reshape(depth, n_a, share).transpose(1, 0, 2)

    gate_up = exchange(jnp.concatenate([shares(gate_weight), shares(up_weight)], axis=2))
    gate_up = gate_up.reshape(n_a * depth, 2 * share)
    gate_up = lax.all_gather(gate_up, "sb", axis=0, tiled=True)
    down_mine = exchange(down_weight.reshape(n_a, share, depth))
    down_mine = down_mine.transpose(0, 2, 1).reshape(n_a * depth, share)

    heads_here = query_rows.shape[1] // HD
    group_share = HEADS // KVH
    groups_here = max(1, heads_here // group_share)
    per_group = heads_here // groups_here
    group_first = tp_place * heads_here // group_share
    keys_here = lax.dynamic_slice_in_dim(key_rows, group_first * HD, groups_here * HD, 1)
    values_here = lax.dynamic_slice_in_dim(value_rows, group_first * HD, groups_here * HD, 1)
    docs_col = jnp.broadcast_to(doc_ids.astype(jnp.bfloat16)[:, None], (row_count, HD))
    packed = halo(jnp.concatenate([keys_here, values_here, docs_col], axis=1), WIN)
    span = groups_here * HD
    keys_wide, values_wide = packed[:, :span], packed[:, span : 2 * span]
    docs_wide = packed[:, 2 * span].astype(jnp.int32)
    seq_offset = sp_place * row_count
    seq_total = row_count * n_a * n_b
    query_pos = seq_offset + jnp.arange(row_count, dtype=jnp.int32)
    key_pos = seq_offset - WIN + jnp.arange(row_count + 2 * WIN, dtype=jnp.int32)
    allowed = (
        (jnp.abs(query_pos[:, None] - key_pos[None, :]) <= WIN)
        & (key_pos[None, :] >= 0)
        & (key_pos[None, :] < seq_total)
        & (doc_ids[:, None] == docs_wide[None, :])
    )
    queries = query_rows.reshape(row_count, groups_here, per_group, HD)
    keys_grid = keys_wide.reshape(row_count + 2 * WIN, groups_here, HD)
    values_grid = values_wide.reshape(row_count + 2 * WIN, groups_here, HD)
    scores = jnp.einsum(
        "qgrd,kgd->grqk", queries, keys_grid, preferred_element_type=jnp.float32
    ) * HD ** (-0.5)
    masked = jnp.where(allowed[None, None], scores, masked_low)
    sinks = sink_logit.reshape(groups_here, per_group, 1, 1)
    peak = jnp.maximum(jnp.max(masked, axis=-1, keepdims=True), sinks)
    lifted = jnp.where(allowed[None, None], jnp.exp(masked - peak), 0.0)
    denom = jnp.sum(lifted, axis=-1, keepdims=True) + jnp.exp(sinks - peak)
    probs = (lifted / denom).astype(jnp.bfloat16)
    attended = jnp.einsum("grqk,kgd->qgrd", probs, values_grid, preferred_element_type=jnp.float32)
    attended = attended.astype(jnp.bfloat16).reshape(row_count, heads_here * HD)
    partial_value = jnp.dot(attended, out_weight, preferred_element_type=jnp.float32)

    rows_mine = row_count // n_tp
    branch = lax.psum_scatter(
        partial_value.astype(jnp.bfloat16), "tp", scatter_dimension=0, tiled=True
    )
    stream_mine = lax.dynamic_slice_in_dim(stream, tp_place * rows_mine, rows_mine, 0)
    carried = (stream_mine.astype(jnp.float32) + branch.astype(jnp.float32)).astype(jnp.bfloat16)
    carried_f = carried.astype(jnp.float32)
    normed = (
        carried_f
        * lax.rsqrt(jnp.mean(carried_f * carried_f, axis=1, keepdims=True) + norm_eps)
        * norm_gain[None, :]
    ).astype(jnp.bfloat16)
    normed = normed.reshape(rows_mine, n_a, n_b, depth).transpose(0, 2, 1, 3).reshape(rows_mine, width)
    rows_all = lax.all_gather(normed, ("sa", "tp"), axis=0, tiled=True)
    down_mine, _ = lax.optimization_barrier((down_mine, normed))
    down_all = lax.all_gather(down_mine, "sb", axis=0, tiled=True)

    gate_acc = jnp.dot(rows_all, gate_up[:, :share], preferred_element_type=jnp.float32)
    up_acc = jnp.dot(rows_all, gate_up[:, share:], preferred_element_type=jnp.float32)
    hidden = (jax.nn.silu(gate_acc) * up_acc).astype(jnp.bfloat16)
    terms = lax.dot_general(
        hidden, down_all, (((1,), (1,)), ((), ())), preferred_element_type=jnp.float32
    )
    feed = lax.psum_scatter(
        terms.astype(jnp.bfloat16), ("sa", "tp"), scatter_dimension=0, tiled=True
    )
    feed = feed.reshape(rows_mine, n_b, n_a, depth).transpose(0, 2, 1, 3).reshape(rows_mine, width)
    mixed = (carried_f + 0.5 * feed.astype(jnp.float32)).astype(jnp.bfloat16)
    return lax.all_gather(mixed, "tp", axis=0, tiled=True)


MESH = pl.DeviceIdType.MESH
AX = ("sa", "sy", "sx", "tp")
CHUNKS = 4
UNITS = 2


def kind_shares(share):
    shift = share // 14 // 16 * 16
    return share - shift, share + shift


def fused(
    stream_hbm, query_hbm, key_hbm, value_hbm, docs_ref, sink_ref, out_w_hbm, gain_ref,
    gate_hbm, up_hbm, down_hbm,
    mixed_ref,
    stream_ref, query_ref, key_ref, value_ref, out_w_ref, gate_ref, up_ref, gate_t, up_t,
    keys, values, docs, attended, branch_out, branch_in, carried_keep, rows, weights,
    sum_keep, pair_out, pair_in, chain_out, chain_fwd, chain_back,
    load_s, halo_s, halo_r, a2a_s, a2a_r, x_s, x_r, y_s, y_r, fx_s, fx_r, fy_s, fy_r,
    br_s, br_r, agf_s, agb_s, agz_r, agc_s, agc_r, pair_s, pair_r,
    cf_s, cl_s, cf_r, cb_r, fin_s, fin_r,
):
    n_a, row_count, width = rows.shape
    n_tp = 2
    z, y, x, c = [lax.axis_index(a) for a in AX]
    place = (z * 2 + y) * 2 + x
    places = n_a * 4
    half = row_count // n_tp
    size = half // CHUNKS
    shares = kind_shares(gate_hbm.shape[1] // n_a)
    depth = gate_hbm.shape[0]
    hi = z // 2
    w = z + hi * (3 - 2 * z)
    here = (z, y, x, c)
    partner = (z, y, x, 1 - c)
    x_next = (z, y, 1 - x, c)
    y_next = (z, 1 - y, x, c)
    fwd = (z + 1 - 2 * hi, y, x, c)
    back = (z - 1 + 2 * hi, y, x, c)
    peers = [z + 1 - 2 * (z % 2), (z + 2) % n_a, n_a - 1 - z]

    def block_at(b):
        return b + hi * (3 - 2 * b)

    def remote(src, dst, s_sem, r_sem, device):
        return pltpu.make_async_remote_copy(
            src_ref=src, dst_ref=dst, send_sem=s_sem, recv_sem=r_sem,
            device_id=device, device_id_type=MESH,
        )

    def at_place(p):
        return (p // 4, (p // 2) % 2, p % 2, c)

    head_cols = pl.ds(pl.multiple_of(c * HD, HD), HD)
    edge = row_count - WIN
    blocks = row_count // WIN

    loads = [
        pltpu.make_async_copy(a, b, load_s.at[i])
        for i, (a, b) in enumerate([
            (key_hbm.at[:, head_cols], key_ref), (value_hbm.at[:, head_cols], value_ref),
            (gate_hbm, gate_ref), (up_hbm, up_ref), (query_hbm, query_ref),
            (out_w_hbm, out_w_ref), (stream_hbm, stream_ref),
        ])
    ]
    barrier = pltpu.get_barrier_semaphore()
    nearby = [at_place((place + 1) % places), at_place((place + places - 1) % places)]
    for device in [partner, x_next, y_next] + [(p, y, x, c) for p in peers] + nearby:
        pl.semaphore_signal(barrier, inc=1, device_id=device, device_id_type=MESH)
    for cp in loads:
        cp.start()
    pl.semaphore_wait(barrier, 8)
    loads[0].wait()
    loads[1].wait()

    def halo_copies(to_next):
        if to_next:
            dev, src, dst, o = at_place(place + 1), edge, 0, 0
        else:
            dev, src, dst, o = at_place(place - 1), 0, row_count + WIN, 3
        src, dst = pl.ds(src, WIN), pl.ds(dst, WIN)
        return [
            remote(key_ref.at[src], keys.at[dst], halo_s.at[o], halo_r.at[o], dev),
            remote(value_ref.at[src], values.at[dst], halo_s.at[o + 1], halo_r.at[o + 1], dev),
            remote(docs_ref.at[src], docs.at[dst], halo_s.at[o + 2], halo_r.at[o + 2], dev),
        ]

    @pl.when(place < places - 1)
    def _():
        for cp in halo_copies(True):
            cp.start()

    @pl.when(place > 0)
    def _():
        for cp in halo_copies(False):
            cp.start()

    def column(zz, yy, xx):
        return pl.ds(pl.multiple_of(((zz * 2 + yy) * 2 + xx) * depth, depth), depth)

    mine_col = column(z, y, x)

    def by_kind(act):
        for kind in (0, 1):

            @pl.when(w == kind)
            def _(kind=kind):
                act(kind)

    def peer_kind(kind, k):
        return kind if k == 2 else 1 - kind

    def first_unit(q):
        inner = shares[0] + (q // 2) * (shares[1] - shares[0])
        return pl.multiple_of((q // 2) * (shares[0] + shares[1]) + (q % 2) * inner, 16)

    def own_piece(q, kind, part_id, s_sem, r_sem, device):
        share = shares[kind]
        src = (gate_t, up_t, down_hbm)[part_id].at[pl.ds(first_unit(q), share)]
        dst = weights.at[pl.ds(part_id * share, share), mine_col]
        return remote(src, dst, s_sem, r_sem, device)

    def a2a(kind, k, part_id):
        to = peers[k]
        return own_piece(to, peer_kind(kind, k), part_id, a2a_s.at[to], a2a_r.at[z], (to, y, x, c))

    def own_x(kind, part_id):
        return own_piece(z, kind, part_id, x_s, x_r.at[z], x_next)

    def own_y(kind, part_id):
        return own_piece(z, kind, part_id, y_s, y_r.at[z], y_next)

    def whole(kind, col):
        return weights.at[pl.ds(0, 3 * shares[kind]), col]

    def parts(kind, second):
        cut = 3 * shares[kind] // 32 * 16
        return pl.ds(cut, 3 * shares[kind] - cut) if second else pl.ds(0, cut)

    def wait_bytes(block, s_sem, r_sem):
        return remote(block, block, s_sem, r_sem, here)

    def side(kind, zz, along_x):
        block = whole(kind, column(zz, y, x))
        if along_x:
            return remote(block, block, x_s, x_r.at[zz], x_next)
        return remote(block, block, y_s, y_r.at[zz], y_next)

    def side_arrived(kind, zz, along_x):
        if along_x:
            wait_bytes(whole(kind, column(zz, y, 1 - x)), x_s, x_r.at[zz]).wait_recv()
        else:
            wait_bytes(whole(kind, column(zz, 1 - y, x)), y_s, y_r.at[zz]).wait_recv()

    def corner(kind, zz, along_x):
        if along_x:
            block = weights.at[parts(kind, True), column(zz, 1 - y, x)]
            return remote(block, block, fx_s, fx_r, x_next)
        block = weights.at[parts(kind, False), column(zz, y, 1 - x)]
        return remote(block, block, fy_s, fy_r, y_next)

    def corners_arrived(kind):
        four = pl.ds(0, n_a * depth)
        wait_bytes(weights.at[parts(kind, True), four], fx_s, fx_r).wait_recv()
        wait_bytes(weights.at[parts(kind, False), four], fy_s, fy_r).wait_recv()

    def own_down(kind):
        share = shares[kind]
        return pltpu.make_async_copy(
            down_hbm.at[pl.ds(first_unit(z), share)], weights.at[pl.ds(2 * share, share), mine_col], load_s.at[7]
        )

    @by_kind
    def _(kind):
        a2a(kind, 0, 2).start()
        own_x(kind, 2).start()
        own_y(kind, 2).start()
        if kind == 1:
            a2a(kind, 2, 2).start()
        own_down(kind).start()

    with jax.named_scope("turn"):
        loads[2].wait()
        loads[3].wait()

        def turn(i, _):
            at = pl.ds(pl.multiple_of(i * HD, HD), HD)
            gate_t[at, :] = gate_ref[:, at].T
            up_t[at, :] = up_ref[:, at].T
            return 0

        lax.fori_loop(0, gate_hbm.shape[1] // HD, turn, 0)

    @by_kind
    def _(kind):
        for part_id in range(2):
            a2a(kind, 0, part_id).start()
        if kind == 1:
            for part_id in range(2):
                a2a(kind, 2, part_id).start()
        for part_id in range(2):
            own_x(kind, part_id).start()
            own_y(kind, part_id).start()
        share = shares[kind]
        weights[pl.ds(0, share), mine_col] = gate_t[pl.ds(first_unit(z), share), :]
        weights[pl.ds(share, share), mine_col] = up_t[pl.ds(first_unit(z), share), :]

    def far_send(kind, k):
        for part_id in range(3):
            a2a(kind, k, part_id).start()

    keys[pl.ds(WIN, row_count), :] = key_ref[...]
    values[pl.ds(WIN, row_count), :] = value_ref[...]
    docs[pl.ds(WIN, row_count)] = docs_ref[...]

    @pl.when(place == 0)
    def _():
        keys[pl.ds(0, WIN), :] = jnp.zeros((WIN, HD), keys.dtype)
        values[pl.ds(0, WIN), :] = jnp.zeros((WIN, HD), values.dtype)
        docs[pl.ds(0, WIN)] = jnp.full((WIN,), -1, jnp.int32)

    @pl.when(place == places - 1)
    def _():
        keys[pl.ds(row_count + WIN, WIN), :] = jnp.zeros((WIN, HD), keys.dtype)
        values[pl.ds(row_count + WIN, WIN), :] = jnp.zeros((WIN, HD), values.dtype)
        docs[pl.ds(row_count + WIN, WIN)] = jnp.full((WIN,), -1, jnp.int32)

    heads_here = query_ref.shape[1] // HD
    row_id = lax.broadcasted_iota(jnp.int32, (WIN, 3 * WIN), 0)
    col_id = lax.broadcasted_iota(jnp.int32, (WIN, 3 * WIN), 1)
    band = (col_id >= row_id) & (col_id <= row_id + 2 * WIN)
    loads[4].wait()

    def attend(b):
        mine = jnp.broadcast_to(docs[pl.ds((b + 1) * WIN, WIN)].reshape(1, WIN), (WIN, WIN)).T
        key_docs = jnp.broadcast_to(docs[pl.ds(b * WIN, 3 * WIN)].reshape(1, 3 * WIN), (WIN, 3 * WIN))
        query_docs = jnp.concatenate([mine] * 3, axis=1)
        allowed = band & (key_docs == query_docs)
        k_block = keys[pl.ds(b * WIN, 3 * WIN), :]
        v_block = values[pl.ds(b * WIN, 3 * WIN), :]
        for h in range(heads_here):
            q = query_ref[pl.ds(b * WIN, WIN), pl.ds(h * HD, HD)]
            scores = lax.dot_general(
                q, k_block, (((1,), (1,)), ((), ())), preferred_element_type=jnp.float32
            ) * HD ** (-0.5)
            masked = jnp.where(allowed, scores, masked_low)
            sink = sink_ref[h]
            peak = jnp.maximum(jnp.max(masked, axis=1, keepdims=True), sink)
            lifted = jnp.where(allowed, jnp.exp(masked - peak), 0.0)
            denom = jnp.sum(lifted, axis=1, keepdims=True) + jnp.exp(sink - peak)
            probs = (lifted / denom).astype(jnp.bfloat16)
            got = jnp.dot(probs, v_block, preferred_element_type=jnp.float32)
            attended[pl.ds(b * WIN, WIN), pl.ds(h * HD, HD)] = got.astype(jnp.bfloat16)

    with jax.named_scope("attend_mid"):
        for b in range(1, blocks - 1):
            attend(b)

    with jax.named_scope("halo_wait"):

        @pl.when(place > 0)
        def _():
            for cp in halo_copies(True):
                cp.wait_recv()

        @pl.when(place < places - 1)
        def _():
            for cp in halo_copies(False):
                cp.wait_recv()

    with jax.named_scope("attend_edge"):
        attend(0)
        attend(blocks - 1)

    mine_rows = pl.ds(pl.multiple_of(c * half, half), half)
    other_rows = pl.ds(pl.multiple_of((1 - c) * half, half), half)
    loads[5].wait()
    loads[6].wait()
    branch_out[...] = jnp.dot(
        attended[other_rows, :], out_w_ref[...], preferred_element_type=jnp.float32
    ).astype(jnp.bfloat16)
    branch_copy = remote(branch_out, branch_in, br_s, br_r, partner)
    branch_copy.start()
    own_branch = jnp.dot(
        attended[mine_rows, :], out_w_ref[...], preferred_element_type=jnp.float32
    ).astype(jnp.bfloat16)

    @by_kind
    def _(kind):
        own_down(kind).wait()

    with jax.named_scope("branch_wait"):
        branch_copy.wait_recv()
    branch = (own_branch.astype(jnp.float32) + branch_in[...].astype(jnp.float32)).astype(jnp.bfloat16)
    carried = (
        stream_ref[mine_rows, :].astype(jnp.float32) + branch.astype(jnp.float32)
    ).astype(jnp.bfloat16)
    carried_keep[...] = carried
    carried_f = carried.astype(jnp.float32)
    normed = (
        carried_f
        * lax.rsqrt(jnp.mean(carried_f * carried_f, axis=1, keepdims=True) + norm_eps)
        * gain_ref[...]
    ).astype(jnp.bfloat16)
    rows[z, mine_rows, :] = normed

    def chunk_rows(core, j):
        return pl.ds(pl.multiple_of(core * half + j * size, 16), size)

    def ag(blk, j, to):
        block = rows.at[blk, chunk_rows(c, j)]
        if to == "core":
            return remote(block, block, agc_s, agc_r.at[blk, j], partner)
        if to == "fwd":
            return remote(block, block, agf_s, agz_r.at[blk, j], fwd)
        return remote(block, block, agb_s, agz_r.at[blk, j], back)

    def ag_arrived(blk, j):
        wait_bytes(rows.at[blk, chunk_rows(c, j)], agf_s, agz_r.at[blk, j]).wait_recv()

    def ag_core_arrived(blk, j):
        wait_bytes(rows.at[blk, chunk_rows(1 - c, j)], agc_s, agc_r.at[blk, j]).wait_recv()

    for j in range(CHUNKS):
        ag(z, j, "core").start()

    def rows_fwd():
        for j in range(CHUNKS):
            ag(z, j, "fwd").start()

    def far_sent(kind, k):
        block = whole(peer_kind(kind, k), mine_col)
        wait_bytes(block, a2a_s.at[peers[k]], a2a_r.at[peers[k]]).wait_send()

    def rows_back():
        far_sent(1, 1)
        for j in range(CHUNKS):
            ag(z, j, "back").start()

    def relay_rows(b, j, to=None):
        blk = block_at(b)
        ag_arrived(blk, j)
        if to is not None:
            ag(blk, j, to).start()
        ag(blk, j, "core").start()

    def relay_corner(kind, zz):
        side_arrived(kind, zz, True)
        corner(kind, zz, False).start()
        side_arrived(kind, zz, False)
        corner(kind, zz, True).start()

    def relay_side(kind, k):
        frm = peers[k]
        wait_bytes(whole(kind, column(frm, y, x)), a2a_s.at[frm], a2a_r.at[frm]).wait_recv()
        side(kind, frm, True).start()
        side(kind, frm, False).start()

    def run(plan):
        for name, step, args in plan:
            with jax.named_scope(name):
                step(*args)

    every = range(CHUNKS)
    unit = half // UNITS
    per_unit = CHUNKS // UNITS

    def gather_end():
        run(
            [
                ("corner_own", relay_corner, (0, z)),
                ("side0", relay_side, (0, 0)),
                ("far", far_send, (0, 2)),
                ("rows_fwd", rows_fwd, ()),
                ("side2", relay_side, (0, 2)),
                ("corner0", relay_corner, (0, peers[0])),
                ("side1", relay_side, (0, 1)),
                ("far", far_send, (0, 1)),
                ("corner2", relay_corner, (0, peers[2])),
            ]
            + [("rows1", relay_rows, (1, j)) for j in every]
            + [
                ("corner1", relay_corner, (0, peers[1])),
            ]
            + [("rows2", relay_rows, (2, j)) for j in range(per_unit)]
            + [("last", corners_arrived, (0,))]
        )

    def gather_middle():
        both = [[("rows0", relay_rows, (0, j, "fwd")), ("rows2", relay_rows, (2, j, "back"))] for j in every]
        run(
            [
                ("corner_own", relay_corner, (1, z)),
                ("side0", relay_side, (1, 0)),
                ("far", far_send, (1, 1)),
                ("rows_fwd", rows_fwd, ()),
                ("side2", relay_side, (1, 2)),
                ("corner0", relay_corner, (1, peers[0])),
                ("rows_back", rows_back, ()),
                ("corner2", relay_corner, (1, peers[2])),
                ("side1", relay_side, (1, 1)),
            ]
            + sum(both, [])
            + [
                ("corner1", relay_corner, (1, peers[1])),
                ("rows3", relay_rows, (3, 0, "back")),
                ("rows3", relay_rows, (3, 1, "back")),
                ("last", corners_arrived, (1,)),
            ]
        )

    chain_b = [2, 3, 1]
    dims = (((1,), (1,)), ((), ()))

    def unit_rows(u):
        return pl.ds(pl.multiple_of(u * unit, 16), unit)

    def pair(blk, u):
        return remote(
            pair_out.at[blk, unit_rows(u)], pair_in.at[blk, unit_rows(u)], pair_s, pair_r.at[blk, u], partner
        )

    def chunk(j):
        return pl.ds(pl.multiple_of(j * size, 16), size)

    def chip_sum(blk, j):
        return sum_keep[blk, chunk(j)] + pair_in[blk, chunk(j)].astype(jnp.float32)

    def chain_fwd_copy(slot, j):
        return remote(chain_out.at[slot, chunk(j)], chain_fwd.at[slot, chunk(j)], cf_s, cf_r.at[slot, j], fwd)

    def chain_mid_copy(slot, j):
        return remote(chain_out.at[slot, chunk(j)], chain_back.at[1 - slot, chunk(j)], cf_s, cb_r.at[1 - slot, j], fwd)

    def chain_last_copy(j):
        return remote(chain_out.at[2, chunk(j)], chain_back.at[0, chunk(j)], cl_s, cb_r.at[0, j], back)

    def back_arrived(slot, j):
        wait_bytes(chain_back.at[slot, chunk(j)], cl_s, cb_r.at[slot, j]).wait_recv()

    def send_end(slot, u):
        blk = block_at(chain_b[slot])
        pair(blk, u).wait_recv()
        for t in range(per_unit):
            j = u * per_unit + t
            chain_out[slot, chunk(j)] = chip_sum(blk, j).astype(jnp.bfloat16)
            chain_fwd_copy(slot, j).start()

    def pass_on(slot, j):
        chain_fwd_copy(slot, j).wait_recv()
        total = chip_sum(block_at(chain_b[slot]), j) + chain_fwd[slot, chunk(j)].astype(jnp.float32)
        chain_out[slot, chunk(j)] = total.astype(jnp.bfloat16)
        chain_mid_copy(slot, j).start()

    def feed_forward(kind, blk, u):
        for t in range(per_unit):
            ag_core_arrived(blk, u * per_unit + t)
        share = shares[kind]
        x_rows = jnp.concatenate(
            [rows[blk, pl.ds(pl.multiple_of(h * half + u * unit, 16), unit)] for h in (1 - c, c)], axis=0
        )
        gate_acc = lax.dot_general(x_rows, weights[pl.ds(0, share), :], dims, preferred_element_type=jnp.float32)
        up_acc = lax.dot_general(x_rows, weights[pl.ds(share, share), :], dims, preferred_element_type=jnp.float32)
        hidden = (gate_acc / (1.0 + jnp.exp(-gate_acc)) * up_acc).astype(jnp.bfloat16)
        out = jnp.dot(hidden, weights[pl.ds(2 * share, share), :], preferred_element_type=jnp.float32)
        pair_out[blk, unit_rows(u)] = out[:unit].astype(jnp.bfloat16)
        pair(blk, u).start()
        sum_keep[blk, unit_rows(u)] = out[unit:]

    def pick(step, order):
        late = jnp.where(step == 2, block_at(order[2]), block_at(order[3]))
        return jnp.where(step == 0, block_at(order[0]), jnp.where(step == 1, block_at(order[1]), late))

    def end_unit(i, _):
        step, u = i // UNITS, i % UNITS

        @pl.when(i == 1)
        def _():
            for j in range(per_unit, CHUNKS):
                relay_rows(2, j)

        @pl.when(step == 2)
        def _():
            for t in range(per_unit):
                relay_rows(3, u * per_unit + t)

        feed_forward(0, pick(step, (2, 0, 3, 1)), u)
        for at, slot in ((0, 0), (2, 1), (3, 2)):

            @pl.when(step == at)
            def _(slot=slot):
                send_end(slot, u)

        return 0

    def middle_unit(i, _):
        def back_rows(j):
            relay_rows(3, j, "back")

        def pair_come(b, v):
            pair(block_at(b), v).wait_recv()

        tasks = {
            1: [(back_rows, 2), (pair_come, 2, 0), (pass_on, 0, 0)],
            2: [(back_rows, 3), (pass_on, 0, 1)],
            3: [(pair_come, 2, 1), (pass_on, 0, 2)],
            4: [(pass_on, 0, 3)],
            6: [(pair_come, 3, 0), (pass_on, 1, 0)],
            7: [(pair_come, 3, 1), (pass_on, 1, 1)],
        }
        for at, todo in tasks.items():

            @pl.when(i == at)
            def _(todo=todo):
                for act, *args in todo:
                    act(*args)

        feed_forward(1, pick(i // UNITS, (2, 3, 0, 1)), i % UNITS)
        return 0

    @pl.when(w == 0)
    def _():
        gather_end()
        with jax.named_scope("ffn"):
            lax.fori_loop(0, n_a * UNITS, end_unit, 0)

    @pl.when(w == 1)
    def _():
        gather_middle()
        with jax.named_scope("ffn"):
            lax.fori_loop(0, n_a * UNITS, middle_unit, 0)

    def last(core, j):
        block = mixed_ref.at[chunk_rows(core, j)]
        return remote(block, block, fin_s, fin_r.at[j], partner)

    def finish(j, total):
        feed = total.astype(jnp.bfloat16).astype(jnp.float32)
        mixed_ref[chunk_rows(c, j), :] = (
            carried_keep[chunk(j)].astype(jnp.float32) + 0.5 * feed
        ).astype(jnp.bfloat16)
        last(c, j).start()

    @pl.when(w == 0)
    def _():
        for u in range(UNITS):
            pair(z, u).wait_recv()
        for j in range(CHUNKS):
            with jax.named_scope(f"fin{j}"):
                back_arrived(0, j)
                finish(j, chip_sum(z, j) + chain_back[0, chunk(j)].astype(jnp.float32))

    @pl.when(w == 1)
    def _():
        for b in (0, 1):
            for u in range(UNITS):
                pair(block_at(b), u).wait_recv()

        def pass_back(j):
            back_arrived(0, j)
            total = chip_sum(block_at(0), j) + chain_back[0, chunk(j)].astype(jnp.float32)
            chain_out[2, chunk(j)] = total.astype(jnp.bfloat16)
            chain_last_copy(j).start()

        def close(j):
            back_arrived(1, j)
            chain_fwd_copy(2, j).wait_recv()
            finish(
                j,
                chip_sum(z, j)
                + chain_fwd[2, chunk(j)].astype(jnp.float32)
                + chain_back[1, chunk(j)].astype(jnp.float32),
            )

        plan = [("on1", pass_on, (1, 2)), ("pback", pass_back, (0,)), ("on1", pass_on, (1, 3))]
        plan += [("pback", pass_back, (1,)), ("pback", pass_back, (2,))]
        plan += [("pback", pass_back, (CHUNKS - 1,))]
        plan += [("close", close, (j,)) for j in range(CHUNKS)]
        run(plan)

    with jax.named_scope("sends_done"):
        @pl.when(place < places - 1)
        def _():
            for cp in halo_copies(True):
                cp.wait_send()

        @pl.when(place > 0)
        def _():
            for cp in halo_copies(False):
                cp.wait_send()

        @by_kind
        def _(kind):
            far_sent(kind, 0)
            far_sent(kind, 2)
            if kind == 0:
                far_sent(kind, 1)
            four = pl.ds(0, n_a * depth)
            wait_bytes(whole(kind, four), x_s, x_r.at[0]).wait_send()
            wait_bytes(whole(kind, four), y_s, y_r.at[0]).wait_send()
            wait_bytes(weights.at[parts(kind, True), four], fx_s, fx_r).wait_send()
            wait_bytes(weights.at[parts(kind, False), four], fy_s, fy_r).wait_send()

        wait_bytes(pair_out, pair_s, pair_r.at[0, 0]).wait_send()
        wait_bytes(rows.at[:, mine_rows], agc_s, agc_r.at[0, 0]).wait_send()
        branch_copy.wait_send()

        @pl.when(w == 0)
        def _():
            wait_bytes(rows.at[z, mine_rows], agf_s, agz_r.at[0, 0]).wait_send()
            wait_bytes(chain_out, cf_s, cf_r.at[0, 0]).wait_send()

        @pl.when(w == 1)
        def _():
            wait_bytes(rows.at[pl.ds(0, 2), mine_rows], agf_s, agz_r.at[0, 0]).wait_send()
            wait_bytes(rows.at[pl.ds(0, 3), mine_rows], agb_s, agz_r.at[0, 0]).wait_send()
            wait_bytes(chain_out.at[pl.ds(0, 2)], cf_s, cf_r.at[0, 0]).wait_send()
            wait_bytes(chain_out.at[2], cl_s, cb_r.at[0, 0]).wait_send()

        for j in range(CHUNKS):
            last(1 - c, j).wait_recv()
        wait_bytes(mixed_ref.at[mine_rows], fin_s, fin_r.at[0]).wait_send()


def fused_device(
    stream, query_rows, key_rows, value_rows, doc_ids, sink_logit,
    out_weight, norm_gain, gate_weight, up_weight, down_weight,
):
    n_a = lax.axis_size("sa")
    row_count, width = stream.shape
    half = row_count // 2
    depth, hidden_here = gate_weight.shape
    share = hidden_here // n_a
    bf = jnp.bfloat16
    vm = pltpu.VMEM
    dma = pltpu.SemaphoreType.DMA
    wide = row_count + 2 * WIN
    per_block = dma((n_a,))
    per_chunk = dma((n_a, CHUNKS))
    per_unit = dma((n_a, UNITS))
    scratch = [
        vm((row_count, width), bf), vm(query_rows.shape, bf), vm((row_count, HD), bf), vm((row_count, HD), bf),
        vm(out_weight.shape, bf), vm(gate_weight.shape, bf), vm(gate_weight.shape, bf),
        vm((hidden_here, depth), bf), vm((hidden_here, depth), bf),
        vm((wide, HD), bf), vm((wide, HD), bf), vm((wide,), jnp.int32),
        vm(query_rows.shape, bf), vm((half, width), bf), vm((half, width), bf),
        vm((half, width), bf), vm((n_a, row_count, width), bf), vm((3 * max(kind_shares(share)), width), bf),
        vm((n_a, half, width), jnp.float32), vm((n_a, half, width), bf), vm((n_a, half, width), bf),
        vm((3, half, width), bf), vm((3, half, width), bf), vm((2, half, width), bf),
        dma((8,)), dma((6,)), dma((6,)), per_block, per_block,
        *([dma, per_block] * 2), *([dma] * 4),
        dma, dma, dma, dma, per_chunk, dma, per_chunk, dma, per_unit,
        dma, dma, dma((3, CHUNKS)), dma((2, CHUNKS)), dma, dma((CHUNKS,)),
    ]
    inside = pl.BlockSpec(memory_space=vm)
    anywhere = pl.BlockSpec(memory_space=pl.ANY)
    return pl.pallas_call(
        fused,
        out_shape=vm((row_count, width), bf),
        in_specs=[anywhere] * 4 + [inside, pl.BlockSpec(memory_space=pltpu.SMEM), anywhere, inside] + [anywhere] * 3,
        out_specs=inside,
        scratch_shapes=scratch,
        compiler_params=pltpu.CompilerParams(collective_id=0, has_side_effects=True, vmem_limit_bytes=56 * 2**20),
        name="fused_layer",
    )(
        stream, query_rows, key_rows, value_rows, doc_ids, sink_logit, out_weight,
        norm_gain.reshape(1, width), gate_weight, up_weight, down_weight,
    )


def solution(mesh):
    n_sp, n_tp = mesh.shape["sp"], mesh.shape["tp"]
    n_a = 4 if n_sp % 4 == 0 else 1
    n_b = n_sp // n_a
    if n_a == 4 and n_b == 4 and n_tp == KVH:
        fine = Mesh(mesh.devices.reshape(n_a, 2, 2, n_tp), AX)
        sp, body = AX[:3], fused_device
    else:
        fine = Mesh(mesh.devices.reshape(n_a, n_b, n_tp), ("sa", "sb", "tp"))
        sp, body = SP, per_device
    in_specs = (
        P(sp, None),
        P(sp, "tp"),
        P(sp, None),
        P(sp, None),
        P(sp),
        P("tp"),
        P("tp", None),
        P(),
        P(sp, "tp"),
        P(sp, "tp"),
        P("tp", sp),
    )
    return jax.shard_map(body, mesh=fine, in_specs=in_specs, out_specs=P(sp, None), check_vma=False)
```
